128 devices in a mesh: grp: 4 (over y, x), ep: 32 (over z, core).
Axes of the slice: x: 2, y: 2, z: 16, core: 2. Of those that a mesh axis runs over, the one named last changes fastest.
The devices are a block of a 8x8x16 slice.
Arguments:
- resid: bfloat16 [1536, 2048], P(('grp', 'ep')), parts along dimension 0, may hold values from -6 to 6
- norm_gains: float32 [4, 2048], replicated, may hold values from 0.1 to 1.9
- w_query: bfloat16 [2048, 1024], P(None, 'ep'), may hold values from -0.125 to 0.125
- w_key: bfloat16 [2048, 1024], P(None, 'ep'), may hold values from -0.125 to 0.125
- w_value: bfloat16 [2048, 1024], P(None, 'ep'), may hold values from -0.125 to 0.125
- w_outgate: bfloat16 [2048, 1024], P(None, 'ep'), may hold values from -0.125 to 0.125
- w_igate: bfloat16 [2048, 8], replicated, may hold values from -0.125 to 0.125
- w_fgate: bfloat16 [2048, 8], replicated, may hold values from -0.125 to 0.125
- igate_bias: float32 [8], replicated, may hold values from -1 to 1
- fgate_bias: float32 [8], replicated, may hold values from -1 to 5
- state_matrix: float32 [1536, 8, 128, 128], P(('grp', 'ep')), parts along dimension 0, may hold values from -0.8 to 0.8
- state_norm: float32 [1536, 8, 128], P(('grp', 'ep')), parts along dimension 0, may hold values from -2.4 to 2.4
- state_max: float32 [1536, 8], P(('grp', 'ep')), parts along dimension 0, may hold values from -1 to 1
- w_mix_out: bfloat16 [1024, 2048], replicated, may hold values from -0.1875 to 0.1875
- routes: int32 [1536, 2], P(('grp', 'ep')), parts along dimension 0, may hold values from 0 to 31, all different within a row; in each aligned block of 12 rows (0 to 11, 12 to 23, ...) at most 2 rows name the same one
- route_scores: bfloat16 [1536, 2], P(('grp', 'ep')), parts along dimension 0, may hold values from 0.099609375 to 1
- expert_gate: bfloat16 [32, 2048, 512], P('ep'), may hold values from -0.125 to 0.125
- expert_up: bfloat16 [32, 2048, 512], P('ep'), may hold values from -0.125 to 0.125
- expert_down: bfloat16 [32, 512, 2048], P('ep'), may hold values from -0.25 to 0.25
- dense_gate: bfloat16 [2048, 8192], P(None, 'ep'), may hold values from -0.125 to 0.125
- dense_up: bfloat16 [2048, 8192], P(None, 'ep'), may hold values from -0.125 to 0.125
- dense_down: bfloat16 [8192, 2048], P('ep'), may hold values from -0.0625 to 0.0625
- branch_weight: bfloat16 [2048], replicated, may hold values from -0.125 to 0.125
Outputs:
- out_stream: bfloat16 [1536, 2048], P(('grp', 'ep')), parts along dimension 0
- new_matrix: float32 [1536, 8, 128, 128], P(('grp', 'ep')), parts along dimension 0
- new_norm: float32 [1536, 8, 128], P(('grp', 'ep')), parts along dimension 0
- new_max: float32 [1536, 8], P(('grp', 'ep')), parts along dimension 0
The draws below stay inside these ranges and needn't reach their ends.
There are 4 independent parts, one for each index of `grp`. The reference program is written for one: setup_inputs(seed, part) draws one part's arguments, and reference() takes and returns one part's arrays. A program takes and returns all parts, laid end to end along the dimension named above; an argument that names none is the same for every part. Nothing has to cross between parts.
Inputs may be any that keep to these rules, and one draw needn't show every extreme that they name: `routes`: each row names 2 different experts. In each aligned block of 12 rows (the rows of one device) no expert is named by more than 2 rows, a bound that some block reaches.
All inputs are finite; a program needn't handle non-finite values.
Results may differ from the reference program's by a relative error of at most 0.015.
Values may be sent and summed in bfloat16 or wider, within the bound.
No kernel may reach another device: no remote copies, remote signals or barrier semaphores. Data moves between devices by JAX's collectives and lax.ppermute only.
A program may use at most 128 MiB of HBM per device.

```python
import math
import jax
import jax.numpy as jnp
import numpy as np
from jax import lax

D = 2048
NH = 8
DH = 128
FE = 512
FFD = 8192
TOPK = 2
SEQ_DEV = 12
INNER = 1024
CAP = 2
EXPERTS = 32
SEQS = 384
N_EP = 32


def steps_of(stream_key, shape, cuts, low, largest):
    factor_of, own = 1.0, jax.random.fold_in(stream_key, 6)
    for position, blocks in cuts:
        heights = jnp.exp(jax.random.uniform(jax.random.fold_in(own, position), (blocks,), jnp.float32, low / len(cuts), largest / len(cuts)))
        factor_of = factor_of * jnp.repeat(heights, shape[position] // blocks).reshape([-1 if axis == position else 1 for axis in range(len(shape))])
    return factor_of


def shared_out(own_key, own, number, rows, number_of, top, most, skew):
    ranking = jax.random.permutation(own_key, number_of)
    heavy_load, ordinary = portions_of(number_of, rows * top, most, skew, True), portions_of(number_of, rows * top, most, skew, False)
    places = jnp.arange(number_of)

    def named(sizes, turn):
        used = int((sizes > 0).sum())
        fixed = max(1, used // 4)
        moved = fixed + (places - fixed + turn * (used - fixed)) % max(1, number_of - fixed)
        return jnp.zeros((number_of,), jnp.int32).at[ranking[jnp.where(places < fixed, places, moved)]].set(jnp.asarray(sizes, jnp.int32))

    sizes = jnp.where(number % 4 == 0, named(heavy_load, number // 4), named(ordinary, number - number // 4 - 1))
    mixed = jax.random.permutation(jax.random.fold_in(own, 3), number_of)
    source_of, taker = mixed[0:number_of // 2 * 2:2], mixed[1:number_of // 2 * 2:2]
    slack = jnp.minimum(sizes[source_of] - 1, most - sizes[taker]) // 2
    slack = jnp.where((source_of == ranking[0]) | (taker == ranking[0]) | (sizes[taker] == 0), 0, jnp.maximum(slack, 0))
    moved = jax.random.randint(jax.random.fold_in(own, 4), (number_of // 2,), 0, 1 << 20) % (slack + 1)
    sizes = sizes.at[source_of].add(-moved).at[taker].add(moved)
    items = jnp.searchsorted(jnp.cumsum(sizes), jnp.arange(rows * top), side="right").astype(jnp.int32)
    table = items.reshape(top, rows).T
    table = table[jax.random.permutation(jax.random.fold_in(own, 1), rows)]
    turn = jax.random.randint(jax.random.fold_in(own, 2), (rows, 1), 0, top)
    return jnp.take_along_axis(table, (jnp.arange(top)[None, :] + turn) % top, axis=1)


def portions_of(number_of, total, limit, skew, full):
    loads = [(1 << 20) // math.isqrt(standing ** skew) + 1 for standing in range(1, number_of + 1)]
    largest = limit if full else min(limit, max(-(-total // number_of), total * loads[0] // sum(loads)))
    least = 1 if total - largest >= number_of - 1 else 0
    counts, spare = [largest] + [least] * (number_of - 1), total - largest - least * (number_of - 1)
    while spare > 0:
        candidates = [i for i in range(1, number_of) if counts[i] < largest] or [i for i in range(1, number_of) if counts[i] < limit]
        pool, left = sum([loads[i] for i in candidates]), spare
        for i in candidates:
            more = min(limit - counts[i], max(1, left * loads[i] // pool), spare)
            counts[i] = counts[i] + more
            spare = spare - more
    return np.array(counts)


def gaussian(rng, extent, scale, limit, cuts=(), kind=jnp.bfloat16):
    values = scale * jax.random.normal(rng, extent, jnp.float32)
    if cuts:
        values = values * steps_of(rng, extent, cuts, -0.22, 0.18)
    return jnp.clip(values, -limit, limit).astype(kind)


def setup_inputs(seed: int = 0, part: int = 0) -> dict:
    splits = jax.random.split(jax.random.key(seed), 24)
    own_keys = jax.random.split(jax.random.fold_in(splits[23], part), 24)
    resid = gaussian(own_keys[0], (SEQS, D), 1.0, 6.0, ((0, 32),))
    norm_gains = jnp.clip(1.0 + 0.18 * jax.random.normal(splits[1], (4, D), jnp.float32), 0.1, 1.9)
    w_query = gaussian(splits[2], (D, INNER), D ** -0.5, 0.125, ((1, 32),))
    w_key = gaussian(splits[3], (D, INNER), D ** -0.5, 0.125, ((1, 32),))
    w_value = gaussian(splits[4], (D, INNER), D ** -0.5, 0.125, ((1, 32),))
    w_outgate = gaussian(splits[5], (D, INNER), D ** -0.5, 0.125, ((1, 32),))
    w_igate = gaussian(splits[6], (D, NH), D ** -0.5, 0.125)
    w_fgate = gaussian(splits[7], (D, NH), D ** -0.5, 0.125)
    igate_bias = jnp.clip(jax.random.uniform(splits[8], (NH,), jnp.float32, -1.0, 1.0), -1.0, 1.0)
    fgate_bias = jnp.clip(jax.random.uniform(splits[9], (NH,), jnp.float32, -1.0, 5.0), -1.0, 5.0)
    state_matrix = gaussian(own_keys[10], (SEQS, NH, DH, DH), 0.1, 0.8, ((0, 32),), jnp.float32)
    state_norm = gaussian(own_keys[11], (SEQS, NH, DH), 0.3, 2.4, ((0, 32),), jnp.float32)
    state_max = jnp.clip(jax.random.uniform(own_keys[12], (SEQS, NH), jnp.float32, -1.0, 1.0) * steps_of(own_keys[12], (SEQS, NH), ((0, 32),), -0.4, 0.0), -1.0, 1.0)
    w_mix_out = gaussian(splits[13], (INNER, D), INNER ** -0.5, 0.1875)
    routes_keys = jax.random.split(jax.random.fold_in(own_keys[14], 1), SEQS // SEQ_DEV)
    routes_turns = jax.random.permutation(jax.random.fold_in(own_keys[14], 3), SEQS // SEQ_DEV)
    routes = jax.vmap(lambda own, number: shared_out(jax.random.fold_in(own_keys[14], 2), own, number, SEQ_DEV, EXPERTS, TOPK, CAP, 2))(routes_keys, routes_turns).reshape((SEQS, TOPK))
    route_scores = jnp.clip(jnp.exp(math.log(1.0) - 2.306499 * jax.random.uniform(own_keys[15], (SEQS, TOPK), jnp.float32) ** steps_of(own_keys[15], (SEQS, TOPK), ((0, 32),), -0.2, 0.2)), 0.099609375, 1.0).astype(jnp.bfloat16)
    expert_gate = gaussian(splits[16], (EXPERTS, D, FE), D ** -0.5, 0.125, ((0, 32),))
    expert_up = gaussian(splits[17], (EXPERTS, D, FE), D ** -0.5, 0.125, ((0, 32),))
    expert_down = gaussian(splits[18], (EXPERTS, FE, D), FE ** -0.5, 0.25, ((0, 32),))
    dense_gate = gaussian(splits[19], (D, FFD), D ** -0.5, 0.125, ((1, 32),))
    dense_up = gaussian(splits[20], (D, FFD), D ** -0.5, 0.125, ((1, 32),))
    dense_down = gaussian(splits[21], (FFD, D), FFD ** -0.5, 0.0625, ((0, 32),))
    branch_weight = gaussian(splits[22], (D,), D ** -0.5, 0.125)
    return {"resid": resid, "norm_gains": norm_gains, "w_query": w_query, "w_key": w_key, "w_value": w_value, "w_outgate": w_outgate, "w_igate": w_igate, "w_fgate": w_fgate, "igate_bias": igate_bias, "fgate_bias": fgate_bias, "state_matrix": state_matrix, "state_norm": state_norm, "state_max": state_max, "w_mix_out": w_mix_out, "routes": routes, "route_scores": route_scores, "expert_gate": expert_gate, "expert_up": expert_up, "expert_down": expert_down, "dense_gate": dense_gate, "dense_up": dense_up, "dense_down": dense_down, "branch_weight": branch_weight}


def rms_scale(values, gains):
    return values * lax.rsqrt(lax.optimization_barrier(jnp.mean(values * values, axis=-1, keepdims=True)) + 1e-06) * gains.astype(jnp.float32)

def round_half(values):
    return lax.optimization_barrier(values.astype(jnp.bfloat16)).astype(jnp.float32)

def expert_ffn(picked, gate_matrix, up_matrix, down_matrix):
    gate_out = jnp.dot(picked, gate_matrix, preferred_element_type=jnp.float32)
    up_out = jnp.dot(picked, up_matrix, preferred_element_type=jnp.float32)
    hidden = (jax.nn.silu(gate_out) * up_out).astype(jnp.bfloat16)
    return jnp.dot(hidden, down_matrix, preferred_element_type=jnp.float32).astype(jnp.bfloat16)

def expert_mix(branch_in, routes, route_scores, expert_gate, expert_up, expert_down):
    tokens = branch_in.shape[0]
    experts = expert_gate.shape[0]
    onehot = (routes[:, :, None] == jnp.arange(experts, dtype=jnp.int32)[None, None, :]).astype(jnp.float32)
    scores = route_scores.astype(jnp.float32)
    shares = scores / lax.optimization_barrier(jnp.sum(scores, axis=-1, keepdims=True))
    weights = lax.optimization_barrier(jnp.sum(shares[:, :, None] * onehot, axis=1))
    hit_count = lax.optimization_barrier(jnp.sum(onehot, axis=1))
    hit_int = hit_count.astype(jnp.int32).reshape(N_EP, SEQ_DEV, experts)
    rank_index = jnp.cumsum(hit_int, axis=1) - hit_int
    block_base = (jnp.arange(N_EP, dtype=jnp.int32) * CAP)[:, None, None]
    slot_index = (rank_index + block_base).reshape(tokens, experts).T
    hit_flags = hit_count.T
    weight_rows = weights.T
    slot_range = jnp.arange(N_EP * CAP, dtype=jnp.int32)

    def expert_step(running_sum, expert_index):
        chosen = ((slot_index[expert_index][None, :] == slot_range[:, None]) & (hit_flags[expert_index][None, :] > 0.5)).astype(jnp.float32)
        picked = jnp.dot(chosen.astype(jnp.bfloat16), branch_in, preferred_element_type=jnp.float32).astype(jnp.bfloat16)
        produced = expert_ffn(picked, expert_gate[expert_index], expert_up[expert_index], expert_down[expert_index])
        weighted = chosen * weight_rows[expert_index][None, :]
        contribution = jnp.dot(weighted.T, produced.astype(jnp.float32), precision=lax.Precision.HIGHEST)
        running_sum = running_sum + round_half(contribution)
        return (running_sum, None)
    start_sum = jnp.zeros(branch_in.shape, jnp.float32)
    result, ignored = lax.scan(expert_step, start_sum, jnp.arange(experts, dtype=jnp.int32))
    return result

def reference(resid, norm_gains, w_query, w_key, w_value, w_outgate, w_igate, w_fgate, igate_bias, fgate_bias, state_matrix, state_norm, state_max, w_mix_out, routes, route_scores, expert_gate, expert_up, expert_down, dense_gate, dense_up, dense_down, branch_weight):
    seqs = resid.shape[0]
    heads = state_matrix.shape[1]
    head_size = state_matrix.shape[2]
    resid32 = resid.astype(jnp.float32)
    normed = rms_scale(resid32, norm_gains[0]).astype(jnp.bfloat16)

    def project(matrix):
        result = jnp.dot(normed, matrix, preferred_element_type=jnp.float32).astype(jnp.bfloat16)
        return result.astype(jnp.float32).reshape(seqs, heads, head_size)
    query = project(w_query)
    key_heads = project(w_key) * head_size ** (-0.5)
    value_heads = project(w_value)
    outgate = project(w_outgate)
    ipre = jnp.dot(normed, w_igate, preferred_element_type=jnp.float32) + igate_bias
    fpre = jnp.dot(normed, w_fgate, preferred_element_type=jnp.float32) + fgate_bias
    logf = jax.nn.log_sigmoid(fpre)
    new_max = jnp.maximum(ipre, logf + state_max)
    keep_gain = jnp.exp(logf + state_max - new_max)
    write_gain = jnp.exp(ipre - new_max)
    new_matrix = keep_gain[:, :, None, None] * state_matrix + write_gain[:, :, None, None] * value_heads[:, :, :, None] * key_heads[:, :, None, :]
    new_norm = keep_gain[:, :, None] * state_norm + write_gain[:, :, None] * key_heads
    numer = jnp.einsum('shed,shd->she', new_matrix, query, precision=lax.Precision.HIGHEST)
    denom = lax.optimization_barrier(jnp.sum(new_norm * query, axis=-1))
    cell = numer / jnp.maximum(jnp.abs(denom), 1.0)[:, :, None]
    gated = (jax.nn.sigmoid(outgate) * cell).reshape(seqs, heads * head_size).astype(jnp.bfloat16)
    mixed = jnp.dot(gated, w_mix_out, preferred_element_type=jnp.float32)
    middle = resid32 + rms_scale(mixed, norm_gains[1])
    branch_in = rms_scale(middle, norm_gains[2]).astype(jnp.bfloat16)
    moe = expert_mix(branch_in, routes, route_scores, expert_gate, expert_up, expert_down)
    gate_out = jnp.dot(branch_in, dense_gate, preferred_element_type=jnp.float32)
    up_out = jnp.dot(branch_in, dense_up, preferred_element_type=jnp.float32)
    hidden = (jax.nn.silu(gate_out) * up_out).astype(jnp.bfloat16)
    logit = jnp.dot(branch_in, branch_weight, preferred_element_type=jnp.float32)
    branch_gate = jax.nn.sigmoid(logit)[:, None]
    block_width = hidden.shape[1] // N_EP
    hidden_blocks = jnp.transpose(hidden.reshape(seqs, N_EP, block_width), (1, 0, 2))
    down_blocks = dense_down.reshape(N_EP, block_width, dense_down.shape[1])

    def dense_step(running_sum, pieces):
        hidden_block, down_block = pieces
        term = jnp.dot(hidden_block, down_block, preferred_element_type=jnp.float32) * branch_gate
        return (running_sum + round_half(term), None)
    dense, ignored = lax.scan(dense_step, jnp.zeros(middle.shape, jnp.float32), (hidden_blocks, down_blocks))
    combined = moe + dense
    out_stream = (middle + rms_scale(combined, norm_gains[3])).astype(jnp.bfloat16)
    return (out_stream, new_matrix, new_norm, new_max)
```

```python
import functools

import jax
import jax.numpy as jnp
from jax import lax
from jax.experimental import pallas as pl
from jax.experimental.pallas import tpu as pltpu
from jax.sharding import PartitionSpec as P

CAP = 2
INTERPRET = False
F32 = jnp.float32
BF16 = jnp.bfloat16


def call(kernel, outs, args, scratch=(), vmem=16, flops=1000000, name=None):
    single = not isinstance(outs, (list, tuple))
    shapes = [outs] if single else list(outs)
    result = pl.pallas_call(
        kernel,
        out_shape=[jax.ShapeDtypeStruct(s, d) for s, d in shapes] if not single
        else None,
        scratch_shapes=[pltpu.VMEM(s, d) for s, d in scratch],
        compiler_params=pltpu.CompilerParams(vmem_limit_bytes=vmem << 20),
        cost_estimate=pl.CostEstimate(flops=flops, bytes_accessed=1000000, transcendentals=0),
        interpret=INTERPRET,
        name=name,
    )(*args)
    return result


def rms(values, gains):
    return values * lax.rsqrt(jnp.mean(values * values, axis=-1, keepdims=True) + 1e-06) * gains


def core():
    return lax.rem(lax.axis_index("ep"), 2)


def dot(a, b):
    return jnp.dot(a, b, preferred_element_type=F32)


def half_of(c, values):
    h = values.shape[-1] // 2
    return jnp.where(c == 0, values[:, :h], values[:, h:])


def norm_kernel(own_ref, other_ref, gains_ref, out_ref, rows):
    c = core()
    r = own_ref.shape[0]
    own, other = own_ref[...].astype(F32), other_ref[...].astype(F32)
    rows[:r] = jnp.where(c == 0, own, other)
    rows[r : 2 * r] = jnp.where(c == 0, other, own)
    normed = rms(rows[...], gains_ref[0:1, :])
    half = half_of(c, normed).astype(BF16)
    for z in range(out_ref.shape[0]):
        out_ref[z] = half


def gates_kernel(
    resid_ref, gains_ref, wi_ref, wf_ref, bi_ref, bf_ref, max_ref, routes_ref, scores_ref,
    keep_ref, write_ref, newmax_ref, info_ref,
):
    r = resid_ref.shape[0]
    normed = rms(resid_ref[...].astype(F32), gains_ref[0:1, :]).astype(BF16)
    ipre = dot(normed, wi_ref[...]) + bi_ref[...]
    fpre = dot(normed, wf_ref[...]) + bf_ref[...]
    logf = jnp.minimum(fpre, 0.0) - jnp.log1p(jnp.exp(-jnp.abs(fpre)))
    decayed = logf + max_ref[...]
    new_max = jnp.maximum(ipre, decayed)
    keep_ref[...] = jnp.exp(decayed - new_max)
    write_ref[...] = jnp.exp(ipre - new_max)
    newmax_ref[...] = new_max
    lanes = lax.broadcasted_iota(jnp.int32, (r, 128), 1)
    row = lax.broadcasted_iota(jnp.int32, (r, 128), 0)
    total = jnp.zeros((r, 128), F32)
    columns = (routes_ref[:, 0:1].astype(F32), routes_ref[:, 1:2].astype(F32),
               scores_ref[:, 0:1].astype(F32), scores_ref[:, 1:2].astype(F32))
    for k, column in enumerate(columns):
        total = total + jnp.where(lanes == row + k * r, column, 0.0)
    info = jnp.sum(total, axis=0, keepdims=True)
    info_ref[...] = jnp.broadcast_to(info, info_ref.shape).astype(BF16)


def proj_kernel(x_ref, y_ref, w_ref, info_ref, out_ref):
    c = core()
    nz, r2, h = x_ref.shape
    x = x_ref[...].reshape(nz * r2, h)
    y = y_ref[...].reshape(nz * r2, h)
    wx = w_ref[pl.ds(pl.multiple_of(c * h, h), h), :]
    wy = w_ref[pl.ds(pl.multiple_of((1 - c) * h, h), h), :]
    p = (dot(x, wx) + dot(y, wy)).astype(BF16).reshape(nz, r2, w_ref.shape[1])
    out_ref[:, :r2, :] = p
    for z in range(nz):
        out_ref[z, r2 : r2 + 8, :] = info_ref[...]


def cell_kernel(
    a_ref, b_ref, keep_ref, write_ref, m_ref, norm_ref, mix_ref, resid_ref, gains_ref,
    middle_ref, mine_ref, send_ref, newnorm_ref, keys_ref, wvt_ref,
    p0, p1, q_scr, wv_scr, gated,
):
    c = core()
    r, heads, dh = norm_ref.shape
    nz = a_ref.shape[0]
    cols = heads * dh // (2 * nz)
    per = dh // cols
    p0[...] = jnp.zeros_like(p0)
    p1[...] = jnp.zeros_like(p1)
    for z in range(nz):
        a, b = a_ref[z].astype(F32), b_ref[z].astype(F32)
        a = jnp.where(c == 0, a[:r], a[r : 2 * r])
        b = jnp.where(c == 0, b[:r], b[r : 2 * r])
        p0[z, :r] = jnp.where(c == 0, a, b)
        p1[z, :r] = jnp.where(c == 0, b, a)
    lanes = lax.broadcasted_iota(jnp.int32, (16, dh), 1)

    def gather(h, kind):
        total = jnp.zeros((16, dh), F32)
        for p in range(per):
            ep = h * per + p
            piece = (p0 if ep % 2 == 0 else p1)[ep // 2]
            shift = ((p - kind) * cols) % dh
            piece = pltpu.roll(piece, shift, 1) if shift else piece
            total = jnp.where((lanes >= p * cols) & (lanes < (p + 1) * cols), piece, total)
        return total

    wv_scr[...] = jnp.zeros_like(wv_scr)
    for h in range(heads):
        q_scr[h] = gather(h, 0)
        keys_ref[h] = gather(h, 1) * dh ** (-0.5)
        wv_scr[h * 16 : h * 16 + r] = gather(h, 2)[:r] * write_ref[:, h : h + 1]
    wvt_ref[...] = wv_scr[...].T
    lane128 = lax.broadcasted_iota(jnp.int32, (dh, 128), 1)

    def step(s, acc):
        for h in range(heads):
            prod = m_ref[s, h] * q_scr[h, pl.ds(s, 1), :]
            red = jnp.sum(prod, axis=1, keepdims=True)
            acc = jnp.where(lane128 == h * 16 + s, red, acc)
        return acc

    numer = lax.fori_loop(0, r, step, jnp.zeros((dh, 128), F32)).T
    for h in range(heads):
        query, key = q_scr[h][:r], keys_ref[h][:r]
        outgate = gather(h, 3)[:r]
        keep, write = keep_ref[:, h : h + 1], write_ref[:, h : h + 1]
        new_norm = keep * norm_ref[:, h, :] + write * key
        newnorm_ref[:, h, :] = new_norm
        denom = jnp.sum(new_norm * query, axis=1, keepdims=True)
        kq = jnp.sum(key * query, axis=1, keepdims=True)
        top = keep * numer[h * 16 : h * 16 + r] + wv_scr[h * 16 : h * 16 + r] * kq
        cell = top / jnp.maximum(jnp.abs(denom), 1.0)
        gated[:, h * dh : (h + 1) * dh] = (jax.nn.sigmoid(outgate) * cell).astype(BF16)
    mixed = dot(gated[...], mix_ref[...])
    middle = resid_ref[...].astype(F32) + rms(mixed, gains_ref[1:2, :])
    middle_ref[...] = middle
    branch = rms(middle, gains_ref[2:3, :])
    mine_ref[...] = half_of(c, branch).astype(BF16)
    send_ref[...] = half_of(1 - c, branch).astype(BF16)


def update_kernel(keep_ref, keys_ref, wvt_ref, m_ref, out_ref):
    r, heads, dh, _ = m_ref.shape

    def step(s, carry):
        rolled = pltpu.roll(wvt_ref[...], lax.rem(128 - s, 128), 1)
        for h in range(heads):
            keep = keep_ref[pl.ds(s, 1), h : h + 1]
            key = keys_ref[h, pl.ds(s, 1), :]
            out_ref[s, h] = keep * m_ref[s, h] + rolled[:, h * 16 : h * 16 + 1] * key
        return carry

    lax.fori_loop(0, r, step, 0)


def pair_kernel(mine_ref, got_ref, out_ref, rows):
    c = core()
    r = mine_ref.shape[0]
    mine, got = mine_ref[...].astype(F32), got_ref[...].astype(F32)
    rows[:r] = jnp.where(c == 0, mine, got)
    rows[r : 2 * r] = jnp.where(c == 0, got, mine)
    both = rows[...].astype(BF16)
    for z in range(out_ref.shape[0]):
        out_ref[z] = both


def silu_mul(gate, up):
    return (gate * jax.nn.sigmoid(gate) * up).astype(BF16)


def branch_kernel(
    x_ref, y_ref, a_ref, b_ref, eg_ref, eu_ref, ed_ref, dg_ref, du_ref, dd_ref, bw_ref,
    keep_ref, send_ref, info, made,
):
    c = core()
    me = lax.axis_index("ep").astype(F32)
    nz, r2, h = x_ref.shape
    r = r2 // 2
    rows = nz * r2
    slots = 2 * nz * CAP
    at = pl.ds(pl.multiple_of(c * h, h), h)
    to = pl.ds(pl.multiple_of((1 - c) * h, h), h)
    x = x_ref[...].reshape(rows, h)
    y = y_ref[...].reshape(rows, h)
    low = lax.broadcasted_iota(jnp.int32, (r2, 128), 0) < r
    for z in range(nz):
        a, b = a_ref[z, r2 : r2 + 8, :].astype(F32)[0:1], b_ref[z, r2 : r2 + 8, :].astype(F32)[0:1]
        first, second = jnp.where(c == 0, a, b), jnp.where(c == 0, b, a)
        info[z * r2 : (z + 1) * r2] = jnp.where(low, first, second)
    lane = lax.broadcasted_iota(jnp.int32, (rows, 128), 1)
    token = lax.broadcasted_iota(jnp.int32, (rows, 128), 0)
    block = lax.div(token, r)
    inner = token - block * r
    table = info[...]

    def column(k):
        return jnp.sum(jnp.where(lane == inner + k * r, table, 0.0), axis=1, keepdims=True)

    e0, e1, s0, s1 = column(0), column(1), column(2), column(3)
    hit0, hit1 = e0 == me, e1 == me
    hit = jnp.where(hit0 | hit1, 1.0, 0.0)
    weight = jnp.where(hit0, s0, jnp.where(hit1, s1, 0.0)) / (s0 + s1)
    row_i = lax.broadcasted_iota(jnp.int32, (rows, rows), 0)
    col_i = lax.broadcasted_iota(jnp.int32, (rows, rows), 1)
    earlier = (col_i < row_i) & (lax.div(row_i, r) == lax.div(col_i, r))
    earlier = jnp.where(earlier, 1.0, 0.0).astype(BF16)
    rank = dot(earlier, jnp.broadcast_to(hit, (rows, 128)).astype(BF16))
    slot = block.astype(F32) * CAP + rank
    chosen = jnp.where((slot == lane.astype(F32)) & (hit > 0.5), 1.0, 0.0)
    picker = chosen.T[:slots].astype(BF16)
    placer = chosen[:, :slots].astype(BF16)
    px = dot(picker, x).astype(BF16)
    py = dot(picker, y).astype(BF16)
    gate = dot(px, eg_ref[0, at, :]) + dot(py, eg_ref[0, to, :])
    up = dot(px, eu_ref[0, at, :]) + dot(py, eu_ref[0, to, :])
    made[...] = dot(silu_mul(gate, up), ed_ref[0]).astype(BF16)

    gate = dot(x, dg_ref[at, :]) + dot(y, dg_ref[to, :])
    up = dot(x, du_ref[at, :]) + dot(y, du_ref[to, :])
    hidden = silu_mul(gate, up)
    logit = jnp.sum(x.astype(F32) * bw_ref[:, at].astype(F32), axis=1, keepdims=True)
    logit = logit + jnp.sum(y.astype(F32) * bw_ref[:, to].astype(F32), axis=1, keepdims=True)
    sig = jax.nn.sigmoid(logit)
    for where, ref in ((at, keep_ref), (to, send_ref)):
        part = dot(hidden, dd_ref[:, where]) * sig
        part = part + dot(placer, made[:, where]) * weight
        ref[...] = part.astype(ref.dtype)


def add_kernel(keep_ref, got_ref, out_ref):
    total = keep_ref[...] + got_ref[...].astype(F32)
    out_ref[...] = total.astype(BF16).reshape(out_ref.shape)


def sum_kernel(x_ref, mine_ref, send_ref):
    c = core()
    r = mine_ref.shape[0]
    total = x_ref[0].astype(F32)
    for z in range(1, x_ref.shape[0]):
        total = total + x_ref[z].astype(F32)
    mine_ref[...] = jnp.where(c == 0, total[:r], total[r:])
    send_ref[...] = jnp.where(c == 0, total[r:], total[:r])


def final_kernel(mine_ref, got_ref, middle_ref, gains_ref, out_ref):
    c = core()
    h = mine_ref.shape[1]
    mine, got = mine_ref[...], got_ref[...]
    low, high = jnp.where(c == 0, mine, got), jnp.where(c == 0, got, mine)
    square = jnp.sum(low * low, axis=1, keepdims=True) + jnp.sum(high * high, axis=1, keepdims=True)
    scale = lax.rsqrt(square / (2 * h) + 1e-06)
    gains = gains_ref[3:4, :]
    out_ref[:, :h] = (middle_ref[:, :h] + low * scale * gains[:, :h]).astype(BF16)
    out_ref[:, h:] = (middle_ref[:, h:] + high * scale * gains[:, h:]).astype(BF16)


def local(
    resid, norm_gains, w_query, w_key, w_value, w_outgate, w_igate, w_fgate, igate_bias,
    fgate_bias, state_matrix, state_norm, state_max, w_mix_out, routes, route_scores,
    expert_gate, expert_up, expert_down, dense_gate, dense_up, dense_down, branch_weight,
):
    n = lax.axis_size("ep")
    nz = n // 2
    r, d = resid.shape
    h = d // 2
    heads, dh = state_matrix.shape[1:3]
    inner = heads * dh
    groups = [[2 * z + c for z in range(nz)] for c in range(2)]
    pairs = [(i, i ^ 1) for i in range(n)]

    def swap(x):
        return lax.ppermute(x, "ep", pairs)

    def exchange(x):
        return lax.all_to_all(x, "ep", 0, 0, axis_index_groups=groups)

    other = swap(resid)
    chunk, = call(norm_kernel, [((nz, 2 * r, h), BF16)], (resid, other, norm_gains),
                  scratch=[((2 * r, d), F32)], name="norm")
    x = exchange(chunk)
    keep, write, new_max, info = call(
        gates_kernel,
        [((r, heads), F32), ((r, heads), F32), ((r, heads), F32), ((8, 128), BF16)],
        (resid, norm_gains, w_igate, w_fgate, igate_bias.reshape(1, heads),
         fgate_bias.reshape(1, heads), state_max, routes, route_scores), name="gates")
    w_all = jnp.concatenate([w_query, w_key, w_value, w_outgate], axis=1)
    y = swap(x)
    projected, = call(proj_kernel, [((nz, 2 * r + 8, w_all.shape[1]), BF16)],
                      (x, y, w_all, info), name="proj")
    a = exchange(projected)
    b = swap(a)
    middle, mine, send, new_norm, keys, wvt = call(
        cell_kernel,
        [((r, d), F32), ((r, h), BF16), ((r, h), BF16), ((r, heads, dh), F32),
         ((heads, 16, dh), F32), ((dh, 128), F32)],
        (a, b, keep, write, state_matrix, state_norm, w_mix_out, resid, norm_gains),
        scratch=[((nz, 16, dh), F32), ((nz, 16, dh), F32), ((heads, 16, dh), F32),
                 ((128, dh), F32), ((r, inner), BF16)],
        vmem=24, name="cell")
    got = swap(send)
    chunk, = call(pair_kernel, [((nz, 2 * r, h), BF16)], (mine, got),
                  scratch=[((2 * r, h), F32)], name="pair")
    x = exchange(chunk)
    new_matrix, = call(update_kernel, [(state_matrix.shape, F32)],
                       (keep, keys, wvt, state_matrix), vmem=24, flops=100000000, name="update")
    y = swap(x)
    part, send = call(
        branch_kernel, [((n * r, h), F32), ((n * r, h), BF16)],
        (x, y, a, b, expert_gate, expert_up, expert_down, dense_gate, dense_up, dense_down,
         branch_weight.reshape(1, d)),
        scratch=[((n * r, 128), F32), ((n * CAP, d), BF16)], vmem=32, name="branch")
    got = swap(send)
    chunk, = call(add_kernel, [((nz, 2 * r, h), BF16)], (part, got), name="add")
    x = exchange(chunk)
    mine, send = call(sum_kernel, [((r, h), F32), ((r, h), F32)], (x,), name="sum")
    got = swap(send)
    out, = call(final_kernel, [((r, d), BF16)], (mine, got, middle, norm_gains), name="final")
    return (out, new_matrix, new_norm, new_max)


def solution(mesh):
    placed = (
        P(("grp", "ep"), None), P(), P(None, "ep"), P(None, "ep"), P(None, "ep"), P(None, "ep"),
        P(), P(), P(), P(), P(("grp", "ep"), None, None, None), P(("grp", "ep"), None, None),
        P(("grp", "ep"), None), P(), P(("grp", "ep"), None), P(("grp", "ep"), None),
        P("ep", None, None), P("ep", None, None), P("ep", None, None), P(None, "ep"),
        P(None, "ep"), P("ep", None), P(),
    )
    return jax.shard_map(
        local,
        mesh=mesh,
        in_specs=placed,
        out_specs=(
            P(("grp", "ep"), None),
            P(("grp", "ep"), None, None, None),
            P(("grp", "ep"), None, None),
            P(("grp", "ep"), None),
        ),
        check_vma=False,
    )
```

```python
import functools

import jax
import jax.numpy as jnp
from jax import lax
from jax.experimental import pallas as pl
from jax.experimental.pallas import tpu as pltpu
from jax.sharding import PartitionSpec as P

CAP = 2
INTERPRET = False
F32 = jnp.float32
BF16 = jnp.bfloat16


def call(kernel, outs, args, scratch=(), vmem=16, flops=1000000, name=None, hbm=(), sems=0, **grid):
    if hbm:
        if not INTERPRET:
            args = [pltpu.with_memory_space_constraint(x, pltpu.HBM) if i in hbm else x
                    for i, x in enumerate(args)]
        grid["in_specs"] = [
            pl.BlockSpec(memory_space=pltpu.HBM if i in hbm else pltpu.VMEM)
            for i in range(len(args))]
    result = pl.pallas_call(
        kernel,
        out_shape=[jax.ShapeDtypeStruct(s, d) for s, d in outs],
        scratch_shapes=[pltpu.VMEM(s, d) for s, d in scratch]
        + ([pltpu.SemaphoreType.DMA((sems,))] if sems else []),
        **grid,
        compiler_params=pltpu.CompilerParams(vmem_limit_bytes=vmem << 20),
        cost_estimate=pl.CostEstimate(flops=flops, bytes_accessed=1000000, transcendentals=0),
        interpret=INTERPRET,
        name=name,
    )(*args)
    return result


def rms(values, gains):
    return values * lax.rsqrt(jnp.mean(values * values, axis=-1, keepdims=True) + 1e-06) * gains


def core():
    return lax.rem(lax.axis_index("ep"), 2)


def dot_t(a, b):
    return lax.dot_general(a, b, (((1,), (1,)), ((), ())), preferred_element_type=F32)


def dot(a, b):
    return jnp.dot(a, b, preferred_element_type=F32)


def half_of(c, values):
    h = values.shape[-1] // 2
    return jnp.where(c == 0, values[:, :h], values[:, h:])


def norm_kernel(own_ref, other_ref, gains_ref, out_ref, rows):
    c = core()
    r = own_ref.shape[0]
    own, other = own_ref[...].astype(F32), other_ref[...].astype(F32)
    rows[:r] = jnp.where(c == 0, own, other)
    rows[r : 2 * r] = jnp.where(c == 0, other, own)
    normed = rms(rows[...], gains_ref[0:1, :])
    out_ref[...] = half_of(c, normed).astype(BF16)


def gates_kernel(
    resid_ref, gains_ref, wi_ref, wf_ref, bi_ref, bf_ref, bit_ref, bft_ref, max_ref, maxt_ref,
    routes_ref, scores_ref, wq_ref, wk_ref, wv_ref, wo_ref,
    keep_ref, write_ref, newmax_ref, info_ref, weights_ref, sems,
):
    r = resid_ref.shape[0]
    cols = wq_ref.shape[0]
    copies = [
        pltpu.make_async_copy(w, weights_ref.at[pl.ds(k * cols, cols)], sems.at[k])
        for k, w in enumerate((wq_ref, wk_ref, wv_ref, wo_ref))]
    for copy in copies:
        copy.start()
    normed = rms(resid_ref[...].astype(F32), gains_ref[0:1, :]).astype(BF16)

    def gates(ipre, fpre, old):
        logf = jnp.minimum(fpre, 0.0) - jnp.log1p(jnp.exp(-jnp.abs(fpre)))
        return ipre, logf + old, jnp.maximum(ipre, logf + old)

    ipre, decayed, new_max = gates(
        dot_t(normed, wi_ref[...]) + bi_ref[...], dot_t(normed, wf_ref[...]) + bf_ref[...],
        max_ref[...])
    keep_ref[...] = jnp.exp(decayed - new_max)
    write_ref[...] = jnp.exp(ipre - new_max)
    newmax_ref[...] = gates(
        dot_t(wi_ref[...], normed) + bit_ref[...], dot_t(wf_ref[...], normed) + bft_ref[...],
        maxt_ref[...])[2]
    lanes = lax.broadcasted_iota(jnp.int32, (r, 128), 1)
    row = lax.broadcasted_iota(jnp.int32, (r, 128), 0)
    total = jnp.zeros((r, 128), F32)
    columns = (routes_ref[:, 0:1].astype(F32), routes_ref[:, 1:2].astype(F32),
               scores_ref[:, 0:1].astype(F32), scores_ref[:, 1:2].astype(F32))
    for k, column in enumerate(columns):
        total = total + jnp.where(lanes == row + k * r, column, 0.0)
    info = jnp.sum(total, axis=0, keepdims=True)
    info_ref[...] = jnp.broadcast_to(info, info_ref.shape).astype(BF16)
    for copy in copies:
        copy.wait()


def proj_kernel(x_ref, y_ref, w_ref, info_ref, out_ref):
    c = core()
    nz, r2, h = x_ref.shape
    x = x_ref[...].reshape(nz * r2, h)
    y = y_ref[...].reshape(nz * r2, h)
    at = pl.ds(pl.multiple_of(c * h, h), h)
    to = pl.ds(pl.multiple_of((1 - c) * h, h), h)
    p = (dot_t(x, w_ref[:, at]) + dot_t(y, w_ref[:, to])).astype(BF16)
    out_ref[:, :r2, :] = p.reshape(nz, r2, p.shape[1])
    for z in range(nz):
        out_ref[z, r2 : r2 + 8, :] = info_ref[...]


def cell_kernel(
    a_ref, b_ref, keep_ref, write_ref, m_ref, norm_ref, mix_ref, resid_ref, gains_ref,
    middle_ref, mine_ref, send_ref, newnorm_ref, keys_ref, wvt_ref,
    p0, p1, q_scr, wv_scr, gated, m_scr, mix_scr, sems,
):
    c = core()
    r, heads, dh = norm_ref.shape

    def state_copy(s):
        return pltpu.make_async_copy(m_ref.at[s], m_scr.at[s], sems.at[s])

    mix_copy = pltpu.make_async_copy(mix_ref, mix_scr, sems.at[r])
    for s in range(r):
        state_copy(s).start()
    mix_copy.start()
    nz = a_ref.shape[0]
    cols = heads * dh // (2 * nz)
    per = dh // cols
    p0[...] = jnp.zeros_like(p0)
    p1[...] = jnp.zeros_like(p1)
    for z in range(nz):
        a, b = a_ref[z].astype(F32), b_ref[z].astype(F32)
        a = jnp.where(c == 0, a[:r], a[r : 2 * r])
        b = jnp.where(c == 0, b[:r], b[r : 2 * r])
        p0[z, :r] = jnp.where(c == 0, a, b)
        p1[z, :r] = jnp.where(c == 0, b, a)
    lanes = lax.broadcasted_iota(jnp.int32, (16, dh), 1)

    def gather(h, kind):
        total = jnp.zeros((16, dh), F32)
        for p in range(per):
            ep = h * per + p
            piece = (p0 if ep % 2 == 0 else p1)[ep // 2]
            shift = ((p - kind) * cols) % dh
            piece = pltpu.roll(piece, shift, 1) if shift else piece
            total = jnp.where((lanes >= p * cols) & (lanes < (p + 1) * cols), piece, total)
        return total

    wv_scr[...] = jnp.zeros_like(wv_scr)
    for h in range(heads):
        q_scr[h] = gather(h, 0)
        keys_ref[h] = gather(h, 1) * dh ** (-0.5)
        wv_scr[h * 16 : h * 16 + r] = gather(h, 2)[:r] * write_ref[:, h : h + 1]
    wvt_ref[...] = wv_scr[...].T
    lane128 = lax.broadcasted_iota(jnp.int32, (dh, 128), 1)

    def step(s, acc):
        state_copy(s).wait()
        for h in range(heads):
            prod = m_scr[s, h] * q_scr[h, pl.ds(s, 1), :]
            red = jnp.sum(prod, axis=1, keepdims=True)
            acc = jnp.where(lane128 == h * 16 + s, red, acc)
        return acc

    numer = lax.fori_loop(0, r, step, jnp.zeros((dh, 128), F32)).T
    for h in range(heads):
        query, key = q_scr[h][:r], keys_ref[h][:r]
        outgate = gather(h, 3)[:r]
        keep, write = keep_ref[:, h : h + 1], write_ref[:, h : h + 1]
        new_norm = keep * norm_ref[:, h, :] + write * key
        newnorm_ref[:, h, :] = new_norm
        denom = jnp.sum(new_norm * query, axis=1, keepdims=True)
        kq = jnp.sum(key * query, axis=1, keepdims=True)
        top = keep * numer[h * 16 : h * 16 + r] + wv_scr[h * 16 : h * 16 + r] * kq
        cell = top / jnp.maximum(jnp.abs(denom), 1.0)
        gated[:, h * dh : (h + 1) * dh] = (jax.nn.sigmoid(outgate) * cell).astype(BF16)
    mix_copy.wait()
    mixed = dot(gated[...], mix_scr[...])
    middle = resid_ref[...].astype(F32) + rms(mixed, gains_ref[1:2, :])
    middle_ref[...] = middle
    branch = rms(middle, gains_ref[2:3, :])
    mine_ref[...] = half_of(c, branch).astype(BF16)
    send_ref[...] = half_of(1 - c, branch).astype(BF16)


def update_kernel(keep_ref, keys_ref, wvt_ref, after_ref, m_ref, out_ref, token_ref):
    token_ref[...] = jnp.zeros_like(token_ref)
    heads = m_ref.shape[1]
    s = pl.program_id(0)
    rolled = pltpu.roll(wvt_ref[...], lax.rem(128 - s, 128), 1)
    for h in range(heads):
        keep = keep_ref[pl.ds(s, 1), h : h + 1]
        key = keys_ref[h, pl.ds(s, 1), :]
        out_ref[0, h] = keep * m_ref[0, h] + rolled[:, h * 16 : h * 16 + 1] * key


def pair_kernel(mine_ref, got_ref, out_ref, rows):
    c = core()
    r = mine_ref.shape[0]
    mine, got = mine_ref[...].astype(F32), got_ref[...].astype(F32)
    rows[:r] = jnp.where(c == 0, mine, got)
    rows[r : 2 * r] = jnp.where(c == 0, got, mine)
    out_ref[...] = rows[...].astype(BF16)


def silu_mul(gate, up):
    return (gate * jax.nn.sigmoid(gate) * up).astype(BF16)


def branch_kernel(
    x_ref, y_ref, a_ref, b_ref, eg_ref, eu_ref, ed_ref, dg_ref, du_ref, dd_ref, bw_ref,
    keep_ref, send_ref, info, made,
):
    c = core()
    me = lax.axis_index("ep").astype(F32)
    nz, r2, h = x_ref.shape
    r = r2 // 2
    rows = nz * r2
    slots = 2 * nz * CAP
    at = pl.ds(pl.multiple_of(c * h, h), h)
    to = pl.ds(pl.multiple_of((1 - c) * h, h), h)
    x = x_ref[...].reshape(rows, h)
    y = y_ref[...].reshape(rows, h)
    low = lax.broadcasted_iota(jnp.int32, (r2, 128), 0) < r
    for z in range(nz):
        a, b = a_ref[z, r2 : r2 + 8, :].astype(F32)[0:1], b_ref[z, r2 : r2 + 8, :].astype(F32)[0:1]
        first, second = jnp.where(c == 0, a, b), jnp.where(c == 0, b, a)
        info[z * r2 : (z + 1) * r2] = jnp.where(low, first, second)
    lane = lax.broadcasted_iota(jnp.int32, (rows, 128), 1)
    token = lax.broadcasted_iota(jnp.int32, (rows, 128), 0)
    block = lax.div(token, r)
    inner = token - block * r
    table = info[...]

    def column(k):
        return jnp.sum(jnp.where(lane == inner + k * r, table, 0.0), axis=1, keepdims=True)

    e0, e1, s0, s1 = column(0), column(1), column(2), column(3)
    hit0, hit1 = e0 == me, e1 == me
    hit = jnp.where(hit0 | hit1, 1.0, 0.0)
    weight = jnp.where(hit0, s0, jnp.where(hit1, s1, 0.0)) / (s0 + s1)
    row_i = lax.broadcasted_iota(jnp.int32, (rows, rows), 0)
    col_i = lax.broadcasted_iota(jnp.int32, (rows, rows), 1)
    earlier = (col_i < row_i) & (lax.div(row_i, r) == lax.div(col_i, r))
    earlier = jnp.where(earlier, 1.0, 0.0).astype(BF16)
    rank = dot(earlier, jnp.broadcast_to(hit, (rows, 128)).astype(BF16))
    slot = block.astype(F32) * CAP + rank
    chosen = jnp.where((slot == lane.astype(F32)) & (hit > 0.5), 1.0, 0.0)
    picker = chosen.T[:slots].astype(BF16)
    placer = chosen[:, :slots].astype(BF16)
    px = dot(picker, x).astype(BF16)
    py = dot(picker, y).astype(BF16)
    gate = dot(px, eg_ref[0, at, :]) + dot(py, eg_ref[0, to, :])
    up = dot(px, eu_ref[0, at, :]) + dot(py, eu_ref[0, to, :])
    made[...] = dot(silu_mul(gate, up), ed_ref[0]).astype(BF16)

    gate = dot(x, dg_ref[at, :]) + dot(y, dg_ref[to, :])
    up = dot(x, du_ref[at, :]) + dot(y, du_ref[to, :])
    hidden = silu_mul(gate, up)
    logit = jnp.sum(x.astype(F32) * bw_ref[:, at].astype(F32), axis=1, keepdims=True)
    logit = logit + jnp.sum(y.astype(F32) * bw_ref[:, to].astype(F32), axis=1, keepdims=True)
    sig = jax.nn.sigmoid(logit)
    for where, ref in ((at, keep_ref), (to, send_ref)):
        part = dot(hidden, dd_ref[:, where]) * sig
        part = part + dot(placer, made[:, where]) * weight
        ref[...] = part.astype(ref.dtype)


NEAR = (1, -1, 2, -2)
FAR = 5


def spread_kernel(keep_ref, got_ref, *out_refs):
    z = lax.div(lax.axis_index("ep"), 2)
    own_ref, near_refs, last_ref = out_refs[0], out_refs[1:-1], out_refs[-1]
    nz = keep_ref.shape[0]

    def term(offset):
        at = lax.rem(z + offset + nz, nz)
        return keep_ref[at] + got_ref[at].astype(F32)

    for i, far in enumerate((0, FAR, -FAR)):
        own_ref[i] = term(far)
        for near, ref in zip(NEAR, near_refs):
            ref[i] = term(near + far).astype(BF16)
    last_ref[...] = term(nz // 2).astype(BF16)


def fold_kernel(
    own_ref, a_ref, b_ref, c_ref, d_ref, last_ref, token_ref, own_out, plus_ref, minus_ref,
):
    def total(i):
        t = own_ref[i] + a_ref[i].astype(F32) + b_ref[i].astype(F32)
        return t + c_ref[i].astype(F32) + d_ref[i].astype(F32)

    own_out[...] = total(0)
    plus_ref[...] = (total(1) + last_ref[...].astype(F32)).astype(BF16)
    minus_ref[...] = total(2).astype(BF16)


def sum_kernel(own_ref, a_ref, b_ref, mine_ref, send_ref):
    c = core()
    r = mine_ref.shape[0]
    total = own_ref[...] + a_ref[...].astype(F32) + b_ref[...].astype(F32)
    mine_ref[...] = jnp.where(c == 0, total[:r], total[r:])
    send_ref[...] = jnp.where(c == 0, total[r:], total[:r])


def final_kernel(mine_ref, got_ref, middle_ref, gains_ref, out_ref):
    c = core()
    h = mine_ref.shape[1]
    mine, got = mine_ref[...], got_ref[...]
    low, high = jnp.where(c == 0, mine, got), jnp.where(c == 0, got, mine)
    square = jnp.sum(low * low, axis=1, keepdims=True) + jnp.sum(high * high, axis=1, keepdims=True)
    scale = lax.rsqrt(square / (2 * h) + 1e-06)
    gains = gains_ref[3:4, :]
    out_ref[:, :h] = (middle_ref[:, :h] + low * scale * gains[:, :h]).astype(BF16)
    out_ref[:, h:] = (middle_ref[:, h:] + high * scale * gains[:, h:]).astype(BF16)


def local(
    resid, norm_gains, w_query, w_key, w_value, w_outgate, w_igate, w_fgate, igate_bias,
    fgate_bias, state_matrix, state_norm, state_max, w_mix_out, routes, route_scores,
    expert_gate, expert_up, expert_down, dense_gate, dense_up, dense_down, branch_weight,
):
    n = lax.axis_size("ep")
    nz = n // 2
    r, d = resid.shape
    h = d // 2
    heads, dh = state_matrix.shape[1:3]
    inner = heads * dh
    groups = [[2 * z + c for z in range(nz)] for c in range(2)]
    pairs = [(i, i ^ 1) for i in range(n)]

    def swap(x):
        return lax.ppermute(x, "ep", pairs)

    def exchange(x):
        return lax.all_to_all(x, "ep", 0, 0, axis_index_groups=groups)

    def shift(x, offset):
        return lax.ppermute(
            x, "ep", [(2 * z + c, 2 * ((z + offset) % nz) + c) for z in range(nz) for c in range(2)])

    def gather(x):
        return lax.all_gather(x, "ep", axis=0, axis_index_groups=groups)

    other = swap(resid)
    chunk, = call(norm_kernel, [((2 * r, h), BF16)], (resid, other, norm_gains),
                  scratch=[((2 * r, d), F32)], name="norm")
    x = gather(chunk)
    keep, write, new_max, info, w_all = call(
        gates_kernel,
        [((r, heads), F32), ((r, heads), F32), ((heads, r), F32), ((8, 128), BF16),
         ((4 * inner // n, d), BF16)],
        (resid, norm_gains, w_igate.T, w_fgate.T, igate_bias.reshape(1, heads),
         fgate_bias.reshape(1, heads), igate_bias.reshape(heads, 1),
         fgate_bias.reshape(heads, 1), state_max, state_max.T, routes, route_scores,
         w_query.T, w_key.T, w_value.T, w_outgate.T),
        hbm=(12, 13, 14, 15), sems=4, name="gates")
    y = swap(x)
    projected, = call(
        proj_kernel, [((nz, 2 * r + 8, 4 * inner // n), BF16)],
        (x, y, w_all, info), name="proj")
    a = exchange(projected)
    b = swap(a)
    middle, mine, send, new_norm, keys, wvt = call(
        cell_kernel,
        [((r, d), F32), ((r, h), BF16), ((r, h), BF16), ((r, heads, dh), F32),
         ((heads, 16, dh), F32), ((dh, 128), F32)],
        (a, b, keep, write, state_matrix, state_norm, w_mix_out, resid, norm_gains),
        scratch=[((nz, 16, dh), F32), ((nz, 16, dh), F32), ((heads, 16, dh), F32),
                 ((128, dh), F32), ((r, inner), BF16), (state_matrix.shape, F32),
                 (w_mix_out.shape, BF16)],
        hbm=(4, 6), sems=r + 1, vmem=24, name="cell")
    got = swap(send)
    chunk, = call(pair_kernel, [((2 * r, h), BF16)], (mine, got),
                  scratch=[((2 * r, h), F32)], name="pair")
    x = gather(chunk)
    y = swap(x)
    part, send = call(
        branch_kernel, [((n * r, h), F32), ((n * r, h), BF16)],
        (x, y, a, b, expert_gate, expert_up, expert_down, dense_gate, dense_up, dense_down,
         branch_weight.reshape(1, d)),
        scratch=[((n * r, 128), F32), ((n * CAP, d), BF16)], vmem=32, name="branch")
    got = swap(send)
    tile = (2 * r, h)
    own, *near, last = call(
        spread_kernel, [((3,) + tile, F32)] + [((3,) + tile, BF16)] * 4 + [(tile, BF16)],
        (part.reshape((nz,) + tile), got.reshape((nz,) + tile)), name="spread")
    near = [shift(x, offset) for x, offset in zip(near, NEAR)]
    tail, last = last, shift(last, nz // 2 - FAR)
    new_matrix, token = call(
        update_kernel, [(state_matrix.shape, F32), ((8, 128), F32)],
        (keep, keys, wvt, tail, state_matrix),
        grid=(r,),
        in_specs=[pl.BlockSpec(keep.shape, lambda s: (0, 0)),
                  pl.BlockSpec(keys.shape, lambda s: (0, 0, 0)),
                  pl.BlockSpec(wvt.shape, lambda s: (0, 0)),
                  pl.BlockSpec((8, 128), lambda s: (0, 0)),
                  pl.BlockSpec((1, heads, dh, dh), lambda s: (s, 0, 0, 0))],
        out_specs=[pl.BlockSpec((1, heads, dh, dh), lambda s: (s, 0, 0, 0)),
                   pl.BlockSpec((8, 128), lambda s: (0, 0))],
        vmem=8, flops=500000000, name="update")
    own, plus, minus = call(fold_kernel, [(tile, F32), (tile, BF16), (tile, BF16)],
                            (own, *near, last, token), name="fold")
    plus, minus = shift(plus, FAR), shift(minus, -FAR)
    mine, send = call(sum_kernel, [((r, h), F32), ((r, h), F32)], (own, plus, minus), name="sum")
    got = swap(send)
    out, = call(final_kernel, [((r, d), BF16)], (mine, got, middle, norm_gains), name="final")
    return (out, new_matrix, new_norm, new_max.T)


def solution(mesh):
    placed = (
        P(("grp", "ep"), None), P(), P(None, "ep"), P(None, "ep"), P(None, "ep"), P(None, "ep"),
        P(), P(), P(), P(), P(("grp", "ep"), None, None, None), P(("grp", "ep"), None, None),
        P(("grp", "ep"), None), P(), P(("grp", "ep"), None), P(("grp", "ep"), None),
        P("ep", None, None), P("ep", None, None), P("ep", None, None), P(None, "ep"),
        P(None, "ep"), P("ep", None), P(),
    )
    return jax.shard_map(
        local,
        mesh=mesh,
        in_specs=placed,
        out_specs=(
            P(("grp", "ep"), None),
            P(("grp", "ep"), None, None, None),
            P(("grp", "ep"), None, None),
            P(("grp", "ep"), None),
        ),
        check_vma=False,
    )
```

```python
import functools

import jax
import jax.numpy as jnp
from jax import lax
from jax.experimental import pallas as pl
from jax.experimental.pallas import tpu as pltpu
from jax.sharding import PartitionSpec as P

CAP = 2
INTERPRET = False
F32 = jnp.float32
BF16 = jnp.bfloat16


def in_hbm(x):
    return x if INTERPRET else pltpu.with_memory_space_constraint(x, pltpu.HBM)


def call(kernel, outs, args, scratch=(), vmem=16, flops=1000000, name=None, hbm=(), sems=0, held=(), **grid):
    if hbm:
        args = [in_hbm(x) if i in hbm else x for i, x in enumerate(args)]
        grid["in_specs"] = [
            pl.BlockSpec(memory_space=pltpu.HBM if i in hbm else pltpu.VMEM)
            for i in range(len(args))]
    result = pl.pallas_call(
        kernel,
        out_shape=[pltpu.VMEM(s, d) if i in held and not INTERPRET else jax.ShapeDtypeStruct(s, d)
                   for i, (s, d) in enumerate(outs)],
        scratch_shapes=[pltpu.VMEM(s, d) for s, d in scratch]
        + ([pltpu.SemaphoreType.DMA((sems,))] if sems else []),
        **grid,
        compiler_params=pltpu.CompilerParams(vmem_limit_bytes=vmem << 20),
        cost_estimate=pl.CostEstimate(flops=flops, bytes_accessed=1000000, transcendentals=0),
        interpret=INTERPRET,
        name=name,
    )(*args)
    return result


def rms(values, gains):
    return values * lax.rsqrt(jnp.mean(values * values, axis=-1, keepdims=True) + 1e-06) * gains


def core():
    return lax.rem(lax.axis_index("ep"), 2)


def dot_t(a, b):
    return lax.dot_general(a, b, (((1,), (1,)), ((), ())), preferred_element_type=F32)


def dot(a, b):
    return jnp.dot(a, b, preferred_element_type=F32)


def half_of(c, values):
    h = values.shape[-1] // 2
    return jnp.where(c == 0, values[:, :h], values[:, h:])


FAR = 5


def offsets(nz):
    ring = [0, -FAR, FAR]
    near = [n + o for n in (-1, 1, -2, 2) for o in ring]
    return [o % nz for o in ring + near + [-8]]


def own_kernel(resid_hbm, gains_hbm, out_ref, gains_ref, resid, sems):
    copies = [pltpu.make_async_copy(resid_hbm, resid, sems.at[0]),
              pltpu.make_async_copy(gains_hbm, gains_ref, sems.at[1])]
    for copy in copies:
        copy.start()
    for copy in copies:
        copy.wait()
    out_ref[...] = rms(resid[...].astype(F32), gains_ref[0:1, :]).astype(BF16)


def norm_kernel(own_ref, other_ref, gains_ref, out_ref, rows):
    c = core()
    r = own_ref.shape[0]
    own = half_of(c, own_ref[...].astype(F32))
    other = half_of(c, rms(other_ref[...].astype(F32), gains_ref[0:1, :]))
    rows[:r] = jnp.where(c == 0, own, other)
    rows[r : 2 * r] = jnp.where(c == 0, other, own)
    out_ref[...] = rows[...].astype(BF16)


def relay_kernel(x_ref, after_ref, out_ref):
    out_ref[...] = x_ref[...]


def stack_kernel(a_ref, b_ref, c_ref, after_ref, out_ref):
    out_ref[0] = a_ref[...]
    out_ref[1] = b_ref[...]
    out_ref[2] = c_ref[...]


def gates_kernel(
    normed_ref, wi_hbm, wf_hbm, bi_hbm, bf_hbm, max_hbm, routes_hbm, scores_hbm,
    wq_ref, wk_ref, wv_ref, wo_ref, state_ref, mix_ref,
    keep_ref, write_ref, newmax_ref, info_ref, weights_ref, state_out, mix_out,
    wi_ref, wf_ref, bi_ref, bf_ref, max_ref, routes_ref, scores_ref, turn_ref, info_scr, sems,
):
    heads, r = max_ref.shape
    cols = wq_ref.shape[0]
    small = [(wi_hbm, wi_ref), (wf_hbm, wf_ref), (max_hbm, max_ref), (routes_hbm, routes_ref),
             (scores_hbm, scores_ref), (bi_hbm, bi_ref), (bf_hbm, bf_ref)]
    small = [pltpu.make_async_copy(x, y, sems.at[k]) for k, (x, y) in enumerate(small)]
    copies = [
        pltpu.make_async_copy(w, weights_ref.at[pl.ds(k * cols, cols)], sems.at[7 + k])
        for k, w in enumerate((wq_ref, wk_ref, wv_ref, wo_ref))]
    copies.append(pltpu.make_async_copy(mix_ref, mix_out, sems.at[11]))
    for k in range(state_ref.shape[0]):
        copies.append(pltpu.make_async_copy(state_ref.at[k], state_out.at[k], sems.at[12 + k]))
    for copy in small + copies:
        copy.start()
    for copy in small:
        copy.wait()
    diagonal = lax.broadcasted_iota(jnp.int32, (heads, heads), 0) == lax.broadcasted_iota(
        jnp.int32, (heads, heads), 1)

    def column(bias):
        return jnp.sum(jnp.where(diagonal, bias, 0.0), axis=1, keepdims=True)

    normed = normed_ref[...]
    ipre = dot_t(wi_ref[...], normed) + column(bi_ref[...])
    fpre = dot_t(wf_ref[...], normed) + column(bf_ref[...])
    logf = jnp.minimum(fpre, 0.0) - jnp.log1p(jnp.exp(-jnp.abs(fpre)))
    decayed = logf + max_ref[...]
    new_max = jnp.maximum(ipre, decayed)
    newmax_ref[...] = new_max
    turn_ref[...] = jnp.zeros_like(turn_ref)
    turn_ref[0:heads, :r] = jnp.exp(decayed - new_max)
    keep_ref[...] = turn_ref[...].T[:r, :heads]
    turn_ref[0:heads, :r] = jnp.exp(ipre - new_max)
    write_ref[...] = turn_ref[...].T[:r, :heads]
    info_scr[...] = jnp.zeros_like(info_scr)
    info_scr[0:2, :r] = routes_ref[...].astype(F32)
    info_scr[2:4, :r] = scores_ref[...].astype(F32)
    info_ref[...] = info_scr[...].astype(BF16)
    for copy in copies:
        copy.wait()


def collect(refs, out):
    at = 0
    for ref in refs:
        size = 1
        for extent in ref.shape[:-1]:
            size *= extent
        out[at : at + size] = ref[...].reshape(size, ref.shape[-1])
        at += size


def proj_kernel(*refs):
    xs, ys, (w_ref, info_ref, out_ref, x, y) = refs[:6], refs[6:12], refs[12:]
    c = core()
    z = lax.div(lax.axis_index("ep"), 2)
    nz = out_ref.shape[0]
    h = x.shape[1]
    r2 = x.shape[0] // nz
    collect(xs, x)
    collect(ys, y)
    at = pl.ds(pl.multiple_of(c * h, h), h)
    to = pl.ds(pl.multiple_of((1 - c) * h, h), h)
    p = (dot_t(x[...], w_ref[:, at]) + dot_t(y[...], w_ref[:, to])).astype(BF16)
    for k, offset in enumerate(offsets(nz)):
        where = lax.rem(z + offset, nz)
        out_ref[where, :r2, :] = p[k * r2 : (k + 1) * r2]
        out_ref[k, r2 : r2 + 8, :] = info_ref[...]


def cell_kernel(
    a_ref, b_ref, keep_ref, write_ref, m_ref, norm_ref, mix_ref, resid_ref, gains_ref,
    middle_ref, mine_ref, send_ref, newnorm_ref, keys_ref, wvt_ref,
    p0, p1, q_scr, wv_scr, gated,
):
    c = core()
    r, heads, dh = norm_ref.shape
    nz = a_ref.shape[0]
    cols = heads * dh // (2 * nz)
    per = dh // cols
    p0[...] = jnp.zeros_like(p0)
    p1[...] = jnp.zeros_like(p1)
    for z in range(nz):
        a, b = a_ref[z].astype(F32), b_ref[z].astype(F32)
        a = jnp.where(c == 0, a[:r], a[r : 2 * r])
        b = jnp.where(c == 0, b[:r], b[r : 2 * r])
        p0[z, :r] = jnp.where(c == 0, a, b)
        p1[z, :r] = jnp.where(c == 0, b, a)
    lanes = lax.broadcasted_iota(jnp.int32, (16, dh), 1)

    def gather(h, kind):
        total = jnp.zeros((16, dh), F32)
        for p in range(per):
            ep = h * per + p
            piece = (p0 if ep % 2 == 0 else p1)[ep // 2]
            shift = ((p - kind) * cols) % dh
            piece = pltpu.roll(piece, shift, 1) if shift else piece
            total = jnp.where((lanes >= p * cols) & (lanes < (p + 1) * cols), piece, total)
        return total

    wv_scr[...] = jnp.zeros_like(wv_scr)
    for h in range(heads):
        q_scr[h] = gather(h, 0)
        keys_ref[h] = gather(h, 1) * dh ** (-0.5)
        wv_scr[h * 16 : h * 16 + r] = gather(h, 2)[:r] * write_ref[:, h : h + 1]
    wvt_ref[...] = wv_scr[...].T
    lane128 = lax.broadcasted_iota(jnp.int32, (dh, 128), 1)

    def step(s, acc):
        for h in range(heads):
            prod = m_ref[s, h] * q_scr[h, pl.ds(s, 1), :]
            red = jnp.sum(prod, axis=1, keepdims=True)
            acc = jnp.where(lane128 == h * 16 + s, red, acc)
        return acc

    numer = lax.fori_loop(0, r, step, jnp.zeros((dh, 128), F32)).T
    for h in range(heads):
        query, key = q_scr[h][:r], keys_ref[h][:r]
        outgate = gather(h, 3)[:r]
        keep, write = keep_ref[:, h : h + 1], write_ref[:, h : h + 1]
        new_norm = keep * norm_ref[:, h, :] + write * key
        newnorm_ref[:, h, :] = new_norm
        denom = jnp.sum(new_norm * query, axis=1, keepdims=True)
        kq = jnp.sum(key * query, axis=1, keepdims=True)
        top = keep * numer[h * 16 : h * 16 + r] + wv_scr[h * 16 : h * 16 + r] * kq
        cell = top / jnp.maximum(jnp.abs(denom), 1.0)
        gated[:, h * dh : (h + 1) * dh] = (jax.nn.sigmoid(outgate) * cell).astype(BF16)
    mixed = dot(gated[...], mix_ref[...])
    middle = resid_ref[...].astype(F32) + rms(mixed, gains_ref[1:2, :])
    middle_ref[...] = middle
    branch = rms(middle, gains_ref[2:3, :])
    mine_ref[...] = half_of(c, branch).astype(BF16)
    send_ref[...] = half_of(1 - c, branch).astype(BF16)


def update_kernel(keep_ref, keys_ref, wvt_ref, m_ref, out_ref, token_ref, new, sems):
    r, heads = m_ref.shape[:2]
    token_ref[...] = jnp.zeros_like(token_ref)

    def put(s):
        return pltpu.make_async_copy(new.at[s], out_ref.at[s], sems.at[s])

    def step(s, carry):
        rolled = pltpu.roll(wvt_ref[...], lax.rem(128 - s, 128), 1)
        for h in range(heads):
            keep = keep_ref[pl.ds(s, 1), h : h + 1]
            key = keys_ref[h, pl.ds(s, 1), :]
            new[s, h] = keep * m_ref[s, h] + rolled[:, h * 16 : h * 16 + 1] * key
        put(s).start()
        return carry

    lax.fori_loop(0, r, step, 0)
    for s in range(r):
        put(s).wait()


def pair_kernel(mine_ref, got_ref, out_ref, rows):
    c = core()
    r = mine_ref.shape[0]
    mine, got = mine_ref[...].astype(F32), got_ref[...].astype(F32)
    rows[:r] = jnp.where(c == 0, mine, got)
    rows[r : 2 * r] = jnp.where(c == 0, got, mine)
    out_ref[...] = rows[...].astype(BF16)


def silu_mul(gate, up):
    return (gate * jax.nn.sigmoid(gate) * up).astype(BF16)


def branch_kernel(*refs):
    xs, ys = refs[:6], refs[6:12]
    (a_ref, b_ref, eg_ref, eu_ref, ed_ref, dg_ref, du_ref, dd_ref, bw_ref,
     keep_ref, send_ref, table, made, x_scr, y_scr) = refs[12:]
    c = core()
    me = lax.axis_index("ep").astype(F32)
    home = lax.div(lax.axis_index("ep"), 2)
    nz = a_ref.shape[0]
    rows, h = x_scr.shape
    r2 = rows // nz
    r = r2 // 2
    slots = 2 * nz * CAP
    at = pl.ds(pl.multiple_of(c * h, h), h)
    to = pl.ds(pl.multiple_of((1 - c) * h, h), h)
    collect(xs, x_scr)
    collect(ys, y_scr)
    x, y = x_scr[...], y_scr[...]
    low = lax.broadcasted_iota(jnp.int32, (r2, 128), 0) < r
    for k, offset in enumerate(offsets(nz)):
        z = lax.rem(home + offset, nz)
        a, b = a_ref[z, r2 : r2 + 8, :].astype(F32), b_ref[z, r2 : r2 + 8, :].astype(F32)
        first, second = jnp.where(c == 0, a, b), jnp.where(c == 0, b, a)
        for j in range(4):
            table[j, k * r2 : (k + 1) * r2] = jnp.where(low, first[j : j + 1], second[j : j + 1])
    lane = lax.broadcasted_iota(jnp.int32, (rows, 128), 1)
    token = lax.broadcasted_iota(jnp.int32, (rows, 128), 0)
    block = lax.div(token, r)
    inner = token - block * r

    def column(k):
        return jnp.sum(jnp.where(lane == inner, table[k], 0.0), axis=1, keepdims=True)

    e0, e1, s0, s1 = column(0), column(1), column(2), column(3)
    hit0, hit1 = e0 == me, e1 == me
    hit = jnp.where(hit0 | hit1, 1.0, 0.0)
    weight = jnp.where(hit0, s0, jnp.where(hit1, s1, 0.0)) / (s0 + s1)
    row_i = lax.broadcasted_iota(jnp.int32, (rows, rows), 0)
    col_i = lax.broadcasted_iota(jnp.int32, (rows, rows), 1)
    earlier = (col_i < row_i) & (lax.div(row_i, r) == lax.div(col_i, r))
    earlier = jnp.where(earlier, 1.0, 0.0).astype(BF16)
    rank = dot(earlier, jnp.broadcast_to(hit, (rows, 128)).astype(BF16))
    slot = block.astype(F32) * CAP + rank
    chosen = jnp.where((slot == lane.astype(F32)) & (hit > 0.5), 1.0, 0.0)
    picker = chosen.T[:slots].astype(BF16)
    placer = chosen[:, :slots].astype(BF16)
    px = dot(picker, x).astype(BF16)
    py = dot(picker, y).astype(BF16)
    gate = dot(px, eg_ref[0, at, :]) + dot(py, eg_ref[0, to, :])
    up = dot(px, eu_ref[0, at, :]) + dot(py, eu_ref[0, to, :])
    made[...] = dot(silu_mul(gate, up), ed_ref[0]).astype(BF16)

    gate = dot(x, dg_ref[at, :]) + dot(y, dg_ref[to, :])
    up = dot(x, du_ref[at, :]) + dot(y, du_ref[to, :])
    hidden = silu_mul(gate, up)
    logit = jnp.sum(x.astype(F32) * bw_ref[:, at].astype(F32), axis=1, keepdims=True)
    logit = logit + jnp.sum(y.astype(F32) * bw_ref[:, to].astype(F32), axis=1, keepdims=True)
    sig = jax.nn.sigmoid(logit)
    for where, ref in ((at, keep_ref), (to, send_ref)):
        part = dot(hidden, dd_ref[:, where]) * sig
        part = part + dot(placer, made[:, where]) * weight
        ref[...] = part.astype(ref.dtype)


NEAR = (1, -1, 2, -2)


def spread_kernel(keep_ref, got_ref, *out_refs):
    own_ref, near_refs, last_ref = out_refs[0], out_refs[1:-1], out_refs[-1]
    nz = keep_ref.shape[0]
    order = offsets(nz)

    def term(offset):
        at = order.index(offset % nz)
        return keep_ref[at] + got_ref[at].astype(F32)

    for i, far in enumerate((0, FAR, -FAR)):
        own_ref[i] = term(far)
        for near, ref in zip(NEAR, near_refs):
            ref[i] = term(near + far).astype(BF16)
    last_ref[...] = term(8).astype(BF16)


def fold_kernel(
    own_ref, a_ref, b_ref, c_ref, d_ref, last_ref, own_out, plus_ref, minus_ref,
):
    def total(i):
        t = own_ref[i] + a_ref[i].astype(F32) + b_ref[i].astype(F32)
        return t + c_ref[i].astype(F32) + d_ref[i].astype(F32)

    own_out[...] = total(0)
    plus_ref[...] = (total(1) + last_ref[...].astype(F32)).astype(BF16)
    minus_ref[...] = total(2).astype(BF16)


def sum_kernel(own_ref, a_ref, b_ref, mine_ref, send_ref):
    c = core()
    r = mine_ref.shape[0]
    total = own_ref[...] + a_ref[...].astype(F32) + b_ref[...].astype(F32)
    mine_ref[...] = jnp.where(c == 0, total[:r], total[r:])
    send_ref[...] = jnp.where(c == 0, total[r:], total[:r])


def final_kernel(mine_ref, got_ref, middle_ref, gains_ref, out_ref):
    c = core()
    h = mine_ref.shape[1]
    mine, got = mine_ref[...], got_ref[...]
    low, high = jnp.where(c == 0, mine, got), jnp.where(c == 0, got, mine)
    square = jnp.sum(low * low, axis=1, keepdims=True) + jnp.sum(high * high, axis=1, keepdims=True)
    scale = lax.rsqrt(square / (2 * h) + 1e-06)
    gains = gains_ref[3:4, :]
    out_ref[:, :h] = (middle_ref[:, :h] + low * scale * gains[:, :h]).astype(BF16)
    out_ref[:, h:] = (middle_ref[:, h:] + high * scale * gains[:, h:]).astype(BF16)


def local(
    resid, norm_gains, w_query, w_key, w_value, w_outgate, w_igate, w_fgate, igate_bias,
    fgate_bias, state_matrix, state_norm, state_max, w_mix_out, routes, route_scores,
    expert_gate, expert_up, expert_down, dense_gate, dense_up, dense_down, branch_weight,
):
    n = lax.axis_size("ep")
    nz = n // 2
    r, d = resid.shape
    h = d // 2
    heads, dh = state_matrix.shape[1:3]
    inner = heads * dh
    groups = [[2 * z + c for z in range(nz)] for c in range(2)]
    pairs = [(i, i ^ 1) for i in range(n)]

    def swap(x):
        return lax.ppermute(x, "ep", pairs)

    def exchange(x):
        return lax.all_to_all(x, "ep", 0, 0, axis_index_groups=groups)

    def shift(x, offset):
        return lax.ppermute(
            x, "ep", [(2 * z + c, 2 * ((z + offset) % nz) + c) for z in range(nz) for c in range(2)])

    tile = (2 * r, h)

    def gather(own, after):
        plus, minus = shift(own, FAR), shift(own, -FAR)
        ring, = call(stack_kernel, [((3,) + tile, BF16)], (own, plus, minus, after), name="stack")
        last = shift(plus, 8 - FAR)
        up, down = shift(ring, 1), shift(ring, -1)
        relay, = call(relay_kernel, [((3,) + tile, BF16)], (up, last), name="relay")
        pieces = (ring, up, down, shift(relay, 1), shift(down, -1), last)
        return pieces, [swap(piece) for piece in pieces]

    other = swap(resid)
    normed, gains = call(
        own_kernel, [((r, d), BF16), (norm_gains.shape, F32)], (resid, norm_gains),
        scratch=[((r, d), BF16)], hbm=(0, 1), sems=2, name="own")
    keep, write, new_max, info, w_all, state, mix = call(
        gates_kernel,
        [((r, heads), F32), ((r, heads), F32), ((heads, r), F32), ((8, 128), BF16),
         ((4 * inner // n, d), BF16), (state_matrix.shape, F32), (w_mix_out.shape, BF16)],
        (normed, w_igate.T, w_fgate.T, igate_bias.reshape(1, heads),
         fgate_bias.reshape(1, heads), state_max.T, routes.T, route_scores.T,
         w_query.T, w_key.T, w_value.T, w_outgate.T, state_matrix, w_mix_out),
        scratch=[((heads, d), BF16), ((heads, d), BF16), ((1, heads), F32), ((1, heads), F32),
                 ((heads, r), F32), ((2, r), jnp.int32),
                 ((2, r), BF16), ((128, 128), F32), ((8, 128), F32)],
        hbm=tuple(range(1, 14)), sems=12 + r, held=(4, 5, 6), name="gates")
    chunk, = call(norm_kernel, [(tile, BF16)], (normed, other, gains),
                  scratch=[(tile, F32)], name="norm")
    xs, ys = gather(chunk, info)
    projected, = call(
        proj_kernel, [((nz, 2 * r + 8, 4 * inner // n), BF16)],
        (*xs, *ys, w_all, info), scratch=[((n * r, h), BF16)] * 2, name="proj")
    a = exchange(projected)
    b = swap(a)
    middle, mine, send, new_norm, keys, wvt = call(
        cell_kernel,
        [((r, d), F32), ((r, h), BF16), ((r, h), BF16), ((r, heads, dh), F32),
         ((heads, 16, dh), F32), ((dh, 128), F32)],
        (a, b, keep, write, state, state_norm, mix, resid, gains),
        scratch=[((nz, 16, dh), F32), ((nz, 16, dh), F32), ((heads, 16, dh), F32),
                 ((128, dh), F32), ((r, inner), BF16)], name="cell")
    got = swap(send)
    chunk, = call(pair_kernel, [((2 * r, h), BF16)], (mine, got),
                  scratch=[((2 * r, h), F32)], name="pair")
    new_matrix, token = call(
        update_kernel, [(state_matrix.shape, F32), ((8, 128), F32)], (keep, keys, wvt, state),
        scratch=[(state_matrix.shape, F32)], sems=r, name="update",
        out_specs=[pl.BlockSpec(memory_space=pltpu.HBM), pl.BlockSpec(memory_space=pltpu.VMEM)])
    xs, ys = gather(chunk, token)
    part, send = call(
        branch_kernel, [((n * r, h), F32), ((n * r, h), BF16)],
        (*xs, *ys, a, b, expert_gate, expert_up, expert_down, dense_gate, dense_up, dense_down,
         branch_weight.reshape(1, d)),
        scratch=[((4, n * r, 128), F32), ((n * CAP, d), BF16), ((n * r, h), BF16),
                 ((n * r, h), BF16)], vmem=32, name="branch")
    got = swap(send)
    own, *near, last = call(
        spread_kernel, [((3,) + tile, F32)] + [((3,) + tile, BF16)] * 4 + [(tile, BF16)],
        (part.reshape((nz,) + tile), got.reshape((nz,) + tile)), name="spread")
    near = [shift(x, offset) for x, offset in zip(near, NEAR)]
    last = shift(last, 8 - FAR)
    own, plus, minus = call(fold_kernel, [(tile, F32), (tile, BF16), (tile, BF16)],
                            (own, *near, last), name="fold")
    plus, minus = shift(plus, FAR), shift(minus, -FAR)
    mine, send = call(sum_kernel, [((r, h), F32), ((r, h), F32)], (own, plus, minus), name="sum")
    got = swap(send)
    out, = call(final_kernel, [((r, d), BF16)], (mine, got, middle, gains), name="final")
    return (out, new_matrix, new_norm, new_max.T)


def solution(mesh):
    placed = (
        P(("grp", "ep"), None), P(), P(None, "ep"), P(None, "ep"), P(None, "ep"), P(None, "ep"),
        P(), P(), P(), P(), P(("grp", "ep"), None, None, None), P(("grp", "ep"), None, None),
        P(("grp", "ep"), None), P(), P(("grp", "ep"), None), P(("grp", "ep"), None),
        P("ep", None, None), P("ep", None, None), P("ep", None, None), P(None, "ep"),
        P(None, "ep"), P("ep", None), P(),
    )
    return jax.shard_map(
        local,
        mesh=mesh,
        in_specs=placed,
        out_specs=(
            P(("grp", "ep"), None),
            P(("grp", "ep"), None, None, None),
            P(("grp", "ep"), None, None),
            P(("grp", "ep"), None),
        ),
        check_vma=False,
    )
```

```python
import jax
import jax.numpy as jnp
from jax import lax
from jax.experimental import pallas as pl
from jax.experimental.pallas import tpu as pltpu
from jax.sharding import PartitionSpec as P


CAP = 2
INTERPRET = False
F32 = jnp.float32
BF16 = jnp.bfloat16


def in_hbm(x):
    return x if INTERPRET else pltpu.with_memory_space_constraint(x, pltpu.HBM)


def call(kernel, outs, args, scratch=(), vmem=16, flops=1000000, hbm=(), sems=0, held=(), **grid):
    if hbm:
        args = [in_hbm(x) if i in hbm else x for i, x in enumerate(args)]
        grid["in_specs"] = [
            pl.BlockSpec(memory_space=pltpu.HBM if i in hbm else pltpu.VMEM)
            for i in range(len(args))]
    result = pl.pallas_call(
        kernel,
        out_shape=[pltpu.VMEM(s, d) if i in held and not INTERPRET else jax.ShapeDtypeStruct(s, d)
                   for i, (s, d) in enumerate(outs)],
        scratch_shapes=[pltpu.VMEM(s, d) for s, d in scratch]
        + ([pltpu.SemaphoreType.DMA((sems,))] if sems else []),
        **grid,
        compiler_params=pltpu.CompilerParams(vmem_limit_bytes=vmem << 20),
        cost_estimate=pl.CostEstimate(flops=flops, bytes_accessed=1000000, transcendentals=0),
        interpret=INTERPRET,
    )(*args)
    return result


def rms(values, gains):
    return values * lax.rsqrt(jnp.mean(values * values, axis=-1, keepdims=True) + 1e-06) * gains


def core():
    return lax.rem(lax.axis_index("ep"), 2)


def dot_t(a, b):
    return lax.dot_general(a, b, (((1,), (1,)), ((), ())), preferred_element_type=F32)


def dot(a, b):
    return jnp.dot(a, b, preferred_element_type=F32)


def half_of(c, values):
    h = values.shape[-1] // 2
    return jnp.where(c == 0, values[:, :h], values[:, h:])


FAR = 5


def offsets(nz):
    ring = [0, -FAR, FAR]
    near = [n + o for n in (-1, 1, -2, 2) for o in ring]
    return [o % nz for o in ring + near + [-8]]


def own_kernel(resid_hbm, gains_hbm, out_ref, gains_ref, resid, sems):
    copies = [pltpu.make_async_copy(resid_hbm, resid, sems.at[0]),
              pltpu.make_async_copy(gains_hbm, gains_ref, sems.at[1])]
    for copy in copies:
        copy.start()
    for copy in copies:
        copy.wait()
    out_ref[...] = rms(resid[...].astype(F32), gains_ref[0:1, :]).astype(BF16)


def norm_kernel(own_ref, other_ref, gains_ref, out_ref, rows):
    c = core()
    r = own_ref.shape[0]
    own = half_of(c, own_ref[...].astype(F32))
    other = half_of(c, rms(other_ref[...].astype(F32), gains_ref[0:1, :]))
    rows[:r] = jnp.where(c == 0, own, other)
    rows[r : 2 * r] = jnp.where(c == 0, other, own)
    out_ref[...] = rows[...].astype(BF16)


def stack_kernel(a_ref, b_ref, c_ref, after_ref, out_ref):
    out_ref[0] = a_ref[...]
    out_ref[1] = b_ref[...]
    out_ref[2] = c_ref[...]


def gates_kernel(
    normed_ref, wi_hbm, wf_hbm, bi_hbm, bf_hbm, max_hbm, routes_hbm, scores_hbm,
    wq_ref, wk_ref, wv_ref, wo_ref, state_ref, mix_ref,
    keep_ref, write_ref, newmax_ref, info_ref, weights_ref, state_out, mix_out,
    wi_ref, wf_ref, bi_ref, bf_ref, max_ref, routes_ref, scores_ref, turn_ref, info_scr, sems,
):
    heads, r = max_ref.shape
    cols = wq_ref.shape[0]
    small = [(wi_hbm, wi_ref), (wf_hbm, wf_ref), (max_hbm, max_ref), (routes_hbm, routes_ref),
             (scores_hbm, scores_ref), (bi_hbm, bi_ref), (bf_hbm, bf_ref)]
    small = [pltpu.make_async_copy(x, y, sems.at[k]) for k, (x, y) in enumerate(small)]
    copies = [
        pltpu.make_async_copy(w, weights_ref.at[pl.ds(k * cols, cols)], sems.at[7 + k])
        for k, w in enumerate((wq_ref, wk_ref, wv_ref, wo_ref))]
    copies.append(pltpu.make_async_copy(mix_ref, mix_out, sems.at[11]))
    for k in range(state_ref.shape[0]):
        copies.append(pltpu.make_async_copy(state_ref.at[k], state_out.at[k], sems.at[12 + k]))
    for copy in small + copies:
        copy.start()
    for copy in small:
        copy.wait()
    diagonal = lax.broadcasted_iota(jnp.int32, (heads, heads), 0) == lax.broadcasted_iota(
        jnp.int32, (heads, heads), 1)

    def column(bias):
        return jnp.sum(jnp.where(diagonal, bias, 0.0), axis=1, keepdims=True)

    normed = normed_ref[...]
    ipre = dot_t(wi_ref[...], normed) + column(bi_ref[...])
    fpre = dot_t(wf_ref[...], normed) + column(bf_ref[...])
    logf = jnp.minimum(fpre, 0.0) - jnp.log1p(jnp.exp(-jnp.abs(fpre)))
    decayed = logf + max_ref[...]
    new_max = jnp.maximum(ipre, decayed)
    newmax_ref[...] = new_max
    turn_ref[...] = jnp.zeros_like(turn_ref)
    turn_ref[0:heads, :r] = jnp.exp(decayed - new_max)
    keep_ref[...] = turn_ref[...].T[:r, :heads]
    turn_ref[0:heads, :r] = jnp.exp(ipre - new_max)
    write_ref[...] = turn_ref[...].T[:r, :heads]
    info_scr[...] = jnp.zeros_like(info_scr)
    info_scr[0:2, :r] = routes_ref[...].astype(F32)
    info_scr[2:4, :r] = scores_ref[...].astype(F32)
    info_ref[...] = info_scr[...].astype(BF16)
    for copy in copies:
        copy.wait()


def collect(refs, out):
    at = 0
    for ref in refs:
        size = 1
        for extent in ref.shape[:-1]:
            size *= extent
        out[at : at + size] = ref[...].reshape(size, ref.shape[-1])
        at += size


def proj_kernel(*refs):
    xs, ys, (w_ref, info_ref, out_ref, x, y) = refs[:6], refs[6:12], refs[12:]
    c = core()
    z = lax.div(lax.axis_index("ep"), 2)
    nz = out_ref.shape[0]
    h = x.shape[1]
    r2 = x.shape[0] // nz
    collect(xs, x)
    collect(ys, y)
    at = pl.ds(pl.multiple_of(c * h, h), h)
    to = pl.ds(pl.multiple_of((1 - c) * h, h), h)
    p = (dot_t(x[...], w_ref[:, at]) + dot_t(y[...], w_ref[:, to])).astype(BF16)
    for k, offset in enumerate(offsets(nz)):
        where = lax.rem(z + offset, nz)
        out_ref[where, :r2, :] = p[k * r2 : (k + 1) * r2]
        out_ref[k, r2 : r2 + 8, :] = info_ref[...]


def cell_kernel(
    a_ref, b_ref, keep_ref, write_ref, m_ref, norm_ref, mix_ref, resid_ref, gains_ref,
    middle_ref, mine_ref, send_ref, newnorm_ref, keys_ref, wvt_ref,
    p0, p1, q_scr, wv_scr, gated,
):
    c = core()
    r, heads, dh = norm_ref.shape
    nz = a_ref.shape[0]
    cols = heads * dh // (2 * nz)
    per = dh // cols
    p0[...] = jnp.zeros_like(p0)
    p1[...] = jnp.zeros_like(p1)
    for z in range(nz):
        a, b = a_ref[z].astype(F32), b_ref[z].astype(F32)
        a = jnp.where(c == 0, a[:r], a[r : 2 * r])
        b = jnp.where(c == 0, b[:r], b[r : 2 * r])
        p0[z, :r] = jnp.where(c == 0, a, b)
        p1[z, :r] = jnp.where(c == 0, b, a)
    lanes = lax.broadcasted_iota(jnp.int32, (16, dh), 1)

    def gather(h, kind):
        total = jnp.zeros((16, dh), F32)
        for p in range(per):
            ep = h * per + p
            piece = (p0 if ep % 2 == 0 else p1)[ep // 2]
            shift = ((p - kind) * cols) % dh
            piece = pltpu.roll(piece, shift, 1) if shift else piece
            total = jnp.where((lanes >= p * cols) & (lanes < (p + 1) * cols), piece, total)
        return total

    wv_scr[...] = jnp.zeros_like(wv_scr)
    for h in range(heads):
        q_scr[h] = gather(h, 0)
        keys_ref[h] = gather(h, 1) * dh ** (-0.5)
        wv_scr[h * 16 : h * 16 + r] = gather(h, 2)[:r] * write_ref[:, h : h + 1]
    wvt_ref[...] = wv_scr[...].T
    lane128 = lax.broadcasted_iota(jnp.int32, (dh, 128), 1)

    def step(s, acc):
        for h in range(heads):
            prod = m_ref[s, h] * q_scr[h, pl.ds(s, 1), :]
            red = jnp.sum(prod, axis=1, keepdims=True)
            acc = jnp.where(lane128 == h * 16 + s, red, acc)
        return acc

    numer = lax.fori_loop(0, r, step, jnp.zeros((dh, 128), F32)).T
    for h in range(heads):
        query, key = q_scr[h][:r], keys_ref[h][:r]
        outgate = gather(h, 3)[:r]
        keep, write = keep_ref[:, h : h + 1], write_ref[:, h : h + 1]
        new_norm = keep * norm_ref[:, h, :] + write * key
        newnorm_ref[:, h, :] = new_norm
        denom = jnp.sum(new_norm * query, axis=1, keepdims=True)
        kq = jnp.sum(key * query, axis=1, keepdims=True)
        top = keep * numer[h * 16 : h * 16 + r] + wv_scr[h * 16 : h * 16 + r] * kq
        cell = top / jnp.maximum(jnp.abs(denom), 1.0)
        gated[:, h * dh : (h + 1) * dh] = (jax.nn.sigmoid(outgate) * cell).astype(BF16)
    mixed = dot(gated[...], mix_ref[...])
    middle = resid_ref[...].astype(F32) + rms(mixed, gains_ref[1:2, :])
    middle_ref[...] = middle
    branch = rms(middle, gains_ref[2:3, :])
    mine_ref[...] = half_of(c, branch).astype(BF16)
    send_ref[...] = half_of(1 - c, branch).astype(BF16)


def update_kernel(keep_ref, keys_ref, wvt_ref, m_ref, out_ref, token_ref, new, sems):
    r, heads = m_ref.shape[:2]
    token_ref[...] = jnp.zeros_like(token_ref)

    def put(s):
        return pltpu.make_async_copy(new.at[s], out_ref.at[s], sems.at[s])

    def step(s, carry):
        rolled = pltpu.roll(wvt_ref[...], lax.rem(128 - s, 128), 1)
        for h in range(heads):
            keep = keep_ref[pl.ds(s, 1), h : h + 1]
            key = keys_ref[h, pl.ds(s, 1), :]
            new[s, h] = keep * m_ref[s, h] + rolled[:, h * 16 : h * 16 + 1] * key
        put(s).start()
        return carry

    lax.fori_loop(0, r, step, 0)
    for s in range(r):
        put(s).wait()


def pair_kernel(mine_ref, got_ref, out_ref, rows):
    c = core()
    r = mine_ref.shape[0]
    mine, got = mine_ref[...].astype(F32), got_ref[...].astype(F32)
    rows[:r] = jnp.where(c == 0, mine, got)
    rows[r : 2 * r] = jnp.where(c == 0, got, mine)
    out_ref[...] = rows[...].astype(BF16)


def silu_mul(gate, up):
    return (gate * jax.nn.sigmoid(gate) * up).astype(BF16)


def branch_kernel(*refs):
    xs, ys = refs[:6], refs[6:12]
    (a_ref, b_ref, eg_ref, eu_ref, ed_ref, dg_ref, du_ref, dd_ref, bw_ref,
     send_ref, hidden_ref, made, placer_ref, gains_ref, table, x_scr, y_scr) = refs[12:]
    c = core()
    me = lax.axis_index("ep").astype(F32)
    home = lax.div(lax.axis_index("ep"), 2)
    nz = a_ref.shape[0]
    rows, h = x_scr.shape
    r2 = rows // nz
    r = r2 // 2
    slots = 2 * nz * CAP
    at = pl.ds(pl.multiple_of(c * h, h), h)
    to = pl.ds(pl.multiple_of((1 - c) * h, h), h)
    collect(xs, x_scr)
    collect(ys, y_scr)
    x, y = x_scr[...], y_scr[...]
    low = lax.broadcasted_iota(jnp.int32, (r2, 128), 0) < r
    for k, offset in enumerate(offsets(nz)):
        z = lax.rem(home + offset, nz)
        a, b = a_ref[z, r2 : r2 + 8, :].astype(F32), b_ref[z, r2 : r2 + 8, :].astype(F32)
        first, second = jnp.where(c == 0, a, b), jnp.where(c == 0, b, a)
        for j in range(4):
            table[j, k * r2 : (k + 1) * r2] = jnp.where(low, first[j : j + 1], second[j : j + 1])
    lane = lax.broadcasted_iota(jnp.int32, (rows, 128), 1)
    token = lax.broadcasted_iota(jnp.int32, (rows, 128), 0)
    block = lax.div(token, r)
    inner = token - block * r

    def column(k):
        return jnp.sum(jnp.where(lane == inner, table[k], 0.0), axis=1, keepdims=True)

    e0, e1, s0, s1 = column(0), column(1), column(2), column(3)
    hit0, hit1 = e0 == me, e1 == me
    hit = jnp.where(hit0 | hit1, 1.0, 0.0)
    weight = jnp.where(hit0, s0, jnp.where(hit1, s1, 0.0)) / (s0 + s1)
    row_i = lax.broadcasted_iota(jnp.int32, (rows, rows), 0)
    col_i = lax.broadcasted_iota(jnp.int32, (rows, rows), 1)
    earlier = (col_i < row_i) & (lax.div(row_i, r) == lax.div(col_i, r))
    earlier = jnp.where(earlier, 1.0, 0.0).astype(BF16)
    rank = dot(earlier, jnp.broadcast_to(hit, (rows, 128)).astype(BF16))
    slot = block.astype(F32) * CAP + rank
    chosen = jnp.where((slot == lane.astype(F32)) & (hit > 0.5), 1.0, 0.0)
    picker = chosen.T[:slots].astype(BF16)
    placer = chosen[:, :slots].astype(BF16)
    px = dot(picker, x).astype(BF16)
    py = dot(picker, y).astype(BF16)
    gate = dot(px, eg_ref[0, at, :]) + dot(py, eg_ref[0, to, :])
    up = dot(px, eu_ref[0, at, :]) + dot(py, eu_ref[0, to, :])
    made[...] = dot(silu_mul(gate, up), ed_ref[0]).astype(BF16)

    gate = dot(x, dg_ref[at, :]) + dot(y, dg_ref[to, :])
    up = dot(x, du_ref[at, :]) + dot(y, du_ref[to, :])
    hidden = silu_mul(gate, up)
    logit = jnp.sum(x.astype(F32) * bw_ref[:, at].astype(F32), axis=1, keepdims=True)
    logit = logit + jnp.sum(y.astype(F32) * bw_ref[:, to].astype(F32), axis=1, keepdims=True)
    sig = jax.nn.sigmoid(logit)
    hidden_ref[...] = hidden
    placer_ref[...] = placer
    gains_ref[...] = jnp.where(lane == 0, sig, weight)
    part = dot(hidden, dd_ref[:, to]) * sig
    send_ref[...] = (part + dot(placer, made[:, to]) * weight).astype(BF16)


def rest_kernel(hidden_ref, made_ref, placer_ref, gains_ref, dd_ref, keep_ref):
    c = core()
    h = keep_ref.shape[1]
    at = pl.ds(pl.multiple_of(c * h, h), h)
    part = dot(hidden_ref[...], dd_ref[:, at]) * gains_ref[:, 0:1]
    keep_ref[...] = part + dot(placer_ref[...], made_ref[:, at]) * gains_ref[:, 1:2]


def spread_kernel(keep_ref, got_ref, zero_ref, one_ref, back_ref, up_ref, down_ref, last_ref):
    nz = keep_ref.shape[0]
    order = offsets(nz)

    def term(offset):
        at = order.index(offset % nz)
        return keep_ref[at] + got_ref[at].astype(F32)

    for i, far in enumerate((0, FAR, -FAR)):
        zero_ref[i] = term(far)
        one_ref[i] = term(far + 1)
        back_ref[i] = term(far - 1)
        up_ref[i] = term(far + 2).astype(BF16)
        down_ref[i] = term(far - 2).astype(BF16)
    last_ref[...] = term(8).astype(BF16)


def relay_kernel(own_ref, got_ref, out_ref):
    out_ref[...] = (own_ref[...] + got_ref[...].astype(F32)).astype(BF16)


def fold_kernel(own_ref, a_ref, b_ref, last_ref, own_out, plus_ref, minus_ref):
    def total(i):
        return own_ref[i] + a_ref[i].astype(F32) + b_ref[i].astype(F32)

    own_out[...] = total(0)
    plus_ref[...] = (total(1) + last_ref[...].astype(F32)).astype(BF16)
    minus_ref[...] = total(2).astype(BF16)


def sum_kernel(own_ref, a_ref, b_ref, mine_ref, send_ref):
    c = core()
    r = mine_ref.shape[0]
    total = own_ref[...] + a_ref[...].astype(F32) + b_ref[...].astype(F32)
    mine_ref[...] = jnp.where(c == 0, total[:r], total[r:])
    send_ref[...] = jnp.where(c == 0, total[r:], total[:r])


def final_kernel(mine_ref, got_ref, middle_ref, gains_ref, out_ref):
    c = core()
    h = mine_ref.shape[1]
    mine, got = mine_ref[...], got_ref[...]
    low, high = jnp.where(c == 0, mine, got), jnp.where(c == 0, got, mine)
    square = jnp.sum(low * low, axis=1, keepdims=True) + jnp.sum(high * high, axis=1, keepdims=True)
    scale = lax.rsqrt(square / (2 * h) + 1e-06)
    gains = gains_ref[3:4, :]
    out_ref[:, :h] = (middle_ref[:, :h] + low * scale * gains[:, :h]).astype(BF16)
    out_ref[:, h:] = (middle_ref[:, h:] + high * scale * gains[:, h:]).astype(BF16)


def local(
    resid, norm_gains, w_query, w_key, w_value, w_outgate, w_igate, w_fgate, igate_bias,
    fgate_bias, state_matrix, state_norm, state_max, w_mix_out, routes, route_scores,
    expert_gate, expert_up, expert_down, dense_gate, dense_up, dense_down, branch_weight,
):
    n = lax.axis_size("ep")
    nz = n // 2
    r, d = resid.shape
    h = d // 2
    heads, dh = state_matrix.shape[1:3]
    inner = heads * dh
    groups = [[2 * z + c for z in range(nz)] for c in range(2)]
    pairs = [(i, i ^ 1) for i in range(n)]

    def swap(x):
        return lax.ppermute(x, "ep", pairs)

    def exchange(x):
        return lax.all_to_all(x, "ep", 0, 0, axis_index_groups=groups)

    def shift(x, offset):
        return lax.ppermute(
            x, "ep", [(2 * z + c, 2 * ((z + offset) % nz) + c) for z in range(nz) for c in range(2)])

    tile = (2 * r, h)

    def gather(own, after):
        plus, minus = shift(own, FAR), shift(own, -FAR)
        ring, = call(stack_kernel, [((3,) + tile, BF16)], (own, plus, minus, after))
        last = shift(plus, 8 - FAR)
        up, down = shift(ring, 1), shift(ring, -1)
        pieces = (ring, up, down, shift(up, 1), shift(down, -1), last)
        return pieces, [swap(piece) for piece in pieces]

    other = swap(resid)
    normed, gains = call(
        own_kernel, [((r, d), BF16), (norm_gains.shape, F32)], (resid, norm_gains),
        scratch=[((r, d), BF16)], hbm=(0, 1), sems=2)
    keep, write, new_max, info, w_all, state, mix = call(
        gates_kernel,
        [((r, heads), F32), ((r, heads), F32), ((heads, r), F32), ((8, 128), BF16),
         ((4 * inner // n, d), BF16), (state_matrix.shape, F32), (w_mix_out.shape, BF16)],
        (normed, w_igate.T, w_fgate.T, igate_bias.reshape(1, heads),
         fgate_bias.reshape(1, heads), state_max.T, routes.T, route_scores.T,
         w_query.T, w_key.T, w_value.T, w_outgate.T, state_matrix, w_mix_out),
        scratch=[((heads, d), BF16), ((heads, d), BF16), ((1, heads), F32), ((1, heads), F32),
                 ((heads, r), F32), ((2, r), jnp.int32),
                 ((2, r), BF16), ((128, 128), F32), ((8, 128), F32)],
        hbm=tuple(range(1, 14)), sems=12 + r, held=(4, 5, 6))
    chunk, = call(norm_kernel, [(tile, BF16)], (normed, other, gains),
                  scratch=[(tile, F32)])
    xs, ys = gather(chunk, info)
    projected, = call(
        proj_kernel, [((nz, 2 * r + 8, 4 * inner // n), BF16)],
        (*xs, *ys, w_all, info), scratch=[((n * r, h), BF16)] * 2)
    a = exchange(projected)
    b = swap(a)
    middle, mine, send, new_norm, keys, wvt = call(
        cell_kernel,
        [((r, d), F32), ((r, h), BF16), ((r, h), BF16), ((r, heads, dh), F32),
         ((heads, 16, dh), F32), ((dh, 128), F32)],
        (a, b, keep, write, state, state_norm, mix, resid, gains),
        scratch=[((nz, 16, dh), F32), ((nz, 16, dh), F32), ((heads, 16, dh), F32),
                 ((128, dh), F32), ((r, inner), BF16)])
    got = swap(send)
    chunk, = call(pair_kernel, [((2 * r, h), BF16)], (mine, got),
                  scratch=[((2 * r, h), F32)])
    new_matrix, token = call(
        update_kernel, [(state_matrix.shape, F32), ((8, 128), F32)], (keep, keys, wvt, state),
        scratch=[(state_matrix.shape, F32)], sems=r,
        out_specs=[pl.BlockSpec(memory_space=pltpu.HBM), pl.BlockSpec(memory_space=pltpu.VMEM)])
    xs, ys = gather(chunk, token)
    send, hidden, made, placer, scales = call(
        branch_kernel,
        [((n * r, h), BF16), ((n * r, dense_down.shape[0]), BF16), ((n * CAP, d), BF16),
         ((n * r, n * CAP), BF16), ((n * r, 128), F32)],
        (*xs, *ys, a, b, expert_gate, expert_up, expert_down, dense_gate, dense_up, dense_down,
         branch_weight.reshape(1, d)),
        scratch=[((4, n * r, 128), F32), ((n * r, h), BF16), ((n * r, h), BF16)], vmem=32)
    got = swap(send)
    part, = call(rest_kernel, [((n * r, h), F32)], (hidden, made, placer, scales, dense_down),
                 flops=400000000)
    three = (3,) + tile
    own, one, back, up, down, last = call(
        spread_kernel, [(three, F32)] * 3 + [(three, BF16)] * 2 + [(tile, BF16)],
        (part.reshape((nz,) + tile), got.reshape((nz,) + tile)))
    up, down = shift(up, 1), shift(down, -1)
    last = shift(last, 8 - FAR)
    up, = call(relay_kernel, [(three, BF16)], (one, up))
    down, = call(relay_kernel, [(three, BF16)], (back, down))
    up, down = shift(up, 1), shift(down, -1)
    own, plus, minus = call(fold_kernel, [(tile, F32), (tile, BF16), (tile, BF16)],
                            (own, up, down, last))
    plus, minus = shift(plus, FAR), shift(minus, -FAR)
    mine, send = call(sum_kernel, [((r, h), F32), ((r, h), F32)], (own, plus, minus))
    got = swap(send)
    out, = call(final_kernel, [((r, d), BF16)], (mine, got, middle, gains))
    return (out, new_matrix, new_norm, new_max.T)


def solution(mesh):
    placed = (
        P(("grp", "ep"), None), P(), P(None, "ep"), P(None, "ep"), P(None, "ep"), P(None, "ep"),
        P(), P(), P(), P(), P(("grp", "ep"), None, None, None), P(("grp", "ep"), None, None),
        P(("grp", "ep"), None), P(), P(("grp", "ep"), None), P(("grp", "ep"), None),
        P("ep", None, None), P("ep", None, None), P("ep", None, None), P(None, "ep"),
        P(None, "ep"), P("ep", None), P(),
    )
    return jax.shard_map(
        local,
        mesh=mesh,
        in_specs=placed,
        out_specs=(
            P(("grp", "ep"), None),
            P(("grp", "ep"), None, None, None),
            P(("grp", "ep"), None, None),
            P(("grp", "ep"), None),
        ),
        check_vma=False,
    )
```

```python
import jax
import jax.numpy as jnp
from jax import lax
from jax.experimental import pallas as pl
from jax.experimental.pallas import tpu as pltpu
from jax.sharding import PartitionSpec as P


CAP = 2
INTERPRET = False
F32 = jnp.float32
BF16 = jnp.bfloat16


def in_hbm(x):
    return x if INTERPRET else pltpu.with_memory_space_constraint(x, pltpu.HBM)


def call(kernel, outs, args, scratch=(), vmem=16, flops=1000000, hbm=(), sems=0, held=(), **grid):
    if hbm:
        args = [in_hbm(x) if i in hbm else x for i, x in enumerate(args)]
        grid["in_specs"] = [
            pl.BlockSpec(memory_space=pltpu.HBM if i in hbm else pltpu.VMEM)
            for i in range(len(args))]
    result = pl.pallas_call(
        kernel,
        out_shape=[pltpu.VMEM(s, d) if i in held and not INTERPRET else jax.ShapeDtypeStruct(s, d)
                   for i, (s, d) in enumerate(outs)],
        scratch_shapes=[pltpu.VMEM(s, d) for s, d in scratch]
        + ([pltpu.SemaphoreType.DMA((sems,))] if sems else []),
        **grid,
        compiler_params=pltpu.CompilerParams(vmem_limit_bytes=vmem << 20),
        cost_estimate=pl.CostEstimate(flops=flops, bytes_accessed=1000000, transcendentals=0),
        interpret=INTERPRET,
    )(*args)
    return result


def rms(values, gains):
    return values * lax.rsqrt(jnp.mean(values * values, axis=-1, keepdims=True) + 1e-06) * gains


def core():
    return lax.rem(lax.axis_index("ep"), 2)


def dot_t(a, b):
    return lax.dot_general(a, b, (((1,), (1,)), ((), ())), preferred_element_type=F32)


def dot(a, b):
    return jnp.dot(a, b, preferred_element_type=F32)


def half_of(c, values):
    h = values.shape[-1] // 2
    return jnp.where(c == 0, values[:, :h], values[:, h:])


FAR = 5


def offsets(nz):
    ring = [0, -FAR, FAR]
    near = [n + o for n in (-1, 1, -2, 2) for o in ring]
    return [o % nz for o in ring + near + [-8]]


def own_kernel(resid_hbm, gains_hbm, out_ref, gains_ref, resid, sems):
    copies = [pltpu.make_async_copy(resid_hbm, resid, sems.at[0]),
              pltpu.make_async_copy(gains_hbm, gains_ref, sems.at[1])]
    for copy in copies:
        copy.start()
    for copy in copies:
        copy.wait()
    out_ref[...] = rms(resid[...].astype(F32), gains_ref[0:1, :]).astype(BF16)


def norm_kernel(own_ref, other_ref, gains_ref, out_ref, rows):
    c = core()
    r = own_ref.shape[0]
    own = half_of(c, own_ref[...].astype(F32))
    other = half_of(c, rms(other_ref[...].astype(F32), gains_ref[0:1, :]))
    rows[:r] = jnp.where(c == 0, own, other)
    rows[r : 2 * r] = jnp.where(c == 0, other, own)
    out_ref[...] = rows[...].astype(BF16)


def stack_kernel(a_ref, b_ref, c_ref, after_ref, out_ref):
    out_ref[0] = a_ref[...]
    out_ref[1] = b_ref[...]
    out_ref[2] = c_ref[...]


def gates_kernel(
    normed_ref, wi_hbm, wf_hbm, bi_hbm, bf_hbm, max_hbm, routes_hbm, scores_hbm,
    wq_ref, wk_ref, wv_ref, wo_ref, state_ref, mix_ref,
    keep_ref, write_ref, newmax_ref, info_ref, weights_ref, state_out, mix_out,
    wi_ref, wf_ref, bi_ref, bf_ref, max_ref, routes_ref, scores_ref, turn_ref, info_scr, sems,
):
    heads, r = max_ref.shape
    cols = wq_ref.shape[0]
    small = [(wi_hbm, wi_ref), (wf_hbm, wf_ref), (max_hbm, max_ref), (routes_hbm, routes_ref),
             (scores_hbm, scores_ref), (bi_hbm, bi_ref), (bf_hbm, bf_ref)]
    small = [pltpu.make_async_copy(x, y, sems.at[k]) for k, (x, y) in enumerate(small)]
    copies = [
        pltpu.make_async_copy(w, weights_ref.at[pl.ds(k * cols, cols)], sems.at[7 + k])
        for k, w in enumerate((wq_ref, wk_ref, wv_ref, wo_ref))]
    copies.append(pltpu.make_async_copy(mix_ref, mix_out, sems.at[11]))
    for k in range(state_ref.shape[0]):
        copies.append(pltpu.make_async_copy(state_ref.at[k], state_out.at[k], sems.at[12 + k]))
    for copy in small + copies:
        copy.start()
    for copy in small:
        copy.wait()
    diagonal = lax.broadcasted_iota(jnp.int32, (heads, heads), 0) == lax.broadcasted_iota(
        jnp.int32, (heads, heads), 1)

    def column(bias):
        return jnp.sum(jnp.where(diagonal, bias, 0.0), axis=1, keepdims=True)

    normed = normed_ref[...]
    ipre = dot_t(wi_ref[...], normed) + column(bi_ref[...])
    fpre = dot_t(wf_ref[...], normed) + column(bf_ref[...])
    logf = jnp.minimum(fpre, 0.0) - jnp.log1p(jnp.exp(-jnp.abs(fpre)))
    decayed = logf + max_ref[...]
    new_max = jnp.maximum(ipre, decayed)
    newmax_ref[...] = new_max
    turn_ref[...] = jnp.zeros_like(turn_ref)
    turn_ref[0:heads, :r] = jnp.exp(decayed - new_max)
    keep_ref[...] = turn_ref[...].T[:r, :heads]
    turn_ref[0:heads, :r] = jnp.exp(ipre - new_max)
    write_ref[...] = turn_ref[...].T[:r, :heads]
    info_scr[...] = jnp.zeros_like(info_scr)
    info_scr[0:2, :r] = routes_ref[...].astype(F32)
    info_scr[2:4, :r] = scores_ref[...].astype(F32)
    info_ref[...] = info_scr[...].astype(BF16)
    for copy in copies:
        copy.wait()


def collect(refs, out):
    at = 0
    for ref in refs:
        size = 1
        for extent in ref.shape[:-1]:
            size *= extent
        out[at : at + size] = ref[...].reshape(size, ref.shape[-1])
        at += size


def proj_kernel(*refs):
    xs, ys, (w_ref, info_ref, out_ref, x, y) = refs[:6], refs[6:12], refs[12:]
    c = core()
    z = lax.div(lax.axis_index("ep"), 2)
    nz = out_ref.shape[0]
    h = x.shape[1]
    r2 = x.shape[0] // nz
    collect(xs, x)
    collect(ys, y)
    at = pl.ds(pl.multiple_of(c * h, h), h)
    to = pl.ds(pl.multiple_of((1 - c) * h, h), h)
    p = (dot_t(x[...], w_ref[:, at]) + dot_t(y[...], w_ref[:, to])).astype(BF16)
    for k, offset in enumerate(offsets(nz)):
        where = lax.rem(z + offset, nz)
        out_ref[where, :r2, :] = p[k * r2 : (k + 1) * r2]
        out_ref[k, r2 : r2 + 8, :] = info_ref[...]


def cell_kernel(
    a_ref, b_ref, keep_ref, write_ref, m_ref, norm_ref, mix_ref, resid_ref, gains_ref,
    middle_ref, mine_ref, send_ref, newnorm_ref, keys_ref, wvt_ref,
    p0, p1, q_scr, wv_scr, gated,
):
    c = core()
    r, heads, dh = norm_ref.shape
    nz = a_ref.shape[0]
    cols = heads * dh // (2 * nz)
    per = dh // cols
    p0[...] = jnp.zeros_like(p0)
    p1[...] = jnp.zeros_like(p1)
    for z in range(nz):
        a, b = a_ref[z].astype(F32), b_ref[z].astype(F32)
        a = jnp.where(c == 0, a[:r], a[r : 2 * r])
        b = jnp.where(c == 0, b[:r], b[r : 2 * r])
        p0[z, :r] = jnp.where(c == 0, a, b)
        p1[z, :r] = jnp.where(c == 0, b, a)
    lanes = lax.broadcasted_iota(jnp.int32, (16, dh), 1)

    def gather(h, kind):
        total = jnp.zeros((16, dh), F32)
        for p in range(per):
            ep = h * per + p
            piece = (p0 if ep % 2 == 0 else p1)[ep // 2]
            shift = ((p - kind) * cols) % dh
            piece = pltpu.roll(piece, shift, 1) if shift else piece
            total = jnp.where((lanes >= p * cols) & (lanes < (p + 1) * cols), piece, total)
        return total

    wv_scr[...] = jnp.zeros_like(wv_scr)
    for h in range(heads):
        q_scr[h] = gather(h, 0)
        keys_ref[h] = gather(h, 1) * dh ** (-0.5)
        wv_scr[h * 16 : h * 16 + r] = gather(h, 2)[:r] * write_ref[:, h : h + 1]
    wvt_ref[...] = wv_scr[...].T
    lane128 = lax.broadcasted_iota(jnp.int32, (dh, 128), 1)

    def step(s, acc):
        for h in range(heads):
            prod = m_ref[s, h] * q_scr[h, pl.ds(s, 1), :]
            red = jnp.sum(prod, axis=1, keepdims=True)
            acc = jnp.where(lane128 == h * 16 + s, red, acc)
        return acc

    numer = lax.fori_loop(0, r, step, jnp.zeros((dh, 128), F32)).T
    for h in range(heads):
        query, key = q_scr[h][:r], keys_ref[h][:r]
        outgate = gather(h, 3)[:r]
        keep, write = keep_ref[:, h : h + 1], write_ref[:, h : h + 1]
        new_norm = keep * norm_ref[:, h, :] + write * key
        newnorm_ref[:, h, :] = new_norm
        denom = jnp.sum(new_norm * query, axis=1, keepdims=True)
        kq = jnp.sum(key * query, axis=1, keepdims=True)
        top = keep * numer[h * 16 : h * 16 + r] + wv_scr[h * 16 : h * 16 + r] * kq
        cell = top / jnp.maximum(jnp.abs(denom), 1.0)
        gated[:, h * dh : (h + 1) * dh] = (jax.nn.sigmoid(outgate) * cell).astype(BF16)
    mixed = dot(gated[...], mix_ref[...])
    middle = resid_ref[...].astype(F32) + rms(mixed, gains_ref[1:2, :])
    middle_ref[...] = middle
    branch = rms(middle, gains_ref[2:3, :])
    mine_ref[...] = half_of(c, branch).astype(BF16)
    send_ref[...] = half_of(1 - c, branch).astype(BF16)


def update_kernel(keep_ref, keys_ref, wvt_ref, m_ref, out_ref, token_ref, new, sems):
    r, heads = m_ref.shape[:2]
    token_ref[...] = jnp.zeros_like(token_ref)

    def put(s):
        return pltpu.make_async_copy(new.at[s], out_ref.at[s], sems.at[s])

    def step(s, carry):
        rolled = pltpu.roll(wvt_ref[...], lax.rem(128 - s, 128), 1)
        for h in range(heads):
            keep = keep_ref[pl.ds(s, 1), h : h + 1]
            key = keys_ref[h, pl.ds(s, 1), :]
            new[s, h] = keep * m_ref[s, h] + rolled[:, h * 16 : h * 16 + 1] * key
        put(s).start()
        return carry

    lax.fori_loop(0, r, step, 0)
    for s in range(r):
        put(s).wait()


def pair_kernel(mine_ref, got_ref, out_ref, rows):
    c = core()
    r = mine_ref.shape[0]
    mine, got = mine_ref[...].astype(F32), got_ref[...].astype(F32)
    rows[:r] = jnp.where(c == 0, mine, got)
    rows[r : 2 * r] = jnp.where(c == 0, got, mine)
    out_ref[...] = rows[...].astype(BF16)


def silu_mul(gate, up):
    return (gate * jax.nn.sigmoid(gate) * up).astype(BF16)


def route_kernel(a_ref, b_ref, picker_ref, placer_ref, weight_ref, table):
    c = core()
    me = lax.axis_index("ep").astype(F32)
    home = lax.div(lax.axis_index("ep"), 2)
    nz = a_ref.shape[0]
    slots, rows = picker_ref.shape
    r2 = rows // nz
    r = r2 // 2
    low = lax.broadcasted_iota(jnp.int32, (r2, 128), 0) < r
    for k, offset in enumerate(offsets(nz)):
        z = lax.rem(home + offset, nz)
        a, b = a_ref[z, r2 : r2 + 8, :].astype(F32), b_ref[z, r2 : r2 + 8, :].astype(F32)
        first, second = jnp.where(c == 0, a, b), jnp.where(c == 0, b, a)
        for j in range(4):
            table[j, k * r2 : (k + 1) * r2] = jnp.where(low, first[j : j + 1], second[j : j + 1])
    lane = lax.broadcasted_iota(jnp.int32, (rows, 128), 1)
    token = lax.broadcasted_iota(jnp.int32, (rows, 128), 0)
    block = lax.div(token, r)
    inner = token - block * r

    def column(k):
        return jnp.sum(jnp.where(lane == inner, table[k], 0.0), axis=1, keepdims=True)

    e0, e1, s0, s1 = column(0), column(1), column(2), column(3)
    hit0, hit1 = e0 == me, e1 == me
    hit = jnp.where(hit0 | hit1, 1.0, 0.0)
    weight = jnp.where(hit0, s0, jnp.where(hit1, s1, 0.0)) / (s0 + s1)
    row_i = lax.broadcasted_iota(jnp.int32, (rows, rows), 0)
    col_i = lax.broadcasted_iota(jnp.int32, (rows, rows), 1)
    earlier = (col_i < row_i) & (lax.div(row_i, r) == lax.div(col_i, r))
    earlier = jnp.where(earlier, 1.0, 0.0).astype(BF16)
    rank = dot(earlier, jnp.broadcast_to(hit, (rows, 128)).astype(BF16))
    slot = block.astype(F32) * CAP + rank
    chosen = jnp.where((slot == lane.astype(F32)) & (hit > 0.5), 1.0, 0.0)
    picker_ref[...] = chosen.T[:slots].astype(BF16)
    placer_ref[...] = chosen[:, :slots].astype(BF16)
    weight_ref[...] = jnp.broadcast_to(weight, weight_ref.shape)


def branch_kernel(*refs):
    xs, ys = refs[:6], refs[6:12]
    (picker_ref, placer_ref, weight_ref, eg_ref, eu_ref, ed_ref, dg_ref, du_ref, dd_ref, bw_ref,
     send_ref, hidden_ref, made, gains_ref, x_scr, y_scr) = refs[12:]
    c = core()
    rows, h = x_scr.shape
    at = pl.ds(pl.multiple_of(c * h, h), h)
    to = pl.ds(pl.multiple_of((1 - c) * h, h), h)
    collect(xs, x_scr)
    collect(ys, y_scr)
    x, y = x_scr[...], y_scr[...]
    lane = lax.broadcasted_iota(jnp.int32, (rows, 128), 1)
    picker, weight = picker_ref[...], weight_ref[:, 0:1]
    px = dot(picker, x).astype(BF16)
    py = dot(picker, y).astype(BF16)
    gate = dot(px, eg_ref[0, at, :]) + dot(py, eg_ref[0, to, :])
    up = dot(px, eu_ref[0, at, :]) + dot(py, eu_ref[0, to, :])
    made[...] = dot(silu_mul(gate, up), ed_ref[0]).astype(BF16)

    gate = dot(x, dg_ref[at, :]) + dot(y, dg_ref[to, :])
    up = dot(x, du_ref[at, :]) + dot(y, du_ref[to, :])
    hidden = silu_mul(gate, up)
    logit = jnp.sum(x.astype(F32) * bw_ref[:, at].astype(F32), axis=1, keepdims=True)
    logit = logit + jnp.sum(y.astype(F32) * bw_ref[:, to].astype(F32), axis=1, keepdims=True)
    sig = jax.nn.sigmoid(logit)
    hidden_ref[...] = hidden
    gains_ref[...] = jnp.where(lane == 0, sig, weight)
    part = dot(hidden, dd_ref[:, to]) * sig
    send_ref[...] = (part + dot(placer_ref[...], made[:, to]) * weight).astype(BF16)


def rest_kernel(hidden_ref, made_ref, placer_ref, gains_ref, dd_ref, keep_ref):
    c = core()
    h = keep_ref.shape[1]
    at = pl.ds(pl.multiple_of(c * h, h), h)
    part = dot(hidden_ref[...], dd_ref[:, at]) * gains_ref[:, 0:1]
    keep_ref[...] = part + dot(placer_ref[...], made_ref[:, at]) * gains_ref[:, 1:2]


def spread_kernel(keep_ref, got_ref, zero_ref, one_ref, back_ref, up_ref, down_ref, last_ref):
    nz = keep_ref.shape[0]
    order = offsets(nz)

    def term(offset):
        at = order.index(offset % nz)
        return keep_ref[at] + got_ref[at].astype(F32)

    for i, far in enumerate((0, FAR, -FAR)):
        zero_ref[i] = term(far)
        one_ref[i] = term(far + 1)
        back_ref[i] = term(far - 1)
        up_ref[i] = term(far + 2).astype(BF16)
        down_ref[i] = term(far - 2).astype(BF16)
    last_ref[...] = term(8).astype(BF16)


def relay_kernel(own_ref, got_ref, out_ref):
    out_ref[...] = (own_ref[...] + got_ref[...].astype(F32)).astype(BF16)


def fold_kernel(own_ref, a_ref, b_ref, last_ref, own_out, plus_ref, minus_ref):
    def total(i):
        return own_ref[i] + a_ref[i].astype(F32) + b_ref[i].astype(F32)

    own_out[...] = total(0)
    plus_ref[...] = (total(1) + last_ref[...].astype(F32)).astype(BF16)
    minus_ref[...] = total(2).astype(BF16)


def sum_kernel(own_ref, a_ref, b_ref, mine_ref, send_ref):
    c = core()
    r = mine_ref.shape[0]
    total = own_ref[...] + a_ref[...].astype(F32) + b_ref[...].astype(F32)
    mine_ref[...] = jnp.where(c == 0, total[:r], total[r:])
    send_ref[...] = jnp.where(c == 0, total[r:], total[:r])


def final_kernel(mine_ref, got_ref, middle_ref, gains_ref, out_ref):
    c = core()
    h = mine_ref.shape[1]
    mine, got = mine_ref[...], got_ref[...]
    low, high = jnp.where(c == 0, mine, got), jnp.where(c == 0, got, mine)
    square = jnp.sum(low * low, axis=1, keepdims=True) + jnp.sum(high * high, axis=1, keepdims=True)
    scale = lax.rsqrt(square / (2 * h) + 1e-06)
    gains = gains_ref[3:4, :]
    out_ref[:, :h] = (middle_ref[:, :h] + low * scale * gains[:, :h]).astype(BF16)
    out_ref[:, h:] = (middle_ref[:, h:] + high * scale * gains[:, h:]).astype(BF16)


def local(
    resid, norm_gains, w_query, w_key, w_value, w_outgate, w_igate, w_fgate, igate_bias,
    fgate_bias, state_matrix, state_norm, state_max, w_mix_out, routes, route_scores,
    expert_gate, expert_up, expert_down, dense_gate, dense_up, dense_down, branch_weight,
):
    n = lax.axis_size("ep")
    nz = n // 2
    r, d = resid.shape
    h = d // 2
    heads, dh = state_matrix.shape[1:3]
    inner = heads * dh
    groups = [[2 * z + c for z in range(nz)] for c in range(2)]
    pairs = [(i, i ^ 1) for i in range(n)]

    def swap(x):
        return lax.ppermute(x, "ep", pairs)

    def exchange(x):
        return lax.all_to_all(x, "ep", 0, 0, axis_index_groups=groups)

    def shift(x, offset):
        return lax.ppermute(
            x, "ep", [(2 * z + c, 2 * ((z + offset) % nz) + c) for z in range(nz) for c in range(2)])

    tile = (2 * r, h)

    def gather(own, after):
        plus, minus = shift(own, FAR), shift(own, -FAR)
        ring, = call(stack_kernel, [((3,) + tile, BF16)], (own, plus, minus, after))
        last = shift(plus, 8 - FAR)
        up, down = shift(ring, 1), shift(ring, -1)
        pieces = (ring, up, down, shift(up, 1), shift(down, -1), last)
        return pieces, [swap(piece) for piece in pieces]

    other = swap(resid)
    normed, gains = call(
        own_kernel, [((r, d), BF16), (norm_gains.shape, F32)], (resid, norm_gains),
        scratch=[((r, d), BF16)], hbm=(0, 1), sems=2)
    keep, write, new_max, info, w_all, state, mix = call(
        gates_kernel,
        [((r, heads), F32), ((r, heads), F32), ((heads, r), F32), ((8, 128), BF16),
         ((4 * inner // n, d), BF16), (state_matrix.shape, F32), (w_mix_out.shape, BF16)],
        (normed, w_igate.T, w_fgate.T, igate_bias.reshape(1, heads),
         fgate_bias.reshape(1, heads), state_max.T, routes.T, route_scores.T,
         w_query.T, w_key.T, w_value.T, w_outgate.T, state_matrix, w_mix_out),
        scratch=[((heads, d), BF16), ((heads, d), BF16), ((1, heads), F32), ((1, heads), F32),
                 ((heads, r), F32), ((2, r), jnp.int32),
                 ((2, r), BF16), ((128, 128), F32), ((8, 128), F32)],
        hbm=tuple(range(1, 14)), sems=12 + r, held=(4, 5, 6))
    chunk, = call(norm_kernel, [(tile, BF16)], (normed, other, gains),
                  scratch=[(tile, F32)])
    xs, ys = gather(chunk, info)
    projected, = call(
        proj_kernel, [((nz, 2 * r + 8, 4 * inner // n), BF16)],
        (*xs, *ys, w_all, info), scratch=[((n * r, h), BF16)] * 2)
    a = exchange(projected)
    b = swap(a)
    middle, mine, send, new_norm, keys, wvt = call(
        cell_kernel,
        [((r, d), F32), ((r, h), BF16), ((r, h), BF16), ((r, heads, dh), F32),
         ((heads, 16, dh), F32), ((dh, 128), F32)],
        (a, b, keep, write, state, state_norm, mix, resid, gains),
        scratch=[((nz, 16, dh), F32), ((nz, 16, dh), F32), ((heads, 16, dh), F32),
                 ((128, dh), F32), ((r, inner), BF16)])
    got = swap(send)
    chunk, = call(pair_kernel, [((2 * r, h), BF16)], (mine, got),
                  scratch=[((2 * r, h), F32)])
    new_matrix, token = call(
        update_kernel, [(state_matrix.shape, F32), ((8, 128), F32)], (keep, keys, wvt, state),
        scratch=[(state_matrix.shape, F32)], sems=r,
        out_specs=[pl.BlockSpec(memory_space=pltpu.HBM), pl.BlockSpec(memory_space=pltpu.VMEM)])
    xs, ys = gather(chunk, token)
    picker, placer, weight = call(
        route_kernel,
        [((n * CAP, n * r), BF16), ((n * r, n * CAP), BF16), ((n * r, 128), F32)],
        (a, b), scratch=[((4, n * r, 128), F32)])
    send, hidden, made, scales = call(
        branch_kernel,
        [((n * r, h), BF16), ((n * r, dense_down.shape[0]), BF16), ((n * CAP, d), BF16),
         ((n * r, 128), F32)],
        (*xs, *ys, picker, placer, weight, expert_gate, expert_up, expert_down, dense_gate,
         dense_up, dense_down, branch_weight.reshape(1, d)),
        scratch=[((n * r, h), BF16), ((n * r, h), BF16)], vmem=32)
    got = swap(send)
    part, = call(rest_kernel, [((n * r, h), F32)], (hidden, made, placer, scales, dense_down),
                 flops=400000000)
    three = (3,) + tile
    own, one, back, up, down, last = call(
        spread_kernel, [(three, F32)] * 3 + [(three, BF16)] * 2 + [(tile, BF16)],
        (part.reshape((nz,) + tile), got.reshape((nz,) + tile)))
    last = shift(last, 8 - FAR)
    up, down = shift(up, 1), shift(down, -1)
    up, = call(relay_kernel, [(three, BF16)], (one, up))
    down, = call(relay_kernel, [(three, BF16)], (back, down))
    up, down = shift(up, 1), shift(down, -1)
    own, plus, minus = call(fold_kernel, [(tile, F32), (tile, BF16), (tile, BF16)],
                            (own, up, down, last))
    plus, minus = shift(plus, FAR), shift(minus, -FAR)
    mine, send = call(sum_kernel, [((r, h), F32), ((r, h), F32)], (own, plus, minus))
    got = swap(send)
    out, = call(final_kernel, [((r, d), BF16)], (mine, got, middle, gains))
    return (out, new_matrix, new_norm, new_max.T)


def solution(mesh):
    placed = (
        P(("grp", "ep"), None), P(), P(None, "ep"), P(None, "ep"), P(None, "ep"), P(None, "ep"),
        P(), P(), P(), P(), P(("grp", "ep"), None, None, None), P(("grp", "ep"), None, None),
        P(("grp", "ep"), None), P(), P(("grp", "ep"), None), P(("grp", "ep"), None),
        P("ep", None, None), P("ep", None, None), P("ep", None, None), P(None, "ep"),
        P(None, "ep"), P("ep", None), P(),
    )
    return jax.shard_map(
        local,
        mesh=mesh,
        in_specs=placed,
        out_specs=(
            P(("grp", "ep"), None),
            P(("grp", "ep"), None, None, None),
            P(("grp", "ep"), None, None),
            P(("grp", "ep"), None),
        ),
        check_vma=False,
    )
```

```python
import jax
import jax.numpy as jnp
from jax import lax
from jax.experimental import pallas as pl
from jax.experimental.pallas import tpu as pltpu
from jax.sharding import PartitionSpec as P


CAP = 2
INTERPRET = False
F32 = jnp.float32
BF16 = jnp.bfloat16


def in_hbm(x):
    return x if INTERPRET else pltpu.with_memory_space_constraint(x, pltpu.HBM)


def call(kernel, outs, args, scratch=(), vmem=16, flops=1000000, hbm=(), sems=0, held=(), **grid):
    if hbm:
        args = [in_hbm(x) if i in hbm else x for i, x in enumerate(args)]
        grid["in_specs"] = [
            pl.BlockSpec(memory_space=pltpu.HBM if i in hbm else pltpu.VMEM)
            for i in range(len(args))]
    result = pl.pallas_call(
        kernel,
        out_shape=[pltpu.VMEM(s, d) if i in held and not INTERPRET else jax.ShapeDtypeStruct(s, d)
                   for i, (s, d) in enumerate(outs)],
        scratch_shapes=[pltpu.VMEM(s, d) for s, d in scratch]
        + ([pltpu.SemaphoreType.DMA((sems,))] if sems else []),
        **grid,
        compiler_params=pltpu.CompilerParams(vmem_limit_bytes=vmem << 20),
        cost_estimate=pl.CostEstimate(flops=flops, bytes_accessed=1000000, transcendentals=0),
        interpret=INTERPRET,
    )(*args)
    return result


def rms(values, gains):
    return values * lax.rsqrt(jnp.mean(values * values, axis=-1, keepdims=True) + 1e-06) * gains


def core():
    return lax.rem(lax.axis_index("ep"), 2)


def dot_t(a, b):
    return lax.dot_general(a, b, (((1,), (1,)), ((), ())), preferred_element_type=F32)


def dot(a, b):
    return jnp.dot(a, b, preferred_element_type=F32)


def half_of(c, values):
    h = values.shape[-1] // 2
    return jnp.where(c == 0, values[:, :h], values[:, h:])


FAR = 5


def offsets(nz):
    ring = [0, -FAR, FAR]
    near = [n + o for n in (-1, 1, -2, 2) for o in ring]
    return [o % nz for o in ring + near + [-8]]


def own_kernel(resid_hbm, gains_hbm, out_ref, gains_ref, resid, sems):
    copies = [pltpu.make_async_copy(resid_hbm, resid, sems.at[0]),
              pltpu.make_async_copy(gains_hbm, gains_ref, sems.at[1])]
    for copy in copies:
        copy.start()
    for copy in copies:
        copy.wait()
    out_ref[...] = rms(resid[...].astype(F32), gains_ref[0:1, :]).astype(BF16)


def norm_kernel(own_ref, other_ref, gains_ref, out_ref, rows):
    c = core()
    r = own_ref.shape[0]
    own = own_ref[...].astype(F32)
    other = rms(other_ref[...].astype(F32), gains_ref[0:1, :])
    rows[:r] = jnp.where(c == 0, own, other)
    rows[r : 2 * r] = jnp.where(c == 0, other, own)
    out_ref[...] = rows[...].astype(BF16)


def stack_kernel(own_ref, far_ref, other_ref, after_ref, out_ref, half_ref):
    c = core()
    far, other = far_ref[...].astype(F32), other_ref[...].astype(F32)
    minus = jnp.where(c == 0, far, other)
    out_ref[0] = own_ref[...]
    out_ref[1] = minus.astype(BF16)
    out_ref[2] = jnp.where(c == 0, other, far).astype(BF16)
    half_ref[...] = half_of(c, minus).astype(BF16)


def gates_kernel(
    normed_ref, wi_hbm, wf_hbm, bi_hbm, bf_hbm, max_hbm, routes_hbm, scores_hbm,
    wq_ref, wk_ref, wv_ref, wo_ref, state_ref, mix_ref,
    keep_ref, write_ref, newmax_ref, info_ref, weights_ref, state_out, mix_out,
    wi_ref, wf_ref, bi_ref, bf_ref, max_ref, routes_ref, scores_ref, turn_ref, info_scr, sems,
):
    heads, r = max_ref.shape
    cols = wq_ref.shape[0]
    small = [(wi_hbm, wi_ref), (wf_hbm, wf_ref), (max_hbm, max_ref), (routes_hbm, routes_ref),
             (scores_hbm, scores_ref), (bi_hbm, bi_ref), (bf_hbm, bf_ref)]
    small = [pltpu.make_async_copy(x, y, sems.at[k]) for k, (x, y) in enumerate(small)]
    copies = [
        pltpu.make_async_copy(w, weights_ref.at[pl.ds(k * cols, cols)], sems.at[7 + k])
        for k, w in enumerate((wq_ref, wk_ref, wv_ref, wo_ref))]
    copies.append(pltpu.make_async_copy(mix_ref, mix_out, sems.at[11]))
    for k in range(state_ref.shape[0]):
        copies.append(pltpu.make_async_copy(state_ref.at[k], state_out.at[k], sems.at[12 + k]))
    for copy in small + copies:
        copy.start()
    for copy in small:
        copy.wait()
    diagonal = lax.broadcasted_iota(jnp.int32, (heads, heads), 0) == lax.broadcasted_iota(
        jnp.int32, (heads, heads), 1)

    def column(bias):
        return jnp.sum(jnp.where(diagonal, bias, 0.0), axis=1, keepdims=True)

    normed = normed_ref[...]
    ipre = dot_t(wi_ref[...], normed) + column(bi_ref[...])
    fpre = dot_t(wf_ref[...], normed) + column(bf_ref[...])
    logf = jnp.minimum(fpre, 0.0) - jnp.log1p(jnp.exp(-jnp.abs(fpre)))
    decayed = logf + max_ref[...]
    new_max = jnp.maximum(ipre, decayed)
    newmax_ref[...] = new_max
    turn_ref[...] = jnp.zeros_like(turn_ref)
    turn_ref[0:heads, :r] = jnp.exp(decayed - new_max)
    keep_ref[...] = turn_ref[...].T[:r, :heads]
    turn_ref[0:heads, :r] = jnp.exp(ipre - new_max)
    write_ref[...] = turn_ref[...].T[:r, :heads]
    info_scr[...] = jnp.zeros_like(info_scr)
    info_scr[0:2, :r] = routes_ref[...].astype(F32)
    info_scr[2:4, :r] = scores_ref[...].astype(F32)
    info_ref[...] = info_scr[...].astype(BF16)
    for copy in copies:
        copy.wait()


def collect(refs, out):
    ring_ref, one_ref, one_swap, two_ref, two_swap, last_ref, last_swap = refs
    c = core()
    h = last_ref.shape[1]
    out[0:3] = ring_ref[...]
    out[pl.ds(3 + 3 * c, 3)] = one_ref[...]
    out[pl.ds(6 - 3 * c, 3)] = one_swap[...]
    out[pl.ds(9 + 3 * c, 3)] = two_ref[...]
    out[pl.ds(12 - 3 * c, 3)] = two_swap[...]
    mine, got = last_ref[...].astype(F32), last_swap[...].astype(F32)
    out[15, :, :h] = jnp.where(c == 0, mine, got).astype(BF16)
    out[15, :, h:] = jnp.where(c == 0, got, mine).astype(BF16)


def proj_kernel(*refs):
    pieces, (w_ref, info_ref, out_ref, x) = refs[:7], refs[7:]
    z = lax.div(lax.axis_index("ep"), 2)
    nz, r2, d = x.shape
    collect(pieces, x)
    p = dot_t(x[...].reshape(nz * r2, d), w_ref[...]).astype(BF16)
    for k, offset in enumerate(offsets(nz)):
        where = lax.rem(z + offset, nz)
        out_ref[where, :r2, :] = p[k * r2 : (k + 1) * r2]
        out_ref[k, r2 : r2 + 8, :] = info_ref[...]


def cell_kernel(
    a_ref, b_ref, keep_ref, write_ref, m_ref, norm_ref, mix_ref, resid_ref, gains_ref,
    middle_ref, rows_ref, newnorm_ref, keys_ref, wvt_ref,
    p0, p1, q_scr, wv_scr, gated,
):
    c = core()
    r, heads, dh = norm_ref.shape
    nz = a_ref.shape[0]
    cols = heads * dh // (2 * nz)
    per = dh // cols
    p0[...] = jnp.zeros_like(p0)
    p1[...] = jnp.zeros_like(p1)
    for z in range(nz):
        a, b = a_ref[z].astype(F32), b_ref[z].astype(F32)
        a = jnp.where(c == 0, a[:r], a[r : 2 * r])
        b = jnp.where(c == 0, b[:r], b[r : 2 * r])
        p0[z, :r] = jnp.where(c == 0, a, b)
        p1[z, :r] = jnp.where(c == 0, b, a)
    lanes = lax.broadcasted_iota(jnp.int32, (16, dh), 1)

    def gather(h, kind):
        total = jnp.zeros((16, dh), F32)
        for p in range(per):
            ep = h * per + p
            piece = (p0 if ep % 2 == 0 else p1)[ep // 2]
            shift = ((p - kind) * cols) % dh
            piece = pltpu.roll(piece, shift, 1) if shift else piece
            total = jnp.where((lanes >= p * cols) & (lanes < (p + 1) * cols), piece, total)
        return total

    wv_scr[...] = jnp.zeros_like(wv_scr)
    for h in range(heads):
        q_scr[h] = gather(h, 0)
        keys_ref[h] = gather(h, 1) * dh ** (-0.5)
        wv_scr[h * 16 : h * 16 + r] = gather(h, 2)[:r] * write_ref[:, h : h + 1]
    wvt_ref[...] = wv_scr[...].T
    lane128 = lax.broadcasted_iota(jnp.int32, (dh, 128), 1)

    def step(s, acc):
        for h in range(heads):
            prod = m_ref[s, h] * q_scr[h, pl.ds(s, 1), :]
            red = jnp.sum(prod, axis=1, keepdims=True)
            acc = jnp.where(lane128 == h * 16 + s, red, acc)
        return acc

    numer = lax.fori_loop(0, r, step, jnp.zeros((dh, 128), F32)).T
    for h in range(heads):
        query, key = q_scr[h][:r], keys_ref[h][:r]
        outgate = gather(h, 3)[:r]
        keep, write = keep_ref[:, h : h + 1], write_ref[:, h : h + 1]
        new_norm = keep * norm_ref[:, h, :] + write * key
        newnorm_ref[:, h, :] = new_norm
        denom = jnp.sum(new_norm * query, axis=1, keepdims=True)
        kq = jnp.sum(key * query, axis=1, keepdims=True)
        top = keep * numer[h * 16 : h * 16 + r] + wv_scr[h * 16 : h * 16 + r] * kq
        cell = top / jnp.maximum(jnp.abs(denom), 1.0)
        gated[:, h * dh : (h + 1) * dh] = (jax.nn.sigmoid(outgate) * cell).astype(BF16)
    mixed = dot(gated[...], mix_ref[...])
    middle = resid_ref[...].astype(F32) + rms(mixed, gains_ref[1:2, :])
    middle_ref[...] = middle
    rows_ref[...] = rms(middle, gains_ref[2:3, :]).astype(BF16)


def update_kernel(keep_ref, keys_ref, wvt_ref, m_ref, out_ref, token_ref, new, sems):
    r, heads = m_ref.shape[:2]
    token_ref[...] = jnp.zeros_like(token_ref)

    def put(s):
        return pltpu.make_async_copy(new.at[s], out_ref.at[s], sems.at[s])

    def step(s, carry):
        rolled = pltpu.roll(wvt_ref[...], lax.rem(128 - s, 128), 1)
        for h in range(heads):
            keep = keep_ref[pl.ds(s, 1), h : h + 1]
            key = keys_ref[h, pl.ds(s, 1), :]
            new[s, h] = keep * m_ref[s, h] + rolled[:, h * 16 : h * 16 + 1] * key
        put(s).start()
        return carry

    lax.fori_loop(0, r, step, 0)
    for s in range(r):
        put(s).wait()


def pair_kernel(mine_ref, got_ref, out_ref, rows):
    c = core()
    r = mine_ref.shape[0]
    mine, got = mine_ref[...].astype(F32), got_ref[...].astype(F32)
    rows[:r] = jnp.where(c == 0, mine, got)
    rows[r : 2 * r] = jnp.where(c == 0, got, mine)
    out_ref[...] = rows[...].astype(BF16)


def silu_mul(gate, up):
    return (gate * jax.nn.sigmoid(gate) * up).astype(BF16)


def route_kernel(a_ref, b_ref, picker_ref, placer_ref, weight_ref, table):
    c = core()
    me = lax.axis_index("ep").astype(F32)
    home = lax.div(lax.axis_index("ep"), 2)
    nz = a_ref.shape[0]
    slots, rows = picker_ref.shape
    r2 = rows // nz
    r = r2 // 2
    low = lax.broadcasted_iota(jnp.int32, (r2, 128), 0) < r
    for k, offset in enumerate(offsets(nz)):
        z = lax.rem(home + offset, nz)
        a, b = a_ref[z, r2 : r2 + 8, :].astype(F32), b_ref[z, r2 : r2 + 8, :].astype(F32)
        first, second = jnp.where(c == 0, a, b), jnp.where(c == 0, b, a)
        for j in range(4):
            table[j, k * r2 : (k + 1) * r2] = jnp.where(low, first[j : j + 1], second[j : j + 1])
    lane = lax.broadcasted_iota(jnp.int32, (rows, 128), 1)
    token = lax.broadcasted_iota(jnp.int32, (rows, 128), 0)
    block = lax.div(token, r)
    inner = token - block * r

    def column(k):
        return jnp.sum(jnp.where(lane == inner, table[k], 0.0), axis=1, keepdims=True)

    e0, e1, s0, s1 = column(0), column(1), column(2), column(3)
    hit0, hit1 = e0 == me, e1 == me
    hit = jnp.where(hit0 | hit1, 1.0, 0.0)
    weight = jnp.where(hit0, s0, jnp.where(hit1, s1, 0.0)) / (s0 + s1)
    row_i = lax.broadcasted_iota(jnp.int32, (rows, rows), 0)
    col_i = lax.broadcasted_iota(jnp.int32, (rows, rows), 1)
    earlier = (col_i < row_i) & (lax.div(row_i, r) == lax.div(col_i, r))
    earlier = jnp.where(earlier, 1.0, 0.0).astype(BF16)
    rank = dot(earlier, jnp.broadcast_to(hit, (rows, 128)).astype(BF16))
    slot = block.astype(F32) * CAP + rank
    chosen = jnp.where((slot == lane.astype(F32)) & (hit > 0.5), 1.0, 0.0)
    picker_ref[...] = chosen.T[:slots].astype(BF16)
    placer_ref[...] = chosen[:, :slots].astype(BF16)
    weight_ref[...] = jnp.broadcast_to(weight, weight_ref.shape)


def branch_kernel(*refs):
    (picker_ref, placer_ref, weight_ref, eg_ref, eu_ref, ed_ref, dg_ref, du_ref, dd_ref, bw_ref,
     send_ref, hidden_ref, made, gains_ref, x_scr) = refs[7:]
    c = core()
    nz, r2, d = x_scr.shape
    rows, h = nz * r2, d // 2
    to = pl.ds(pl.multiple_of((1 - c) * h, h), h)
    collect(refs[:7], x_scr)
    x = x_scr[...].reshape(rows, d)
    lane = lax.broadcasted_iota(jnp.int32, (rows, 128), 1)
    weight = weight_ref[:, 0:1]
    px = dot(picker_ref[...], x).astype(BF16)
    gate = dot(px, eg_ref[0])
    up = dot(px, eu_ref[0])
    made[...] = dot(silu_mul(gate, up), ed_ref[0]).astype(BF16)

    hidden = silu_mul(dot(x, dg_ref[...]), dot(x, du_ref[...]))
    logit = jnp.sum(x.astype(F32) * bw_ref[...].astype(F32), axis=1, keepdims=True)
    sig = jax.nn.sigmoid(logit)
    hidden_ref[...] = hidden
    gains_ref[...] = jnp.where(lane == 0, sig, weight)
    part = dot(hidden, dd_ref[:, to]) * sig
    send_ref[...] = (part + dot(placer_ref[...], made[:, to]) * weight).astype(BF16)


def rest_kernel(hidden_ref, made_ref, placer_ref, gains_ref, dd_ref, keep_ref):
    c = core()
    h = keep_ref.shape[1]
    at = pl.ds(pl.multiple_of(c * h, h), h)
    part = dot(hidden_ref[...], dd_ref[:, at]) * gains_ref[:, 0:1]
    keep_ref[...] = part + dot(placer_ref[...], made_ref[:, at]) * gains_ref[:, 1:2]


def spread_kernel(keep_ref, got_ref, zero_ref, one_ref, back_ref, up_ref, down_ref, last_ref):
    nz = keep_ref.shape[0]
    order = offsets(nz)

    def term(offset):
        at = order.index(offset % nz)
        return keep_ref[at] + got_ref[at].astype(F32)

    for i, far in enumerate((0, FAR, -FAR)):
        zero_ref[i] = term(far)
        one_ref[i] = term(far + 1)
        back_ref[i] = term(far - 1)
        up_ref[i] = term(far + 2).astype(BF16)
        down_ref[i] = term(far - 2).astype(BF16)
    last_ref[...] = term(8).astype(BF16)


def relay_kernel(own_ref, got_ref, out_ref):
    out_ref[...] = (own_ref[...] + got_ref[...].astype(F32)).astype(BF16)


def fold_kernel(own_ref, a_ref, b_ref, last_ref, own_out, plus_ref, minus_ref):
    def total(i):
        return own_ref[i] + a_ref[i].astype(F32) + b_ref[i].astype(F32)

    own_out[...] = total(0)
    plus_ref[...] = (total(1) + last_ref[...].astype(F32)).astype(BF16)
    minus_ref[...] = total(2).astype(BF16)


def sum_kernel(own_ref, a_ref, b_ref, mine_ref, send_ref):
    c = core()
    r = mine_ref.shape[0]
    total = own_ref[...] + a_ref[...].astype(F32) + b_ref[...].astype(F32)
    mine_ref[...] = jnp.where(c == 0, total[:r], total[r:])
    send_ref[...] = jnp.where(c == 0, total[r:], total[:r])


def final_kernel(mine_ref, got_ref, middle_ref, gains_ref, out_ref):
    c = core()
    h = mine_ref.shape[1]
    mine, got = mine_ref[...], got_ref[...]
    low, high = jnp.where(c == 0, mine, got), jnp.where(c == 0, got, mine)
    square = jnp.sum(low * low, axis=1, keepdims=True) + jnp.sum(high * high, axis=1, keepdims=True)
    scale = lax.rsqrt(square / (2 * h) + 1e-06)
    gains = gains_ref[3:4, :]
    out_ref[:, :h] = (middle_ref[:, :h] + low * scale * gains[:, :h]).astype(BF16)
    out_ref[:, h:] = (middle_ref[:, h:] + high * scale * gains[:, h:]).astype(BF16)


def local(
    resid, norm_gains, w_query, w_key, w_value, w_outgate, w_igate, w_fgate, igate_bias,
    fgate_bias, state_matrix, state_norm, state_max, w_mix_out, routes, route_scores,
    expert_gate, expert_up, expert_down, dense_gate, dense_up, dense_down, branch_weight,
):
    n = lax.axis_size("ep")
    nz = n // 2
    r, d = resid.shape
    h = d // 2
    heads, dh = state_matrix.shape[1:3]
    inner = heads * dh
    groups = [[2 * z + c for z in range(nz)] for c in range(2)]
    pairs = [(i, i ^ 1) for i in range(n)]

    def swap(x):
        return lax.ppermute(x, "ep", pairs)

    def exchange(x):
        return lax.all_to_all(x, "ep", 0, 0, axis_index_groups=groups)

    def shift(x, offset):
        return lax.ppermute(
            x, "ep", [(2 * z + c, 2 * ((z + offset) % nz) + c) for z in range(nz) for c in range(2)])

    tile = (2 * r, h)

    def apart(x, offset):
        return lax.ppermute(
            x, "ep", [(2 * z, 2 * ((z + offset) % nz)) for z in range(nz)]
            + [(2 * z + 1, 2 * ((z - offset) % nz) + 1) for z in range(nz)])

    def gather(own, after):
        far = apart(own, FAR)
        ring, half = call(stack_kernel, [((3, 2 * r, d), BF16), (tile, BF16)],
                          (own, far, swap(far), after))
        last = shift(half, 8 - FAR)
        one = apart(ring, 1)
        two = apart(one, 1)
        return ring, one, swap(one), two, swap(two), last, swap(last)

    other = swap(resid)
    normed, gains = call(
        own_kernel, [((r, d), BF16), (norm_gains.shape, F32)], (resid, norm_gains),
        scratch=[((r, d), BF16)], hbm=(0, 1), sems=2)
    keep, write, new_max, info, w_all, state, mix = call(
        gates_kernel,
        [((r, heads), F32), ((r, heads), F32), ((heads, r), F32), ((8, 128), BF16),
         ((4 * inner // n, d), BF16), (state_matrix.shape, F32), (w_mix_out.shape, BF16)],
        (normed, w_igate.T, w_fgate.T, igate_bias.reshape(1, heads),
         fgate_bias.reshape(1, heads), state_max.T, routes.T, route_scores.T,
         w_query.T, w_key.T, w_value.T, w_outgate.T, state_matrix, w_mix_out),
        scratch=[((heads, d), BF16), ((heads, d), BF16), ((1, heads), F32), ((1, heads), F32),
                 ((heads, r), F32), ((2, r), jnp.int32),
                 ((2, r), BF16), ((128, 128), F32), ((8, 128), F32)],
        hbm=tuple(range(1, 14)), sems=12 + r, held=(4, 5, 6))
    chunk, = call(norm_kernel, [((2 * r, d), BF16)], (normed, other, gains),
                  scratch=[((2 * r, d), F32)])
    pieces = gather(chunk, info)
    projected, = call(
        proj_kernel, [((nz, 2 * r + 8, 4 * inner // n), BF16)],
        (*pieces, w_all, info), scratch=[((nz, 2 * r, d), BF16)])
    a = exchange(projected)
    b = swap(a)
    middle, rows, new_norm, keys, wvt = call(
        cell_kernel,
        [((r, d), F32), ((r, d), BF16), ((r, heads, dh), F32),
         ((heads, 16, dh), F32), ((dh, 128), F32)],
        (a, b, keep, write, state, state_norm, mix, resid, gains),
        scratch=[((nz, 16, dh), F32), ((nz, 16, dh), F32), ((heads, 16, dh), F32),
                 ((128, dh), F32), ((r, inner), BF16)])
    chunk, = call(pair_kernel, [((2 * r, d), BF16)], (rows, swap(rows)),
                  scratch=[((2 * r, d), F32)])
    new_matrix, token = call(
        update_kernel, [(state_matrix.shape, F32), ((8, 128), F32)], (keep, keys, wvt, state),
        scratch=[(state_matrix.shape, F32)], sems=r,
        out_specs=[pl.BlockSpec(memory_space=pltpu.HBM), pl.BlockSpec(memory_space=pltpu.VMEM)])
    pieces = gather(chunk, token)
    picker, placer, weight = call(
        route_kernel,
        [((n * CAP, n * r), BF16), ((n * r, n * CAP), BF16), ((n * r, 128), F32)],
        (a, b), scratch=[((4, n * r, 128), F32)])
    send, hidden, made, scales = call(
        branch_kernel,
        [((n * r, h), BF16), ((n * r, dense_down.shape[0]), BF16), ((n * CAP, d), BF16),
         ((n * r, 128), F32)],
        (*pieces, picker, placer, weight, expert_gate, expert_up, expert_down, dense_gate,
         dense_up, dense_down, branch_weight.reshape(1, d)),
        scratch=[((nz, 2 * r, d), BF16)], vmem=32)
    got = swap(send)
    part, = call(rest_kernel, [((n * r, h), F32)], (hidden, made, placer, scales, dense_down),
                 flops=400000000)
    three = (3,) + tile
    own, one, back, up, down, last = call(
        spread_kernel, [(three, F32)] * 3 + [(three, BF16)] * 2 + [(tile, BF16)],
        (part.reshape((nz,) + tile), got.reshape((nz,) + tile)))
    last = shift(last, 8 - FAR)
    up, down = shift(up, 1), shift(down, -1)
    up, = call(relay_kernel, [(three, BF16)], (one, up))
    down, = call(relay_kernel, [(three, BF16)], (back, down))
    up, down = shift(up, 1), shift(down, -1)
    own, plus, minus = call(fold_kernel, [(tile, F32), (tile, BF16), (tile, BF16)],
                            (own, up, down, last))
    plus, minus = shift(plus, FAR), shift(minus, -FAR)
    mine, send = call(sum_kernel, [((r, h), F32), ((r, h), F32)], (own, plus, minus))
    got = swap(send)
    out, = call(final_kernel, [((r, d), BF16)], (mine, got, middle, gains))
    return (out, new_matrix, new_norm, new_max.T)


def solution(mesh):
    placed = (
        P(("grp", "ep"), None), P(), P(None, "ep"), P(None, "ep"), P(None, "ep"), P(None, "ep"),
        P(), P(), P(), P(), P(("grp", "ep"), None, None, None), P(("grp", "ep"), None, None),
        P(("grp", "ep"), None), P(), P(("grp", "ep"), None), P(("grp", "ep"), None),
        P("ep", None, None), P("ep", None, None), P("ep", None, None), P(None, "ep"),
        P(None, "ep"), P("ep", None), P(),
    )
    return jax.shard_map(
        local,
        mesh=mesh,
        in_specs=placed,
        out_specs=(
            P(("grp", "ep"), None),
            P(("grp", "ep"), None, None, None),
            P(("grp", "ep"), None, None),
            P(("grp", "ep"), None),
        ),
        check_vma=False,
    )
```

```python
import jax
import jax.numpy as jnp
from jax import lax
from jax.experimental import pallas as pl
from jax.experimental.pallas import tpu as pltpu
from jax.sharding import PartitionSpec as P


CAP = 2
INTERPRET = False
F32 = jnp.float32
BF16 = jnp.bfloat16


def in_hbm(x):
    return x if INTERPRET else pltpu.with_memory_space_constraint(x, pltpu.HBM)


def call(kernel, outs, args, scratch=(), vmem=16, flops=1000000, hbm=(), sems=0, held=(), **grid):
    if hbm:
        args = [in_hbm(x) if i in hbm else x for i, x in enumerate(args)]
        grid["in_specs"] = [
            pl.BlockSpec(memory_space=pltpu.HBM if i in hbm else pltpu.VMEM)
            for i in range(len(args))]
    result = pl.pallas_call(
        kernel,
        out_shape=[pltpu.VMEM(s, d) if i in held and not INTERPRET else jax.ShapeDtypeStruct(s, d)
                   for i, (s, d) in enumerate(outs)],
        scratch_shapes=[pltpu.VMEM(s, d) for s, d in scratch]
        + ([pltpu.SemaphoreType.DMA((sems,))] if sems else []),
        **grid,
        compiler_params=pltpu.CompilerParams(vmem_limit_bytes=vmem << 20),
        cost_estimate=pl.CostEstimate(flops=flops, bytes_accessed=1000000, transcendentals=0),
        interpret=INTERPRET,
    )(*args)
    return result


def rms(values, gains):
    return values * lax.rsqrt(jnp.mean(values * values, axis=-1, keepdims=True) + 1e-06) * gains


def core():
    return lax.rem(lax.axis_index("ep"), 2)


def dot_t(a, b):
    return lax.dot_general(a, b, (((1,), (1,)), ((), ())), preferred_element_type=F32)


def dot(a, b):
    return jnp.dot(a, b, preferred_element_type=F32)


def half_of(c, values):
    h = values.shape[-1] // 2
    return jnp.where(c == 0, values[:, :h], values[:, h:])


FAR = 5


def offsets(nz):
    ring = [0, -FAR, FAR]
    near = [n + o for n in (-1, 1, -2, 2) for o in ring]
    return [o % nz for o in ring + near + [-8]]


def own_kernel(resid_hbm, gains_hbm, out_ref, gains_ref, resid, sems):
    copies = [pltpu.make_async_copy(resid_hbm, resid, sems.at[0]),
              pltpu.make_async_copy(gains_hbm, gains_ref, sems.at[1])]
    for copy in copies:
        copy.start()
    for copy in copies:
        copy.wait()
    out_ref[...] = rms(resid[...].astype(F32), gains_ref[0:1, :]).astype(BF16)


def norm_kernel(own_ref, other_ref, gains_ref, out_ref, rows):
    c = core()
    r = own_ref.shape[0]
    own = half_of(c, own_ref[...].astype(F32))
    other = half_of(c, rms(other_ref[...].astype(F32), gains_ref[0:1, :]))
    rows[:r] = jnp.where(c == 0, own, other)
    rows[r : 2 * r] = jnp.where(c == 0, other, own)
    out_ref[...] = rows[...].astype(BF16)


def stack_kernel(a_ref, b_ref, c_ref, after_ref, out_ref):
    out_ref[0] = a_ref[...]
    out_ref[1] = b_ref[...]
    out_ref[2] = c_ref[...]


def gates_kernel(
    normed_ref, wi_hbm, wf_hbm, bi_hbm, bf_hbm, max_hbm, routes_hbm, scores_hbm,
    wq_ref, wk_ref, wv_ref, wo_ref, state_ref, mix_ref,
    keep_ref, write_ref, newmax_ref, info_ref, weights_ref, state_out, mix_out,
    wi_ref, wf_ref, bi_ref, bf_ref, max_ref, routes_ref, scores_ref, turn_ref, info_scr, sems,
):
    heads, r = max_ref.shape
    cols = wq_ref.shape[0]
    small = [(wi_hbm, wi_ref), (wf_hbm, wf_ref), (max_hbm, max_ref), (routes_hbm, routes_ref),
             (scores_hbm, scores_ref), (bi_hbm, bi_ref), (bf_hbm, bf_ref)]
    small = [pltpu.make_async_copy(x, y, sems.at[k]) for k, (x, y) in enumerate(small)]
    copies = [
        pltpu.make_async_copy(w, weights_ref.at[pl.ds(k * cols, cols)], sems.at[7 + k])
        for k, w in enumerate((wq_ref, wk_ref, wv_ref, wo_ref))]
    copies.append(pltpu.make_async_copy(mix_ref, mix_out, sems.at[11]))
    for k in range(state_ref.shape[0]):
        copies.append(pltpu.make_async_copy(state_ref.at[k], state_out.at[k], sems.at[12 + k]))
    for copy in small + copies:
        copy.start()
    for copy in small:
        copy.wait()
    diagonal = lax.broadcasted_iota(jnp.int32, (heads, heads), 0) == lax.broadcasted_iota(
        jnp.int32, (heads, heads), 1)

    def column(bias):
        return jnp.sum(jnp.where(diagonal, bias, 0.0), axis=1, keepdims=True)

    normed = normed_ref[...]
    ipre = dot_t(wi_ref[...], normed) + column(bi_ref[...])
    fpre = dot_t(wf_ref[...], normed) + column(bf_ref[...])
    logf = jnp.minimum(fpre, 0.0) - jnp.log1p(jnp.exp(-jnp.abs(fpre)))
    decayed = logf + max_ref[...]
    new_max = jnp.maximum(ipre, decayed)
    newmax_ref[...] = new_max
    turn_ref[...] = jnp.zeros_like(turn_ref)
    turn_ref[0:heads, :r] = jnp.exp(decayed - new_max)
    keep_ref[...] = turn_ref[...].T[:r, :heads]
    turn_ref[0:heads, :r] = jnp.exp(ipre - new_max)
    write_ref[...] = turn_ref[...].T[:r, :heads]
    info_scr[...] = jnp.zeros_like(info_scr)
    info_scr[0:2, :r] = routes_ref[...].astype(F32)
    info_scr[2:4, :r] = scores_ref[...].astype(F32)
    info_ref[...] = info_scr[...].astype(BF16)
    for copy in copies:
        copy.wait()


def collect(refs, out):
    at = 0
    for ref in refs:
        size = 1
        for extent in ref.shape[:-1]:
            size *= extent
        out[at : at + size] = ref[...].reshape(size, ref.shape[-1])
        at += size


def proj_kernel(*refs):
    xs, ys, (w_ref, info_ref, out_ref, x, y) = refs[:6], refs[6:12], refs[12:]
    c = core()
    z = lax.div(lax.axis_index("ep"), 2)
    nz = out_ref.shape[0]
    h = x.shape[1]
    r2 = x.shape[0] // nz
    collect(xs, x)
    collect(ys, y)
    at = pl.ds(pl.multiple_of(c * h, h), h)
    to = pl.ds(pl.multiple_of((1 - c) * h, h), h)
    p = (dot_t(x[...], w_ref[:, at]) + dot_t(y[...], w_ref[:, to])).astype(BF16)
    for k, offset in enumerate(offsets(nz)):
        where = lax.rem(z + offset, nz)
        out_ref[where, :r2, :] = p[k * r2 : (k + 1) * r2]
        out_ref[k, r2 : r2 + 8, :] = info_ref[...]


def cell_kernel(
    a_ref, b_ref, keep_ref, write_ref, m_ref, norm_ref, mix_ref, resid_ref, gains_ref,
    middle_ref, mine_ref, send_ref, newnorm_ref, keys_ref, wvt_ref,
    p0, p1, q_scr, wv_scr, gated,
):
    c = core()
    r, heads, dh = norm_ref.shape
    nz = a_ref.shape[0]
    cols = heads * dh // (2 * nz)
    per = dh // cols
    p0[...] = jnp.zeros_like(p0)
    p1[...] = jnp.zeros_like(p1)
    for z in range(nz):
        a, b = a_ref[z].astype(F32), b_ref[z].astype(F32)
        a = jnp.where(c == 0, a[:r], a[r : 2 * r])
        b = jnp.where(c == 0, b[:r], b[r : 2 * r])
        p0[z, :r] = jnp.where(c == 0, a, b)
        p1[z, :r] = jnp.where(c == 0, b, a)
    lanes = lax.broadcasted_iota(jnp.int32, (16, dh), 1)

    def gather(h, kind):
        total = jnp.zeros((16, dh), F32)
        for p in range(per):
            ep = h * per + p
            piece = (p0 if ep % 2 == 0 else p1)[ep // 2]
            shift = ((p - kind) * cols) % dh
            piece = pltpu.roll(piece, shift, 1) if shift else piece
            total = jnp.where((lanes >= p * cols) & (lanes < (p + 1) * cols), piece, total)
        return total

    wv_scr[...] = jnp.zeros_like(wv_scr)
    for h in range(heads):
        q_scr[h] = gather(h, 0)
        keys_ref[h] = gather(h, 1) * dh ** (-0.5)
        wv_scr[h * 16 : h * 16 + r] = gather(h, 2)[:r] * write_ref[:, h : h + 1]
    wvt_ref[...] = wv_scr[...].T
    lane128 = lax.broadcasted_iota(jnp.int32, (dh, 128), 1)

    def step(s, acc):
        for h in range(heads):
            prod = m_ref[s, h] * q_scr[h, pl.ds(s, 1), :]
            red = jnp.sum(prod, axis=1, keepdims=True)
            acc = jnp.where(lane128 == h * 16 + s, red, acc)
        return acc

    numer = lax.fori_loop(0, r, step, jnp.zeros((dh, 128), F32)).T
    for h in range(heads):
        query, key = q_scr[h][:r], keys_ref[h][:r]
        outgate = gather(h, 3)[:r]
        keep, write = keep_ref[:, h : h + 1], write_ref[:, h : h + 1]
        new_norm = keep * norm_ref[:, h, :] + write * key
        newnorm_ref[:, h, :] = new_norm
        denom = jnp.sum(new_norm * query, axis=1, keepdims=True)
        kq = jnp.sum(key * query, axis=1, keepdims=True)
        top = keep * numer[h * 16 : h * 16 + r] + wv_scr[h * 16 : h * 16 + r] * kq
        cell = top / jnp.maximum(jnp.abs(denom), 1.0)
        gated[:, h * dh : (h + 1) * dh] = (jax.nn.sigmoid(outgate) * cell).astype(BF16)
    mixed = dot(gated[...], mix_ref[...])
    middle = resid_ref[...].astype(F32) + rms(mixed, gains_ref[1:2, :])
    middle_ref[...] = middle
    branch = rms(middle, gains_ref[2:3, :])
    mine_ref[...] = half_of(c, branch).astype(BF16)
    send_ref[...] = half_of(1 - c, branch).astype(BF16)


def update_kernel(keep_ref, keys_ref, wvt_ref, m_ref, out_ref, token_ref, new, sems):
    r, heads = m_ref.shape[:2]
    token_ref[...] = jnp.zeros_like(token_ref)

    def put(s):
        return pltpu.make_async_copy(new.at[s], out_ref.at[s], sems.at[s])

    def step(s, carry):
        rolled = pltpu.roll(wvt_ref[...], lax.rem(128 - s, 128), 1)
        for h in range(heads):
            keep = keep_ref[pl.ds(s, 1), h : h + 1]
            key = keys_ref[h, pl.ds(s, 1), :]
            new[s, h] = keep * m_ref[s, h] + rolled[:, h * 16 : h * 16 + 1] * key
        put(s).start()
        return carry

    lax.fori_loop(0, r, step, 0)
    for s in range(r):
        put(s).wait()


def pair_kernel(mine_ref, got_ref, out_ref, rows):
    c = core()
    r = mine_ref.shape[0]
    mine, got = mine_ref[...].astype(F32), got_ref[...].astype(F32)
    rows[:r] = jnp.where(c == 0, mine, got)
    rows[r : 2 * r] = jnp.where(c == 0, got, mine)
    out_ref[...] = rows[...].astype(BF16)


def silu_mul(gate, up):
    return (gate * jax.nn.sigmoid(gate) * up).astype(BF16)


def route_kernel(a_ref, b_ref, picker_ref, placer_ref, weight_ref, table):
    c = core()
    me = lax.axis_index("ep").astype(F32)
    home = lax.div(lax.axis_index("ep"), 2)
    nz = a_ref.shape[0]
    slots, rows = picker_ref.shape
    r2 = rows // nz
    r = r2 // 2
    low = lax.broadcasted_iota(jnp.int32, (r2, 128), 0) < r
    for k, offset in enumerate(offsets(nz)):
        z = lax.rem(home + offset, nz)
        a, b = a_ref[z, r2 : r2 + 8, :].astype(F32), b_ref[z, r2 : r2 + 8, :].astype(F32)
        first, second = jnp.where(c == 0, a, b), jnp.where(c == 0, b, a)
        for j in range(4):
            table[j, k * r2 : (k + 1) * r2] = jnp.where(low, first[j : j + 1], second[j : j + 1])
    lane = lax.broadcasted_iota(jnp.int32, (rows, 128), 1)
    token = lax.broadcasted_iota(jnp.int32, (rows, 128), 0)
    block = lax.div(token, r)
    inner = token - block * r

    def column(k):
        return jnp.sum(jnp.where(lane == inner, table[k], 0.0), axis=1, keepdims=True)

    e0, e1, s0, s1 = column(0), column(1), column(2), column(3)
    hit0, hit1 = e0 == me, e1 == me
    hit = jnp.where(hit0 | hit1, 1.0, 0.0)
    weight = jnp.where(hit0, s0, jnp.where(hit1, s1, 0.0)) / (s0 + s1)
    row_i = lax.broadcasted_iota(jnp.int32, (rows, rows), 0)
    col_i = lax.broadcasted_iota(jnp.int32, (rows, rows), 1)
    earlier = (col_i < row_i) & (lax.div(row_i, r) == lax.div(col_i, r))
    earlier = jnp.where(earlier, 1.0, 0.0).astype(BF16)
    rank = dot(earlier, jnp.broadcast_to(hit, (rows, 128)).astype(BF16))
    slot = block.astype(F32) * CAP + rank
    chosen = jnp.where((slot == lane.astype(F32)) & (hit > 0.5), 1.0, 0.0)
    picker_ref[...] = chosen.T[:slots].astype(BF16)
    placer_ref[...] = chosen[:, :slots].astype(BF16)
    weight_ref[...] = jnp.broadcast_to(weight, weight_ref.shape)


def branch_kernel(*refs):
    xs, ys = refs[:6], refs[6:12]
    (picker_ref, placer_ref, weight_ref, eg_ref, eu_ref, ed_ref, dg_ref, du_ref, dd_ref, bw_ref,
     send_ref, hidden_ref, made, gains_ref, x_scr, y_scr) = refs[12:]
    c = core()
    rows, h = x_scr.shape
    at = pl.ds(pl.multiple_of(c * h, h), h)
    to = pl.ds(pl.multiple_of((1 - c) * h, h), h)
    collect(xs, x_scr)
    collect(ys, y_scr)
    x, y = x_scr[...], y_scr[...]
    lane = lax.broadcasted_iota(jnp.int32, (rows, 128), 1)
    picker, weight = picker_ref[...], weight_ref[:, 0:1]
    px = dot(picker, x).astype(BF16)
    py = dot(picker, y).astype(BF16)
    gate = dot(px, eg_ref[0, at, :]) + dot(py, eg_ref[0, to, :])
    up = dot(px, eu_ref[0, at, :]) + dot(py, eu_ref[0, to, :])
    made[...] = dot(silu_mul(gate, up), ed_ref[0]).astype(BF16)

    gate = dot(x, dg_ref[at, :]) + dot(y, dg_ref[to, :])
    up = dot(x, du_ref[at, :]) + dot(y, du_ref[to, :])
    hidden = silu_mul(gate, up)
    logit = jnp.sum(x.astype(F32) * bw_ref[:, at].astype(F32), axis=1, keepdims=True)
    logit = logit + jnp.sum(y.astype(F32) * bw_ref[:, to].astype(F32), axis=1, keepdims=True)
    sig = jax.nn.sigmoid(logit)
    hidden_ref[...] = hidden
    gains_ref[...] = jnp.where(lane == 0, sig, weight)
    part = dot(hidden, dd_ref[:, to]) * sig
    send_ref[...] = (part + dot(placer_ref[...], made[:, to]) * weight).astype(BF16)


def rest_kernel(hidden_ref, made_ref, placer_ref, gains_ref, dd_ref, keep_ref):
    c = core()
    h = keep_ref.shape[1]
    at = pl.ds(pl.multiple_of(c * h, h), h)
    part = dot(hidden_ref[...], dd_ref[:, at]) * gains_ref[:, 0:1]
    keep_ref[...] = part + dot(placer_ref[...], made_ref[:, at]) * gains_ref[:, 1:2]


def spread_kernel(keep_ref, got_ref, zero_ref, one_ref, back_ref, up_ref, down_ref, last_ref):
    nz = keep_ref.shape[0]
    order = offsets(nz)

    def term(offset):
        at = order.index(offset % nz)
        return keep_ref[at] + got_ref[at].astype(F32)

    for i, far in enumerate((0, FAR, -FAR)):
        zero_ref[i] = term(far)
        one_ref[i] = term(far + 1)
        back_ref[i] = term(far - 1)
        up_ref[i] = term(far + 2).astype(BF16)
        down_ref[i] = term(far - 2).astype(BF16)
    last_ref[...] = term(8).astype(BF16)


def relay_kernel(own_ref, got_ref, out_ref):
    out_ref[...] = (own_ref[...] + got_ref[...].astype(F32)).astype(BF16)


def fold_kernel(own_ref, a_ref, b_ref, own_out, minus_ref, plus_ref):
    def total(i):
        return own_ref[i] + a_ref[i].astype(F32) + b_ref[i].astype(F32)

    minus_ref[...] = total(2).astype(BF16)
    plus_ref[...] = total(1)
    own_out[...] = total(0)


def mark_kernel(x_ref, out_ref):
    out_ref[...] = x_ref[...]


def join_kernel(plus_ref, last_ref, mark_ref, out_ref):
    out_ref[...] = (plus_ref[...] + last_ref[...].astype(F32)).astype(BF16)


def sum_kernel(own_ref, a_ref, b_ref, mine_ref, send_ref):
    c = core()
    r = mine_ref.shape[0]
    total = own_ref[...] + a_ref[...].astype(F32) + b_ref[...].astype(F32)
    mine_ref[...] = jnp.where(c == 0, total[:r], total[r:])
    send_ref[...] = jnp.where(c == 0, total[r:], total[:r])


def final_kernel(mine_ref, got_ref, middle_ref, gains_ref, out_ref):
    c = core()
    h = mine_ref.shape[1]
    mine, got = mine_ref[...], got_ref[...]
    low, high = jnp.where(c == 0, mine, got), jnp.where(c == 0, got, mine)
    square = jnp.sum(low * low, axis=1, keepdims=True) + jnp.sum(high * high, axis=1, keepdims=True)
    scale = lax.rsqrt(square / (2 * h) + 1e-06)
    gains = gains_ref[3:4, :]
    out_ref[:, :h] = (middle_ref[:, :h] + low * scale * gains[:, :h]).astype(BF16)
    out_ref[:, h:] = (middle_ref[:, h:] + high * scale * gains[:, h:]).astype(BF16)


def local(
    resid, norm_gains, w_query, w_key, w_value, w_outgate, w_igate, w_fgate, igate_bias,
    fgate_bias, state_matrix, state_norm, state_max, w_mix_out, routes, route_scores,
    expert_gate, expert_up, expert_down, dense_gate, dense_up, dense_down, branch_weight,
):
    n = lax.axis_size("ep")
    nz = n // 2
    r, d = resid.shape
    h = d // 2
    heads, dh = state_matrix.shape[1:3]
    inner = heads * dh
    groups = [[2 * z + c for z in range(nz)] for c in range(2)]
    pairs = [(i, i ^ 1) for i in range(n)]

    def swap(x):
        return lax.ppermute(x, "ep", pairs)

    def exchange(x):
        return lax.all_to_all(x, "ep", 0, 0, axis_index_groups=groups)

    def shift(x, offset):
        return lax.ppermute(
            x, "ep", [(2 * z + c, 2 * ((z + offset) % nz) + c) for z in range(nz) for c in range(2)])

    tile = (2 * r, h)

    def gather(own, after):
        plus, minus = shift(own, FAR), shift(own, -FAR)
        ring, = call(stack_kernel, [((3,) + tile, BF16)], (own, plus, minus, after))
        last = shift(plus, 8 - FAR)
        up, down = shift(ring, 1), shift(ring, -1)
        pieces = (ring, up, down, shift(up, 1), shift(down, -1), last)
        return pieces, [swap(piece) for piece in pieces]

    other = swap(resid)
    normed, gains = call(
        own_kernel, [((r, d), BF16), (norm_gains.shape, F32)], (resid, norm_gains),
        scratch=[((r, d), BF16)], hbm=(0, 1), sems=2)
    keep, write, new_max, info, w_all, state, mix = call(
        gates_kernel,
        [((r, heads), F32), ((r, heads), F32), ((heads, r), F32), ((8, 128), BF16),
         ((4 * inner // n, d), BF16), (state_matrix.shape, F32), (w_mix_out.shape, BF16)],
        (normed, w_igate.T, w_fgate.T, igate_bias.reshape(1, heads),
         fgate_bias.reshape(1, heads), state_max.T, routes.T, route_scores.T,
         w_query.T, w_key.T, w_value.T, w_outgate.T, state_matrix, w_mix_out),
        scratch=[((heads, d), BF16), ((heads, d), BF16), ((1, heads), F32), ((1, heads), F32),
                 ((heads, r), F32), ((2, r), jnp.int32),
                 ((2, r), BF16), ((128, 128), F32), ((8, 128), F32)],
        hbm=tuple(range(1, 14)), sems=12 + r, held=(4, 5, 6))
    chunk, = call(norm_kernel, [(tile, BF16)], (normed, other, gains),
                  scratch=[(tile, F32)])
    xs, ys = gather(chunk, info)
    info, = call(mark_kernel, [(info.shape, BF16)], (info,))
    projected, = call(
        proj_kernel, [((nz, 2 * r + 8, 4 * inner // n), BF16)],
        (*xs, *ys, w_all, info), scratch=[((n * r, h), BF16)] * 2)
    a = exchange(projected)
    b = swap(a)
    middle, mine, send, new_norm, keys, wvt = call(
        cell_kernel,
        [((r, d), F32), ((r, h), BF16), ((r, h), BF16), ((r, heads, dh), F32),
         ((heads, 16, dh), F32), ((dh, 128), F32)],
        (a, b, keep, write, state, state_norm, mix, resid, gains),
        scratch=[((nz, 16, dh), F32), ((nz, 16, dh), F32), ((heads, 16, dh), F32),
                 ((128, dh), F32), ((r, inner), BF16)])
    got = swap(send)
    chunk, = call(pair_kernel, [((2 * r, h), BF16)], (mine, got),
                  scratch=[((2 * r, h), F32)])
    new_matrix, token = call(
        update_kernel, [(state_matrix.shape, F32), ((8, 128), F32)], (keep, keys, wvt, state),
        scratch=[(state_matrix.shape, F32)], sems=r,
        out_specs=[pl.BlockSpec(memory_space=pltpu.HBM), pl.BlockSpec(memory_space=pltpu.VMEM)])
    xs, ys = gather(chunk, token)
    picker, placer, weight = call(
        route_kernel,
        [((n * CAP, n * r), BF16), ((n * r, n * CAP), BF16), ((n * r, 128), F32)],
        (a, b), scratch=[((4, n * r, 128), F32)])
    send, hidden, made, scales = call(
        branch_kernel,
        [((n * r, h), BF16), ((n * r, dense_down.shape[0]), BF16), ((n * CAP, d), BF16),
         ((n * r, 128), F32)],
        (*xs, *ys, picker, placer, weight, expert_gate, expert_up, expert_down, dense_gate,
         dense_up, dense_down, branch_weight.reshape(1, d)),
        scratch=[((n * r, h), BF16), ((n * r, h), BF16)], vmem=32)
    got = swap(send)
    part, = call(rest_kernel, [((n * r, h), F32)], (hidden, made, placer, scales, dense_down),
                 flops=400000000)
    three = (3,) + tile
    own, one, back, up, down, last = call(
        spread_kernel, [(three, F32)] * 3 + [(three, BF16)] * 2 + [(tile, BF16)],
        (part.reshape((nz,) + tile), got.reshape((nz,) + tile)))
    last = shift(last, 8 - FAR)
    up, down = shift(up, 1), shift(down, -1)
    mark, = call(mark_kernel, [(token.shape, F32)], (token,))
    up, = call(relay_kernel, [(three, BF16)], (one, up))
    down, = call(relay_kernel, [(three, BF16)], (back, down))
    up, down = shift(up, 1), shift(down, -1)
    own, minus, plus = call(fold_kernel, [(tile, F32), (tile, BF16), (tile, F32)],
                            (own, up, down))
    minus = shift(minus, -FAR)
    plus, = call(join_kernel, [(tile, BF16)], (plus, last, mark))
    plus = shift(plus, FAR)
    mine, send = call(sum_kernel, [((r, h), F32), ((r, h), F32)], (own, plus, minus))
    got = swap(send)
    out, = call(final_kernel, [((r, d), BF16)], (mine, got, middle, gains))
    return (out, new_matrix, new_norm, new_max.T)


def solution(mesh):
    placed = (
        P(("grp", "ep"), None), P(), P(None, "ep"), P(None, "ep"), P(None, "ep"), P(None, "ep"),
        P(), P(), P(), P(), P(("grp", "ep"), None, None, None), P(("grp", "ep"), None, None),
        P(("grp", "ep"), None), P(), P(("grp", "ep"), None), P(("grp", "ep"), None),
        P("ep", None, None), P("ep", None, None), P("ep", None, None), P(None, "ep"),
        P(None, "ep"), P("ep", None), P(),
    )
    return jax.shard_map(
        local,
        mesh=mesh,
        in_specs=placed,
        out_specs=(
            P(("grp", "ep"), None),
            P(("grp", "ep"), None, None, None),
            P(("grp", "ep"), None, None),
            P(("grp", "ep"), None),
        ),
        check_vma=False,
    )
```

```python
import jax
import jax.numpy as jnp
from jax import lax
from jax.experimental import pallas as pl
from jax.experimental.pallas import tpu as pltpu
from jax.sharding import PartitionSpec as P


CAP = 2
INTERPRET = False
F32 = jnp.float32
BF16 = jnp.bfloat16


def in_hbm(x):
    return x if INTERPRET else pltpu.with_memory_space_constraint(x, pltpu.HBM)


def call(kernel, outs, args, scratch=(), vmem=16, flops=1000000, hbm=(), sems=0, held=(), **grid):
    if hbm:
        args = [in_hbm(x) if i in hbm else x for i, x in enumerate(args)]
        grid["in_specs"] = [
            pl.BlockSpec(memory_space=pltpu.HBM if i in hbm else pltpu.VMEM)
            for i in range(len(args))]
    result = pl.pallas_call(
        kernel,
        out_shape=[pltpu.VMEM(s, d) if i in held and not INTERPRET else jax.ShapeDtypeStruct(s, d)
                   for i, (s, d) in enumerate(outs)],
        scratch_shapes=[pltpu.VMEM(s, d) for s, d in scratch]
        + ([pltpu.SemaphoreType.DMA((sems,))] if sems else []),
        **grid,
        compiler_params=pltpu.CompilerParams(vmem_limit_bytes=vmem << 20),
        cost_estimate=pl.CostEstimate(flops=flops, bytes_accessed=1000000, transcendentals=0),
        interpret=INTERPRET,
    )(*args)
    return result


def rms(values, gains):
    return values * lax.rsqrt(jnp.mean(values * values, axis=-1, keepdims=True) + 1e-06) * gains


def core():
    return lax.rem(lax.axis_index("ep"), 2)


def dot_t(a, b):
    return lax.dot_general(a, b, (((1,), (1,)), ((), ())), preferred_element_type=F32)


def dot(a, b):
    return jnp.dot(a, b, preferred_element_type=F32)


def half_of(c, values):
    h = values.shape[-1] // 2
    return jnp.where(c == 0, values[:, :h], values[:, h:])


FAR = 5


def offsets(nz):
    ring = [0, -FAR, FAR]
    near = [n + o for n in (-1, 1, -2, 2) for o in ring]
    return [o % nz for o in ring + near + [-8]]


def own_kernel(resid_hbm, gains_hbm, out_ref, gains_ref, resid, sems):
    copies = [pltpu.make_async_copy(resid_hbm, resid, sems.at[0]),
              pltpu.make_async_copy(gains_hbm, gains_ref, sems.at[1])]
    for copy in copies:
        copy.start()
    for copy in copies:
        copy.wait()
    out_ref[...] = rms(resid[...].astype(F32), gains_ref[0:1, :]).astype(BF16)


def norm_kernel(own_ref, other_ref, gains_ref, out_ref, rows):
    c = core()
    r = own_ref.shape[0]
    own = half_of(c, own_ref[...].astype(F32))
    other = half_of(c, rms(other_ref[...].astype(F32), gains_ref[0:1, :]))
    rows[:r] = jnp.where(c == 0, own, other)
    rows[r : 2 * r] = jnp.where(c == 0, other, own)
    out_ref[...] = rows[...].astype(BF16)


def stack_kernel(a_ref, b_ref, c_ref, after_ref, out_ref):
    out_ref[0] = a_ref[...]
    out_ref[1] = b_ref[...]
    out_ref[2] = c_ref[...]


def gates_kernel(
    normed_ref, wi_hbm, wf_hbm, bi_hbm, bf_hbm, max_hbm, routes_hbm, scores_hbm,
    wq_ref, wk_ref, wv_ref, wo_ref, state_ref, mix_ref,
    keep_ref, write_ref, newmax_ref, info_ref, weights_ref, state_out, mix_out,
    wi_ref, wf_ref, bi_ref, bf_ref, max_ref, routes_ref, scores_ref, turn_ref, info_scr, sems,
):
    heads, r = max_ref.shape
    cols = wq_ref.shape[0]
    small = [(wi_hbm, wi_ref), (wf_hbm, wf_ref), (max_hbm, max_ref), (routes_hbm, routes_ref),
             (scores_hbm, scores_ref), (bi_hbm, bi_ref), (bf_hbm, bf_ref)]
    small = [pltpu.make_async_copy(x, y, sems.at[k]) for k, (x, y) in enumerate(small)]
    copies = [
        pltpu.make_async_copy(w, weights_ref.at[pl.ds(k * cols, cols)], sems.at[7 + k])
        for k, w in enumerate((wq_ref, wk_ref, wv_ref, wo_ref))]
    copies.append(pltpu.make_async_copy(mix_ref, mix_out, sems.at[11]))
    for k in range(state_ref.shape[0]):
        copies.append(pltpu.make_async_copy(state_ref.at[k], state_out.at[k], sems.at[12 + k]))
    for copy in small + copies:
        copy.start()
    for copy in small:
        copy.wait()
    diagonal = lax.broadcasted_iota(jnp.int32, (heads, heads), 0) == lax.broadcasted_iota(
        jnp.int32, (heads, heads), 1)

    def column(bias):
        return jnp.sum(jnp.where(diagonal, bias, 0.0), axis=1, keepdims=True)

    normed = normed_ref[...]
    ipre = dot_t(wi_ref[...], normed) + column(bi_ref[...])
    fpre = dot_t(wf_ref[...], normed) + column(bf_ref[...])
    logf = jnp.minimum(fpre, 0.0) - jnp.log1p(jnp.exp(-jnp.abs(fpre)))
    decayed = logf + max_ref[...]
    new_max = jnp.maximum(ipre, decayed)
    newmax_ref[...] = new_max
    turn_ref[...] = jnp.zeros_like(turn_ref)
    turn_ref[0:heads, :r] = jnp.exp(decayed - new_max)
    keep_ref[...] = turn_ref[...].T[:r, :heads]
    turn_ref[0:heads, :r] = jnp.exp(ipre - new_max)
    write_ref[...] = turn_ref[...].T[:r, :heads]
    info_scr[...] = jnp.zeros_like(info_scr)
    info_scr[0:2, :r] = routes_ref[...].astype(F32)
    info_scr[2:4, :r] = scores_ref[...].astype(F32)
    info_ref[...] = info_scr[...].astype(BF16)
    for copy in copies:
        copy.wait()


def collect(refs, out):
    at = 0
    for ref in refs:
        size = 1
        for extent in ref.shape[:-1]:
            size *= extent
        out[at : at + size] = ref[...].reshape(size, ref.shape[-1])
        at += size


def proj_kernel(*refs):
    xs, ys, (w_ref, info_ref, out_ref, x, y) = refs[:6], refs[6:12], refs[12:]
    c = core()
    z = lax.div(lax.axis_index("ep"), 2)
    nz = out_ref.shape[0]
    h = x.shape[1]
    r2 = x.shape[0] // nz
    collect(xs, x)
    collect(ys, y)
    at = pl.ds(pl.multiple_of(c * h, h), h)
    to = pl.ds(pl.multiple_of((1 - c) * h, h), h)
    p = (dot_t(x[...], w_ref[:, at]) + dot_t(y[...], w_ref[:, to])).astype(BF16)
    for k, offset in enumerate(offsets(nz)):
        where = lax.rem(z + offset, nz)
        out_ref[where, :r2, :] = p[k * r2 : (k + 1) * r2]
        out_ref[k, r2 : r2 + 8, :] = info_ref[...]


def cell_kernel(
    a_ref, b_ref, keep_ref, write_ref, m_ref, norm_ref, mix_ref, resid_ref, gains_ref,
    middle_ref, mine_ref, send_ref, newnorm_ref, keys_ref, wvt_ref,
    p0, p1, q_scr, wv_scr, gated,
):
    c = core()
    r, heads, dh = norm_ref.shape
    nz = a_ref.shape[0]
    cols = heads * dh // (2 * nz)
    per = dh // cols
    p0[...] = jnp.zeros_like(p0)
    p1[...] = jnp.zeros_like(p1)
    for z in range(nz):
        a, b = a_ref[z].astype(F32), b_ref[z].astype(F32)
        a = jnp.where(c == 0, a[:r], a[r : 2 * r])
        b = jnp.where(c == 0, b[:r], b[r : 2 * r])
        p0[z, :r] = jnp.where(c == 0, a, b)
        p1[z, :r] = jnp.where(c == 0, b, a)
    lanes = lax.broadcasted_iota(jnp.int32, (16, dh), 1)

    def gather(h, kind):
        total = jnp.zeros((16, dh), F32)
        for p in range(per):
            ep = h * per + p
            piece = (p0 if ep % 2 == 0 else p1)[ep // 2]
            shift = ((p - kind) * cols) % dh
            piece = pltpu.roll(piece, shift, 1) if shift else piece
            total = jnp.where((lanes >= p * cols) & (lanes < (p + 1) * cols), piece, total)
        return total

    wv_scr[...] = jnp.zeros_like(wv_scr)
    for h in range(heads):
        q_scr[h] = gather(h, 0)
        keys_ref[h] = gather(h, 1) * dh ** (-0.5)
        wv_scr[h * 16 : h * 16 + r] = gather(h, 2)[:r] * write_ref[:, h : h + 1]
    wvt_ref[...] = wv_scr[...].T
    lane128 = lax.broadcasted_iota(jnp.int32, (dh, 128), 1)

    def step(s, acc):
        for h in range(heads):
            prod = m_ref[s, h] * q_scr[h, pl.ds(s, 1), :]
            red = jnp.sum(prod, axis=1, keepdims=True)
            acc = jnp.where(lane128 == h * 16 + s, red, acc)
        return acc

    numer = lax.fori_loop(0, r, step, jnp.zeros((dh, 128), F32)).T
    for h in range(heads):
        query, key = q_scr[h][:r], keys_ref[h][:r]
        outgate = gather(h, 3)[:r]
        keep, write = keep_ref[:, h : h + 1], write_ref[:, h : h + 1]
        new_norm = keep * norm_ref[:, h, :] + write * key
        newnorm_ref[:, h, :] = new_norm
        denom = jnp.sum(new_norm * query, axis=1, keepdims=True)
        kq = jnp.sum(key * query, axis=1, keepdims=True)
        top = keep * numer[h * 16 : h * 16 + r] + wv_scr[h * 16 : h * 16 + r] * kq
        cell = top / jnp.maximum(jnp.abs(denom), 1.0)
        gated[:, h * dh : (h + 1) * dh] = (jax.nn.sigmoid(outgate) * cell).astype(BF16)
    mixed = dot(gated[...], mix_ref[...])
    middle = resid_ref[...].astype(F32) + rms(mixed, gains_ref[1:2, :])
    middle_ref[...] = middle
    branch = rms(middle, gains_ref[2:3, :])
    mine_ref[...] = half_of(c, branch).astype(BF16)
    send_ref[...] = half_of(1 - c, branch).astype(BF16)


def update_kernel(keep_ref, keys_ref, wvt_ref, m_ref, out_ref, token_ref, new, sems):
    r, heads = m_ref.shape[:2]
    token_ref[...] = jnp.zeros_like(token_ref)

    def put(s):
        return pltpu.make_async_copy(new.at[s], out_ref.at[s], sems.at[s])

    def step(s, carry):
        rolled = pltpu.roll(wvt_ref[...], lax.rem(128 - s, 128), 1)
        for h in range(heads):
            keep = keep_ref[pl.ds(s, 1), h : h + 1]
            key = keys_ref[h, pl.ds(s, 1), :]
            new[s, h] = keep * m_ref[s, h] + rolled[:, h * 16 : h * 16 + 1] * key
        put(s).start()
        return carry

    lax.fori_loop(0, r, step, 0)
    for s in range(r):
        put(s).wait()


def pair_kernel(mine_ref, got_ref, out_ref, rows):
    c = core()
    r = mine_ref.shape[0]
    mine, got = mine_ref[...].astype(F32), got_ref[...].astype(F32)
    rows[:r] = jnp.where(c == 0, mine, got)
    rows[r : 2 * r] = jnp.where(c == 0, got, mine)
    out_ref[...] = rows[...].astype(BF16)


def silu_mul(gate, up):
    return (gate * jax.nn.sigmoid(gate) * up).astype(BF16)


def route_kernel(a_ref, b_ref, picker_ref, placer_ref, weight_ref, table):
    c = core()
    me = lax.axis_index("ep").astype(F32)
    home = lax.div(lax.axis_index("ep"), 2)
    nz = a_ref.shape[0]
    slots, rows = picker_ref.shape
    r2 = rows // nz
    r = r2 // 2
    low = lax.broadcasted_iota(jnp.int32, (r2, 128), 0) < r
    for k, offset in enumerate(offsets(nz)):
        z = lax.rem(home + offset, nz)
        a, b = a_ref[z, r2 : r2 + 8, :].astype(F32), b_ref[z, r2 : r2 + 8, :].astype(F32)
        first, second = jnp.where(c == 0, a, b), jnp.where(c == 0, b, a)
        for j in range(4):
            table[j, k * r2 : (k + 1) * r2] = jnp.where(low, first[j : j + 1], second[j : j + 1])
    lane = lax.broadcasted_iota(jnp.int32, (rows, 128), 1)
    token = lax.broadcasted_iota(jnp.int32, (rows, 128), 0)
    block = lax.div(token, r)
    inner = token - block * r

    def column(k):
        return jnp.sum(jnp.where(lane == inner, table[k], 0.0), axis=1, keepdims=True)

    e0, e1, s0, s1 = column(0), column(1), column(2), column(3)
    hit0, hit1 = e0 == me, e1 == me
    hit = jnp.where(hit0 | hit1, 1.0, 0.0)
    weight = jnp.where(hit0, s0, jnp.where(hit1, s1, 0.0)) / (s0 + s1)
    row_i = lax.broadcasted_iota(jnp.int32, (rows, rows), 0)
    col_i = lax.broadcasted_iota(jnp.int32, (rows, rows), 1)
    earlier = (col_i < row_i) & (lax.div(row_i, r) == lax.div(col_i, r))
    earlier = jnp.where(earlier, 1.0, 0.0).astype(BF16)
    rank = dot(earlier, jnp.broadcast_to(hit, (rows, 128)).astype(BF16))
    slot = block.astype(F32) * CAP + rank
    chosen = jnp.where((slot == lane.astype(F32)) & (hit > 0.5), 1.0, 0.0)
    picker_ref[...] = chosen.T[:slots].astype(BF16)
    placer_ref[...] = chosen[:, :slots].astype(BF16)
    weight_ref[...] = jnp.broadcast_to(weight, weight_ref.shape)


def branch_kernel(*refs):
    xs, ys = refs[:6], refs[6:12]
    (picker_ref, placer_ref, weight_ref, eg_ref, eu_ref, ed_ref, dg_ref, du_ref, dd_ref, bw_ref,
     early_ref, late_ref, hidden_ref, made, gains_ref, x_scr, y_scr) = refs[12:]
    c = core()
    rows, h = x_scr.shape
    at = pl.ds(pl.multiple_of(c * h, h), h)
    to = pl.ds(pl.multiple_of((1 - c) * h, h), h)
    collect(xs, x_scr)
    collect(ys, y_scr)
    x, y = x_scr[...], y_scr[...]
    lane = lax.broadcasted_iota(jnp.int32, (rows, 128), 1)
    picker, weight = picker_ref[...], weight_ref[:, 0:1]
    px = dot(picker, x).astype(BF16)
    py = dot(picker, y).astype(BF16)
    gate = dot(px, eg_ref[0, at, :]) + dot(py, eg_ref[0, to, :])
    up = dot(px, eu_ref[0, at, :]) + dot(py, eu_ref[0, to, :])
    made[...] = dot(silu_mul(gate, up), ed_ref[0]).astype(BF16)

    gate = dot(x, dg_ref[at, :]) + dot(y, dg_ref[to, :])
    up = dot(x, du_ref[at, :]) + dot(y, du_ref[to, :])
    hidden = silu_mul(gate, up)
    logit = jnp.sum(x.astype(F32) * bw_ref[:, at].astype(F32), axis=1, keepdims=True)
    logit = logit + jnp.sum(y.astype(F32) * bw_ref[:, to].astype(F32), axis=1, keepdims=True)
    sig = jax.nn.sigmoid(logit)
    hidden_ref[...] = hidden
    gains_ref[...] = jnp.where(lane == 0, sig, weight)
    part = dot(hidden, dd_ref[:, to]) * sig
    send = (part + dot(placer_ref[...], made[:, to]) * weight).astype(BF16)
    size = rows // 16
    early_ref[...] = send[9 * size : 15 * size]
    late_ref[: 9 * size] = send[: 9 * size]
    late_ref[9 * size :] = send[15 * size :]


def rest_kernel(hidden_ref, made_ref, placer_ref, gains_ref, dd_ref, keep_ref):
    c = core()
    h = keep_ref.shape[1]
    at = pl.ds(pl.multiple_of(c * h, h), h)
    part = dot(hidden_ref[...], dd_ref[:, at]) * gains_ref[:, 0:1]
    keep_ref[...] = part + dot(placer_ref[...], made_ref[:, at]) * gains_ref[:, 1:2]


def early_kernel(keep_ref, got_ref, up_ref, down_ref):
    order = offsets(keep_ref.shape[0])

    def term(offset):
        at = order.index(offset % len(order))
        return (keep_ref[at] + got_ref[at - 9].astype(F32)).astype(BF16)

    for i, far in enumerate((0, FAR, -FAR)):
        up_ref[i] = term(far + 2)
        down_ref[i] = term(far - 2)


def late_kernel(keep_ref, got_ref, zero_ref, one_ref, back_ref, last_ref):
    order = offsets(keep_ref.shape[0])

    def term(offset):
        at = order.index(offset % len(order))
        return keep_ref[at] + got_ref[at if at < 9 else 9].astype(F32)

    for i, far in enumerate((0, FAR, -FAR)):
        zero_ref[i] = term(far)
        one_ref[i] = term(far + 1)
        back_ref[i] = term(far - 1)
    last_ref[...] = term(8).astype(BF16)


def relay_kernel(own_ref, got_ref, out_ref):
    out_ref[...] = (own_ref[...] + got_ref[...].astype(F32)).astype(BF16)


def fold_kernel(own_ref, a_ref, b_ref, own_out, minus_ref, plus_ref):
    def total(i):
        return own_ref[i] + a_ref[i].astype(F32) + b_ref[i].astype(F32)

    minus_ref[...] = total(2).astype(BF16)
    plus_ref[...] = total(1)
    own_out[...] = total(0)


def mark_kernel(x_ref, out_ref):
    out_ref[...] = x_ref[...]


def join_kernel(plus_ref, last_ref, mark_ref, out_ref):
    out_ref[...] = (plus_ref[...] + last_ref[...].astype(F32)).astype(BF16)


def sum_kernel(own_ref, a_ref, b_ref, mine_ref, send_ref):
    c = core()
    r = mine_ref.shape[0]
    total = own_ref[...] + a_ref[...].astype(F32) + b_ref[...].astype(F32)
    mine_ref[...] = jnp.where(c == 0, total[:r], total[r:])
    send_ref[...] = jnp.where(c == 0, total[r:], total[:r])


def final_kernel(mine_ref, got_ref, middle_ref, gains_ref, out_ref):
    c = core()
    h = mine_ref.shape[1]
    mine, got = mine_ref[...], got_ref[...]
    low, high = jnp.where(c == 0, mine, got), jnp.where(c == 0, got, mine)
    square = jnp.sum(low * low, axis=1, keepdims=True) + jnp.sum(high * high, axis=1, keepdims=True)
    scale = lax.rsqrt(square / (2 * h) + 1e-06)
    gains = gains_ref[3:4, :]
    out_ref[:, :h] = (middle_ref[:, :h] + low * scale * gains[:, :h]).astype(BF16)
    out_ref[:, h:] = (middle_ref[:, h:] + high * scale * gains[:, h:]).astype(BF16)


def local(
    resid, norm_gains, w_query, w_key, w_value, w_outgate, w_igate, w_fgate, igate_bias,
    fgate_bias, state_matrix, state_norm, state_max, w_mix_out, routes, route_scores,
    expert_gate, expert_up, expert_down, dense_gate, dense_up, dense_down, branch_weight,
):
    n = lax.axis_size("ep")
    nz = n // 2
    r, d = resid.shape
    h = d // 2
    heads, dh = state_matrix.shape[1:3]
    inner = heads * dh
    groups = [[2 * z + c for z in range(nz)] for c in range(2)]
    pairs = [(i, i ^ 1) for i in range(n)]

    def swap(x):
        return lax.ppermute(x, "ep", pairs)

    def exchange(x):
        return lax.all_to_all(x, "ep", 0, 0, axis_index_groups=groups)

    def shift(x, offset):
        return lax.ppermute(
            x, "ep", [(2 * z + c, 2 * ((z + offset) % nz) + c) for z in range(nz) for c in range(2)])

    tile = (2 * r, h)

    def gather(own, after):
        plus, minus = shift(own, FAR), shift(own, -FAR)
        ring, = call(stack_kernel, [((3,) + tile, BF16)], (own, plus, minus, after))
        last = shift(plus, 8 - FAR)
        up, down = shift(ring, 1), shift(ring, -1)
        pieces = (ring, up, down, shift(up, 1), shift(down, -1), last)
        return pieces, [swap(piece) for piece in pieces]

    other = swap(resid)
    normed, gains = call(
        own_kernel, [((r, d), BF16), (norm_gains.shape, F32)], (resid, norm_gains),
        scratch=[((r, d), BF16)], hbm=(0, 1), sems=2)
    keep, write, new_max, info, w_all, state, mix = call(
        gates_kernel,
        [((r, heads), F32), ((r, heads), F32), ((heads, r), F32), ((8, 128), BF16),
         ((4 * inner // n, d), BF16), (state_matrix.shape, F32), (w_mix_out.shape, BF16)],
        (normed, w_igate.T, w_fgate.T, igate_bias.reshape(1, heads),
         fgate_bias.reshape(1, heads), state_max.T, routes.T, route_scores.T,
         w_query.T, w_key.T, w_value.T, w_outgate.T, state_matrix, w_mix_out),
        scratch=[((heads, d), BF16), ((heads, d), BF16), ((1, heads), F32), ((1, heads), F32),
                 ((heads, r), F32), ((2, r), jnp.int32),
                 ((2, r), BF16), ((128, 128), F32), ((8, 128), F32)],
        hbm=tuple(range(1, 14)), sems=12 + r, held=(4, 5, 6))
    chunk, = call(norm_kernel, [(tile, BF16)], (normed, other, gains),
                  scratch=[(tile, F32)])
    xs, ys = gather(chunk, info)
    projected, = call(
        proj_kernel, [((nz, 2 * r + 8, 4 * inner // n), BF16)],
        (*xs, *ys, w_all, info), scratch=[((n * r, h), BF16)] * 2)
    a = exchange(projected)
    b = swap(a)
    middle, mine, send, new_norm, keys, wvt = call(
        cell_kernel,
        [((r, d), F32), ((r, h), BF16), ((r, h), BF16), ((r, heads, dh), F32),
         ((heads, 16, dh), F32), ((dh, 128), F32)],
        (a, b, keep, write, state, state_norm, mix, resid, gains),
        scratch=[((nz, 16, dh), F32), ((nz, 16, dh), F32), ((heads, 16, dh), F32),
                 ((128, dh), F32), ((r, inner), BF16)])
    got = swap(send)
    chunk, = call(pair_kernel, [((2 * r, h), BF16)], (mine, got),
                  scratch=[((2 * r, h), F32)])
    new_matrix, token = call(
        update_kernel, [(state_matrix.shape, F32), ((8, 128), F32)], (keep, keys, wvt, state),
        scratch=[(state_matrix.shape, F32)], sems=r,
        out_specs=[pl.BlockSpec(memory_space=pltpu.HBM), pl.BlockSpec(memory_space=pltpu.VMEM)])
    xs, ys = gather(chunk, token)
    picker, placer, weight = call(
        route_kernel,
        [((n * CAP, n * r), BF16), ((n * r, n * CAP), BF16), ((n * r, 128), F32)],
        (a, b), scratch=[((4, n * r, 128), F32)])
    early, late, hidden, made, scales = call(
        branch_kernel,
        [((6 * 2 * r, h), BF16), ((10 * 2 * r, h), BF16), ((n * r, dense_down.shape[0]), BF16),
         ((n * CAP, d), BF16),
         ((n * r, 128), F32)],
        (*xs, *ys, picker, placer, weight, expert_gate, expert_up, expert_down, dense_gate,
         dense_up, dense_down, branch_weight.reshape(1, d)),
        scratch=[((n * r, h), BF16), ((n * r, h), BF16)], vmem=32)
    early, late = swap(early), swap(late)
    part, = call(rest_kernel, [((n * r, h), F32)], (hidden, made, placer, scales, dense_down),
                 flops=400000000)
    part = part.reshape((nz,) + tile)
    three = (3,) + tile
    up, down = call(early_kernel, [(three, BF16)] * 2, (part, early.reshape((6,) + tile)))
    own, one, back, last = call(
        late_kernel, [(three, F32)] * 3 + [(tile, BF16)], (part, late.reshape((10,) + tile)))
    last = shift(last, 8 - FAR)
    up, down = shift(up, 1), shift(down, -1)
    mark, = call(mark_kernel, [(token.shape, F32)], (token,))
    up, = call(relay_kernel, [(three, BF16)], (one, up))
    down, = call(relay_kernel, [(three, BF16)], (back, down))
    up, down = shift(up, 1), shift(down, -1)
    own, minus, plus = call(fold_kernel, [(tile, F32), (tile, BF16), (tile, F32)],
                            (own, up, down))
    minus = shift(minus, -FAR)
    plus, = call(join_kernel, [(tile, BF16)], (plus, last, mark))
    plus = shift(plus, FAR)
    mine, send = call(sum_kernel, [((r, h), F32), ((r, h), F32)], (own, plus, minus))
    got = swap(send)
    out, = call(final_kernel, [((r, d), BF16)], (mine, got, middle, gains))
    return (out, new_matrix, new_norm, new_max.T)


def solution(mesh):
    placed = (
        P(("grp", "ep"), None), P(), P(None, "ep"), P(None, "ep"), P(None, "ep"), P(None, "ep"),
        P(), P(), P(), P(), P(("grp", "ep"), None, None, None), P(("grp", "ep"), None, None),
        P(("grp", "ep"), None), P(), P(("grp", "ep"), None), P(("grp", "ep"), None),
        P("ep", None, None), P("ep", None, None), P("ep", None, None), P(None, "ep"),
        P(None, "ep"), P("ep", None), P(),
    )
    return jax.shard_map(
        local,
        mesh=mesh,
        in_specs=placed,
        out_specs=(
            P(("grp", "ep"), None),
            P(("grp", "ep"), None, None, None),
            P(("grp", "ep"), None, None),
            P(("grp", "ep"), None),
        ),
        check_vma=False,
    )
```
